128 devices in a mesh: ep: 64 (over z, y, x), tp: 2 (over core).
Axes of the slice: x: 4, y: 4, z: 4, core: 2. Of those that a mesh axis runs over, the one named last changes fastest.
Arguments:
- tokens: bfloat16 [1536, 4096], P('ep'), may hold values from -6 to 6
- cotangent: bfloat16 [1536, 4096], P('ep'), may hold values from -6 to 6
- routes: int32 [1536, 2], P('ep'), may hold values from 0 to 7, all different within a row; in each aligned block of 24 rows (0 to 23, 24 to 47, ...) at most 12 rows name the same one
- route_weights: float32 [1536, 2], P('ep'), may hold values from 0.1 to 0.9
- gate_weight: bfloat16 [64, 4096, 688], P('ep', None, 'tp'), may hold values from -0.09375 to 0.09375
- up_weight: bfloat16 [64, 4096, 688], P('ep', None, 'tp'), may hold values from -0.09375 to 0.09375
- down_weight: bfloat16 [64, 688, 4096], P('ep', 'tp'), may hold values from -0.078125 to 0.078125
Outputs:
- token_grad: bfloat16 [1536, 4096], P('ep', 'tp')
- route_grad: float32 [1536, 2], P('ep')
- gate_grad: bfloat16 [64, 4096, 688], P('ep', None, 'tp')
- up_grad: bfloat16 [64, 4096, 688], P('ep', None, 'tp')
- down_grad: bfloat16 [64, 688, 4096], P('ep', 'tp')
The draws below stay inside these ranges and needn't reach their ends.
Inputs may be any that keep to these rules, and one draw needn't show every extreme that they name: `routes`: each row names 2 different experts of 0 to 7; within the rows of one device (24 aligned rows) no expert is named more than 12 times, and in some blocks one is named exactly 12 times.
All inputs are finite; a program needn't handle non-finite values.
Results may differ from the reference program's by a relative error of at most 0.01.
Values may be sent and summed in bfloat16 or wider, within the bound.
A program may use at most 192 MiB of HBM per device.

```python
import math
import jax
import jax.numpy as jnp
import numpy as np
from jax import lax

D = 4096
FF = 5504
EXPERTS = 8
TOP = 2
TOK_DEV = 24
CAP = 12
SPAN = 8
TOKENS = 1536
N_EP = 64


def shard_levels(stream_key, shape, split, least, top_value):
    def one(dim, shards_of):
        draws = jax.random.uniform(jax.random.fold_in(jax.random.fold_in(stream_key, 6), dim), (shards_of,), jnp.float32, least / len(split), top_value / len(split))
        return jnp.repeat(jnp.exp(draws), shape[dim] // shards_of).reshape((-1,) + (1,) * (len(shape) - dim - 1))

    gain = one(*split[0])
    for cut in split[1:]:
        gain = gain * one(*cut)
    return gain


def assign_block(rng, own, number, rows, count, top, most, slope):
    ranking = jax.random.permutation(rng, count)
    crowded, ordinary = load_shares(count, rows * top, most, slope, True), load_shares(count, rows * top, most, slope, False)
    places = jnp.arange(count)

    def named(lengths, offset_by):
        used = int((lengths > 0).sum())
        fixed = max(1, used // 4)
        moved = fixed + (places - fixed + offset_by * (used - fixed)) % max(1, count - fixed)
        return jnp.zeros((count,), jnp.int32).at[ranking[jnp.where(places < fixed, places, moved)]].set(jnp.asarray(lengths, jnp.int32))

    lengths = jnp.where(number % 4 == 0, named(crowded, number // 4), named(ordinary, number - number // 4 - 1))
    mixed = jax.random.permutation(jax.random.fold_in(own, 3), count)
    source_of, receiver = mixed[0:count // 2 * 2:2], mixed[1:count // 2 * 2:2]
    margin = jnp.minimum(lengths[source_of] - 1, most - lengths[receiver]) // 2
    margin = jnp.where((source_of == ranking[0]) | (receiver == ranking[0]) | (lengths[receiver] == 0), 0, jnp.maximum(margin, 0))
    moved = jax.random.randint(jax.random.fold_in(own, 4), (count // 2,), 0, 1 << 20) % (margin + 1)
    lengths = lengths.at[source_of].add(-moved).at[receiver].add(moved)
    items = jnp.searchsorted(jnp.cumsum(lengths), jnp.arange(rows * top), side="right").astype(jnp.int32)
    grid = items.reshape(top, rows).T
    grid = grid[jax.random.permutation(jax.random.fold_in(own, 1), rows)]
    offset_by = jax.random.randint(jax.random.fold_in(own, 2), (rows, 1), 0, top)
    return jnp.take_along_axis(grid, (jnp.arange(top)[None, :] + offset_by) % top, axis=1)


def load_shares(amount, total, reach, skew, full):
    loads = [(1 << 20) // math.isqrt(rank ** skew) + 1 for rank in range(1, amount + 1)]
    largest = reach if full else min(reach, max(-(-total // amount), total * loads[0] // sum(loads)))
    least = 1 if total - largest >= amount - 1 else 0
    given, surplus = [largest] + [least] * (amount - 1), total - largest - least * (amount - 1)
    while surplus > 0:
        free = [i for i in range(1, amount) if given[i] < largest] or [i for i in range(1, amount) if given[i] < reach]
        whole, left = sum([loads[i] for i in free]), surplus
        for i in free:
            addition = min(reach - given[i], max(1, left * loads[i] // whole), surplus)
            given[i] = given[i] + addition
            surplus = surplus - addition
    return np.array(given)


def bell_draw(stream_key, shape, spread, reach, pieces=(), kind=jnp.bfloat16):
    factor_of = shard_levels(stream_key, shape, pieces, -0.22, 0.18) if pieces else 1.0
    array = jax.random.normal(stream_key, shape, jnp.float32) * spread * factor_of
    return jnp.minimum(jnp.maximum(array, -reach), reach).astype(kind)


def setup_inputs(seed: int = 0) -> dict:
    splits = jax.random.split(jax.random.key(seed), 8)
    tokens = bell_draw(splits[0], (TOKENS, D), 1.0, 6.0, ((0, 64),))
    cotangent = bell_draw(splits[1], (TOKENS, D), 1.0, 6.0, ((0, 64),))
    routes_keys = jax.random.split(jax.random.fold_in(splits[2], 1), TOKENS // TOK_DEV)
    routes_turns = jax.random.permutation(jax.random.fold_in(splits[2], 3), TOKENS // TOK_DEV)
    routes = jax.vmap(lambda own, number: assign_block(jax.random.fold_in(splits[2], 2), own, number, TOK_DEV, EXPERTS, TOP, CAP, 2))(routes_keys, routes_turns).reshape((TOKENS, TOP))
    route_weights = jnp.clip(0.1 + 0.79999997 * jax.random.uniform(splits[3], (TOKENS, TOP), jnp.float32) ** shard_levels(splits[3], (TOKENS, TOP), ((0, 64),), -0.2, 0.2), 0.1, 0.9)
    gate_weight = bell_draw(splits[4], (EXPERTS * SPAN, D, FF // SPAN), D ** -0.5, 0.09375, ((0, 64), (2, 2)))
    up_weight = bell_draw(splits[5], (EXPERTS * SPAN, D, FF // SPAN), D ** -0.5, 0.09375, ((0, 64), (2, 2)))
    down_weight = bell_draw(splits[6], (EXPERTS * SPAN, FF // SPAN, D), FF ** -0.5, 0.078125, ((0, 64), (1, 2)))
    return {"tokens": tokens, "cotangent": cotangent, "routes": routes, "route_weights": route_weights, "gate_weight": gate_weight, "up_weight": up_weight, "down_weight": down_weight}


def silu_slope(pre_gate):
    sigma = jax.nn.sigmoid(pre_gate)
    return sigma * (1.0 + pre_gate * (1.0 - sigma))


def expert_pass(rows_in, rows_cot, shares, gate_mat, up_mat, down_mat):
    pre_gate = jnp.dot(rows_in, gate_mat, preferred_element_type=jnp.float32)
    pre_up = jnp.dot(rows_in, up_mat, preferred_element_type=jnp.float32)
    active = jax.nn.silu(pre_gate)
    hidden = (active * pre_up).astype(jnp.bfloat16)
    expert_out = jnp.dot(hidden, down_mat, preferred_element_type=jnp.float32)
    share_grad = jnp.sum(rows_cot.astype(jnp.float32) * expert_out, axis=1)
    scaled = (rows_cot.astype(jnp.float32) * shares[:, None]).astype(jnp.bfloat16)
    hidden_grad = lax.dot_general(scaled, down_mat, (((1,), (1,)), ((), ())), preferred_element_type=jnp.float32)
    gate_side = (hidden_grad * pre_up * silu_slope(pre_gate)).astype(jnp.bfloat16)
    up_side = (hidden_grad * active).astype(jnp.bfloat16)
    down_grad = lax.dot_general(hidden, scaled, (((0,), (0,)), ((), ())), preferred_element_type=jnp.float32).astype(jnp.bfloat16)
    gate_grad = lax.dot_general(rows_in, gate_side, (((0,), (0,)), ((), ())), preferred_element_type=jnp.float32).astype(jnp.bfloat16)
    up_grad = lax.dot_general(rows_in, up_side, (((0,), (0,)), ((), ())), preferred_element_type=jnp.float32).astype(jnp.bfloat16)
    token_part = lax.dot_general(gate_side, gate_mat, (((1,), (1,)), ((), ())), preferred_element_type=jnp.float32)
    token_part = token_part + lax.dot_general(up_side, up_mat, (((1,), (1,)), ((), ())), preferred_element_type=jnp.float32)
    return gate_grad, up_grad, down_grad, token_part, share_grad


def reference(tokens, cotangent, routes, route_weights, gate_weight, up_weight, down_weight):
    span = N_EP // EXPERTS
    block = FF // span
    listed = N_EP * CAP
    flat_routes = routes.reshape(-1)
    flat_shares = route_weights.reshape(-1)

    def one_expert(expert):
        chosen = flat_routes == expert
        count = jnp.sum(chosen.astype(jnp.int32))
        pairs = jnp.nonzero(chosen, size=listed, fill_value=0)[0].astype(jnp.int32)
        valid = jnp.arange(listed, dtype=jnp.int32) < count
        rows = (pairs // TOP).astype(jnp.int32)
        shares = jnp.where(valid, flat_shares[pairs], jnp.zeros_like(flat_shares[pairs]))
        start = (expert * span).astype(jnp.int32)
        gate_mat = lax.dynamic_slice_in_dim(gate_weight, start, span, 0).transpose(1, 0, 2).reshape(D, FF)
        up_mat = lax.dynamic_slice_in_dim(up_weight, start, span, 0).transpose(1, 0, 2).reshape(D, FF)
        down_mat = lax.dynamic_slice_in_dim(down_weight, start, span, 0).reshape(FF, D)
        gate_grad, up_grad, down_grad, token_part, share_grad = expert_pass(
            tokens[rows], cotangent[rows], shares, gate_mat, up_mat, down_mat)
        share_grad = jnp.where(valid, share_grad, jnp.zeros_like(share_grad))
        return (gate_grad.reshape(D, span, block).transpose(1, 0, 2),
                up_grad.reshape(D, span, block).transpose(1, 0, 2),
                down_grad.reshape(span, block, D), rows, pairs, token_part, share_grad)

    results = lax.map(one_expert, jnp.arange(EXPERTS, dtype=jnp.int32))
    gate_grad = results[0].reshape(EXPERTS * span, D, block)
    up_grad = results[1].reshape(EXPERTS * span, D, block)
    down_grad = results[2].reshape(EXPERTS * span, block, D)
    token_grad = jnp.zeros((TOKENS, D), jnp.float32).at[results[3].reshape(-1)].add(results[5].reshape(-1, D))
    route_grad = jnp.zeros((TOKENS * TOP,), jnp.float32).at[results[4].reshape(-1)].add(results[6].reshape(-1))
    return token_grad.astype(jnp.bfloat16), route_grad.reshape(TOKENS, TOP), gate_grad, up_grad, down_grad
```

```python
import functools

import jax
import jax.numpy as jnp
from jax import lax
from jax.experimental import pallas as pl
from jax.experimental.pallas import tpu as pltpu
from jax.sharding import PartitionSpec as P

EXPERTS = 8
TOP = 2
CAP = 12
SIDE = 4
ROWS = 32
BUNDLE = 48
LANES = 256
BF = jnp.bfloat16
F32 = jnp.float32
MESH = pl.DeviceIdType.MESH


def dot_nt(a, b):
    return lax.dot_general(a, b, (((1,), (1,)), ((), ())), preferred_element_type=F32)


def dot_tn(a, b):
    return lax.dot_general(a, b, (((0,), (0,)), ((), ())), preferred_element_type=F32)


def dot_nn(a, b):
    return jnp.dot(a, b, preferred_element_type=F32)


def kernel(
    nc, hid,
    src, info, gate, up, down,
    out_tok, out_rg, out_gate, out_up, out_down,
    tz, iz, xc, ob, place, place_t, share,
    stg, stu, wd, wc, pre, hg, gsus, hid_t,
    part, tps, tpr, s_f, xa_f, xb_f, yr_f, zs_f, zr_f,
    part_r, tpr_r, s_r, xa_r, xb_r, yr_r, zs_r, zr_r,
    w_sem, z_send, z_recv, y_send, y_recv, x_send, x_recv, d_send, d_recv,
    e_send, e_recv, a_send, a_recv, b_send, b_recv, v_send, v_recv, q_send, q_recv,
    o_sem,
):
    ep = lax.axis_index("ep")
    core = lax.axis_index("tp")
    z, y, x = ep // 16, (ep // 4) % 4, ep % 4
    pair = y // 2
    low = 256
    rest = hid - low

    def chip(zz, yy, xx):
        return (zz * 16 + yy * 4 + xx, core)

    right = chip(z, y, (x + 1) % 4)
    left = chip(z, y, (x + 3) % 4)
    other_core = (ep, 1 - core)
    partner_y = 2 * pair + (1 - y % 2)
    cross_y = 3 - y
    cross2_y = 2 * (1 - pair) + y % 2
    y_peers = [partner_y, cross_y, cross2_y]
    z_peers = [(z + 1) % 4, (z + 3) % 4, (z + 2) % 4]

    barrier = pltpu.get_barrier_semaphore()
    for zz in z_peers:
        pl.semaphore_signal(barrier, inc=1, device_id=chip(zz, y, x), device_id_type=MESH)
    for yy in y_peers:
        pl.semaphore_signal(barrier, inc=1, device_id=chip(z, yy, x), device_id_type=MESH)
    for dev in (right, left, other_core):
        pl.semaphore_signal(barrier, inc=1, device_id=dev, device_id_type=MESH)

    w_copies = [
        pltpu.make_async_copy(gate.at[0], stg, w_sem.at[0]),
        pltpu.make_async_copy(up.at[0], stu, w_sem.at[1]),
    ]
    for k in range(2 * nc):
        w_copies.append(
            pltpu.make_async_copy(
                down.at[0, :, pl.ds(k * LANES, LANES)], wd.at[k], w_sem.at[2 + k]
            )
        )
    for cp in w_copies:
        cp.start()

    pl.semaphore_wait(barrier, 9)

    def remote(a, b, ss, rs, dev):
        return pltpu.make_async_remote_copy(
            src_ref=a, dst_ref=b, send_sem=ss, recv_sem=rs, device_id=dev, device_id_type=MESH
        )

    def z_copy(c, i):
        return remote(
            src.at[c], tz.at[c, z], z_send.at[c, i], z_recv.at[c, i], chip(z_peers[i], y, x)
        )

    def zi_copy(i):
        return remote(
            info, iz.at[i + 1], z_send.at[nc, i], z_recv.at[nc, i], chip(z_peers[i], y, x)
        )

    for i in range(3):
        zi_copy(i).start()

    def start_z(c, carry):
        for i in range(3):
            z_copy(c, i).start()
        return carry

    lax.fori_loop(0, nc, start_z, 0)

    iz[0] = info[...]
    pre[...] = jnp.zeros_like(pre)
    hg[...] = jnp.zeros_like(hg)
    for i in range(3):
        zi_copy(i).wait_recv()

    slot_number = lax.broadcasted_iota(jnp.int32, (BUNDLE, 128), 0).astype(F32) + 1.0

    def info_row(kind, expert):
        total = iz[0, kind, pl.ds(expert, 1), :]
        for i in range(1, 4):
            total = total + iz[i, kind, pl.ds(expert, 1), :]
        return total

    spare = jnp.zeros((128 - 2 * BUNDLE, 128), F32)
    first, second = [], []
    for side, expert in ((0, 2 * z + pair), (1, 2 * z + 1 - pair)):
        first.append(jnp.where(slot_number == info_row(0, expert), 1.0, 0.0))
        second.append(jnp.where(slot_number == info_row(1, expert), 1.0, 0.0))
        share[side * BUNDLE:(side + 1) * BUNDLE, :] = jnp.broadcast_to(
            jnp.sum((first[side] + second[side]) * info_row(2, expert), axis=1, keepdims=True),
            (BUNDLE, 128),
        )
    first = jnp.concatenate(first + [spare], axis=0)
    second = jnp.concatenate(second + [spare], axis=0)
    place[...] = (first + second).astype(BF)
    place_t[0] = (first + second).T.astype(BF)
    place_t[1] = first.T.astype(BF)
    place_t[2] = second.T.astype(BF)

    def y_copy(c, i):
        k = core * nc + c
        at = pl.ds(x * 192 + y * BUNDLE, BUNDLE)
        from_ref = xc.at[k, :, at, :] if i == 0 else ob.at[c]
        return remote(
            from_ref, xc.at[k, :, at, :], y_send.at[c, i], y_recv.at[c, i],
            chip(z, y_peers[i], x),
        )

    def y_arrival(c, i):
        k = core * nc + c
        at = pl.ds(x * 192 + y_peers[i] * BUNDLE, BUNDLE)
        return remote(
            ob.at[c], xc.at[k, :, at, :], y_send.at[c, i], y_recv.at[c, i],
            chip(z, y_peers[i], x),
        )

    def x_copy(c, i):
        k = core * nc + c
        if i < 2:
            at = pl.ds(x * 192, 192)
        elif i == 2:
            at = pl.ds(((x + 3) % 4) * 192, 96)
        else:
            at = pl.ds(((x + 1) % 4) * 192 + 96, 96)
        return remote(
            xc.at[k, :, at, :], xc.at[k, :, at, :], x_send.at[c, i], x_recv.at[c, i],
            right if i % 2 == 0 else left,
        )

    def x_arrival(c, i):
        k = core * nc + c
        if i == 0:
            at = pl.ds(((x + 3) % 4) * 192, 192)
        elif i == 1:
            at = pl.ds(((x + 1) % 4) * 192, 192)
        elif i == 2:
            at = pl.ds(((x + 2) % 4) * 192, 96)
        else:
            at = pl.ds(((x + 2) % 4) * 192 + 96, 96)
        return remote(
            xc.at[k, :, at, :], xc.at[k, :, at, :], x_send.at[c, i], x_recv.at[c, i],
            right if i % 2 == 0 else left,
        )

    def d_copy(c, k):
        return remote(xc.at[k], xc.at[k], d_send.at[c], d_recv.at[c], other_core)

    def compact(c):
        for i in range(3):
            z_copy(c, i).wait_recv()
        k = core * nc + c
        at = pl.ds(pl.multiple_of(x * 192 + y * BUNDLE, BUNDLE), BUNDLE)
        for tensor in range(2):
            rows = dot_nn(place[:2 * BUNDLE], tz[c, :, tensor].reshape(SIDE * ROWS, LANES))
            if tensor == 1:
                rows = rows * share[:, 0:1]
            rows = rows.astype(BF)
            xc[k, tensor, at, :] = rows[:BUNDLE]
            ob[c, tensor] = rows[BUNDLE:]
        for i in range(3):
            y_copy(c, i).start()

    def products(k):
        for m in range(3):
            rows = pl.ds(m * 256, 256)
            pre[rows, :] += dot_nn(xc[k, 0, rows, :], wc[k])
            hg[rows, :hid] += dot_nt(xc[k, 1, rows, :], wd[k])

    def assemble(k, carry):
        rows = pl.ds(pl.multiple_of(k * LANES, LANES), LANES)
        wc[k, :, 512:768] = jnp.zeros((LANES, 256), BF)
        wc[k, :, 0:256] = stg[rows, 0:256]
        wc[k, :, 256:512] = stu[rows, 0:256]
        wc[k, :, 512:512 + rest] = stg[rows, 256:hid]
        wc[k, :, 640:640 + rest] = stu[rows, 256:hid]
        return carry

    def dispatch(t, carry):
        @pl.when(t < nc)
        def _():
            compact(t)

        @pl.when((t >= 1) & (t < nc + 1))
        def _():
            for i in range(3):
                y_arrival(t - 1, i).wait_recv()
            for i in range(2):
                x_copy(t - 1, i).start()

        @pl.when(t == 1)
        def _():
            for cp in w_copies:
                cp.wait()
            lax.fori_loop(0, 2 * nc, assemble, 0)

        @pl.when((t >= 2) & (t < nc + 2))
        def _():
            for i in range(2):
                x_arrival(t - 2, i).wait_recv()
            for i in range(2, 4):
                x_copy(t - 2, i).start()

        @pl.when((t >= 3) & (t < nc + 3))
        def _():
            for i in range(2, 4):
                x_arrival(t - 3, i).wait_recv()
            d_copy(t - 3, core * nc + t - 3).start()
            products(core * nc + t - 3)

        @pl.when(t >= 4)
        def _():
            d_copy(t - 4, (1 - core) * nc + t - 4).wait_recv()
            products((1 - core) * nc + t - 4)

        return carry

    def own_rows(c, carry):
        tz[c, z] = src[c]
        return carry

    lax.fori_loop(0, nc, own_rows, 0)
    lax.fori_loop(0, nc + 4, dispatch, 0)

    def gates(m, carry):
        rows = pl.ds(pl.multiple_of(m * 128, 128), 128)
        value = jnp.zeros((128, 1), F32)
        for g_at, u_at, h_at, n in ((0, 256, 0, 256), (512, 640, 256, 128)):
            g = pre[rows, g_at:g_at + n]
            u = pre[rows, u_at:u_at + n]
            h = hg[rows, h_at:h_at + n]
            s = jax.nn.sigmoid(g)
            active = g * s
            hidden = (active * u).astype(BF)
            gsus[rows, g_at:g_at + n] = (h * u * (s * (1.0 + g * (1.0 - s)))).astype(BF)
            gsus[rows, u_at:u_at + n] = (h * active).astype(BF)
            hidden = hidden.astype(F32)
            value = value + jnp.sum(hidden * h, axis=1, keepdims=True)
            hid_t[h_at:h_at + n, rows] = hidden.T.astype(BF)
        part_r[rows, :] = jnp.broadcast_to(value, (128, 128)).astype(BF)
        return carry

    lax.fori_loop(0, 6, gates, 0)

    def e_copy(n, feature, c):
        if feature:
            return remote(tps.at[c], tpr.at[c], e_send.at[n], e_recv.at[n], other_core)
        return remote(part_r, tpr_r, e_send.at[n], e_recv.at[n], other_core)

    def pick(feature, c, f_ref, r_ref):
        return f_ref.at[c] if feature else r_ref

    def a_copy(n, feature, c, i):
        s, xa = pick(feature, c, s_f, s_r), pick(feature, c, xa_f, xa_r)
        at = pl.ds(((x + 2) % 4) * 192 + 96 * i, 96)
        return remote(
            s.at[at], xa.at[i], a_send.at[n, i], a_recv.at[n, i], right if i == 0 else left
        )

    def b_copy(n, feature, c, i):
        s, xb = pick(feature, c, s_f, s_r), pick(feature, c, xb_f, xb_r)
        at = pl.ds(((x + 1 + 2 * i) % 4) * 192, 192)
        return remote(
            s.at[at], xb.at[i], b_send.at[n, i], b_recv.at[n, i], right if i == 0 else left
        )

    def v_copy(n, feature, c, i):
        s, yr = pick(feature, c, s_f, s_r), pick(feature, c, yr_f, yr_r)
        at = pl.ds(x * 192 + y_peers[i] * BUNDLE, BUNDLE)
        return remote(
            s.at[at], yr.at[i], v_send.at[n, i], v_recv.at[n, i], chip(z, y_peers[i], x)
        )

    def q_copy(n, feature, c, i):
        zs, zr = pick(feature, c, zs_f, zs_r), pick(feature, c, zr_f, zr_r)
        return remote(
            zs.at[z_peers[i]], zr.at[i], q_send.at[n, i], q_recv.at[n, i], chip(z_peers[i], y, x)
        )

    def stage_core(n, feature, c):
        if not feature:
            e_copy(n, False, c).start()
            return
        k = (1 - core) * nc + c
        for m in range(3):
            rows = pl.ds(m * 256, 256)
            tps[c, rows, :] = dot_nt(gsus[rows, :], wc[k]).astype(BF)
        e_copy(n, True, c).start()
        k = core * nc + c
        for m in range(3):
            rows = pl.ds(m * 256, 256)
            part[c % 2, rows, :] = dot_nt(gsus[rows, :], wc[k])

    def stage_a(n, feature, c):
        e_copy(n, feature, c).wait_recv()
        s = pick(feature, c, s_f, s_r)
        mine = part.at[c % 2] if feature else part_r
        theirs = pick(feature, c, tpr, tpr_r)
        for m in range(3):
            rows = pl.ds(m * 256, 256)
            s[rows, :] = (mine[rows, :].astype(F32) + theirs[rows, :].astype(F32)).astype(BF)
        for i in range(2):
            a_copy(n, feature, c, i).start()

    def stage_b(n, feature, c):
        s, xa = pick(feature, c, s_f, s_r), pick(feature, c, xa_f, xa_r)
        for i in range(2):
            a_copy(n, feature, c, i).wait_recv()
            at = pl.ds(pl.multiple_of(((x + 1 + 2 * i) % 4) * 192 + 96 * i, 96), 96)
            s[at, :] = (s[at, :].astype(F32) + xa[i].astype(F32)).astype(BF)
        for i in range(2):
            b_copy(n, feature, c, i).start()

    def stage_v(n, feature, c):
        s, xb = pick(feature, c, s_f, s_r), pick(feature, c, xb_f, xb_r)
        for i in range(2):
            b_copy(n, feature, c, i).wait_recv()
        at = pl.ds(pl.multiple_of(x * 192, 192), 192)
        s[at, :] = (s[at, :].astype(F32) + xb[0].astype(F32) + xb[1].astype(F32)).astype(BF)
        for i in range(3):
            v_copy(n, feature, c, i).start()

    def stage_q(n, feature, c):
        s, yr = pick(feature, c, s_f, s_r), pick(feature, c, yr_f, yr_r)
        zs = pick(feature, c, zs_f, zs_r)
        for i in range(3):
            v_copy(n, feature, c, i).wait_recv()
        at = pl.ds(pl.multiple_of(x * 192 + y * BUNDLE, BUNDLE), BUNDLE)
        mine = (s[at, :].astype(F32) + yr[0].astype(F32)).astype(BF)
        theirs = (yr[1].astype(F32) + yr[2].astype(F32)).astype(BF)
        slots = jnp.concatenate(
            [mine, theirs, jnp.zeros((128 - 2 * BUNDLE, mine.shape[1]), BF)], axis=0
        )
        if feature:
            rows = dot_nn(place_t[0], slots)
        else:
            lane = lax.broadcasted_iota(jnp.int32, (SIDE * ROWS, 128), 1)
            rows = jnp.where(
                lane == 0,
                dot_nn(place_t[1], slots),
                dot_nn(place_t[2], slots),
            )
        zs[...] = rows.astype(BF).reshape(zs.shape)
        for i in range(3):
            q_copy(n, feature, c, i).start()

    def stage_out(n, feature, c):
        zs, zr = pick(feature, c, zs_f, zs_r), pick(feature, c, zr_f, zr_r)
        for i in range(3):
            q_copy(n, feature, c, i).wait_recv()
        total = zs[z].astype(F32)
        for i in range(3):
            total = total + zr[i].astype(F32)
        if feature:
            out_tok[:, pl.ds(pl.multiple_of(c * LANES, LANES), LANES)] = total[:24].astype(BF)
        else:
            out_rg[...] = total

    def out_copies(k):
        rows = pl.ds(pl.multiple_of(k * LANES, LANES), LANES)
        return (
            pltpu.make_async_copy(stg.at[rows], out_gate.at[0, rows], o_sem.at[k, 0]),
            pltpu.make_async_copy(stu.at[rows], out_up.at[0, rows], o_sem.at[k, 1]),
            pltpu.make_async_copy(wd.at[k], out_down.at[0, :, rows], o_sem.at[k, 2]),
        )

    def weight_grads(k):
        rows = pl.ds(pl.multiple_of(k * LANES, LANES), LANES)
        both = dot_tn(xc[k, 0], gsus[...]).astype(BF)
        stg[rows, 0:256] = both[:, 0:256]
        stu[rows, 0:256] = both[:, 256:512]
        stg[rows, 256:hid] = both[:, 512:512 + rest]
        stu[rows, 256:hid] = both[:, 640:640 + rest]
        wd[k] = dot_nn(hid_t[:hid], xc[k, 1]).astype(BF)
        for cp in out_copies(k):
            cp.start()

    stages = (stage_core, stage_a, stage_b, stage_v, stage_q, stage_out)

    def give_back(t, carry):
        for depth, stage in enumerate(stages):
            n = t - depth

            @pl.when(n == 0)
            def _():
                stage(0, False, 0)

            @pl.when((n >= 1) & (n <= nc))
            def _():
                stage(n, True, n - 1)

        @pl.when(t < nc)
        def _():
            weight_grads(2 * t)
            weight_grads(2 * t + 1)

        return carry

    lax.fori_loop(0, nc + 1 + len(stages) - 1, give_back, 0)

    for i in range(3):
        zi_copy(i).wait_send()

    def drain_dispatch(c, carry):
        for i in range(3):
            z_copy(c, i).wait_send()
            y_copy(c, i).wait_send()
        for i in range(4):
            x_copy(c, i).wait_send()
        d_copy(c, core * nc + c).wait_send()
        return carry

    lax.fori_loop(0, nc, drain_dispatch, 0)

    def drain_return(n, feature, c):
        e_copy(n, feature, c).wait_send()
        for i in range(2):
            a_copy(n, feature, c, i).wait_send()
            b_copy(n, feature, c, i).wait_send()
        for i in range(3):
            v_copy(n, feature, c, i).wait_send()
            q_copy(n, feature, c, i).wait_send()

    drain_return(0, False, 0)

    def drain_features(n, carry):
        drain_return(n, True, n - 1)
        return carry

    lax.fori_loop(1, nc + 1, drain_features, 0)

    def drain_outputs(k, carry):
        for cp in out_copies(k):
            cp.wait()
        return carry

    lax.fori_loop(0, 2 * nc, drain_outputs, 0)


def per_device(tokens, cotangent, routes, route_weights, gate_weight, up_weight, down_weight):
    ep = lax.axis_index("ep")
    core = lax.axis_index("tp")
    z = ep // 16
    rows, width = tokens.shape
    half = width // lax.axis_size("tp")
    nc = half // LANES
    hid = gate_weight.shape[2]

    def halves(a):
        piece = lax.dynamic_slice_in_dim(a, core * half, half, 1)
        piece = jnp.pad(piece, ((0, ROWS - rows), (0, 0)))
        return piece.reshape(ROWS, nc, LANES).transpose(1, 0, 2)

    src = jnp.stack([halves(tokens), halves(cotangent)], axis=1)

    hot = routes[:, :, None] == jnp.arange(EXPERTS, dtype=jnp.int32)[None, None, :]
    hit = jnp.any(hot, axis=1)
    earlier = jnp.arange(rows)[:, None] > jnp.arange(rows)[None, :]
    position = jnp.sum((earlier[:, :, None] & hit[None, :, :]).astype(jnp.int32), axis=1)
    code = (position + z * CAP + 1).astype(F32)
    kinds = jnp.stack(
        [
            jnp.where(hot[:, 0], code, 0.0),
            jnp.where(hot[:, 1], code, 0.0),
            jnp.sum(jnp.where(hot, route_weights[:, :, None], 0.0), axis=1),
        ]
    )
    info = jnp.pad(kinds.transpose(0, 2, 1), ((0, 0), (0, 0), (0, ROWS - rows)))
    column = jnp.arange(SIDE, dtype=jnp.int32) == z
    info = jnp.where(column[None, None, :, None], info[:, :, None, :], 0.0)
    info = info.reshape(3, EXPERTS, SIDE * ROWS)

    vmem, anywhere = pltpu.VMEM, pl.ANY
    slots = 16 * BUNDLE

    def chunk_buffers(lead, lanes):
        return [
            vmem((*lead, slots, lanes), BF),
            vmem((*lead, 2, 96, lanes), BF),
            vmem((*lead, 2, 192, lanes), BF),
            vmem((*lead, 3, BUNDLE, lanes), BF),
            vmem((*lead, SIDE, ROWS, lanes), BF),
            vmem((*lead, 3, ROWS, lanes), BF),
        ]

    dma = pltpu.SemaphoreType.DMA
    token_grad, shares, gate_grad, up_grad, down_grad = pl.pallas_call(
        functools.partial(kernel, nc, hid),
        out_shape=(
            jax.ShapeDtypeStruct((rows, half), BF),
            jax.ShapeDtypeStruct((ROWS, 128), F32),
            jax.ShapeDtypeStruct(gate_weight.shape, BF),
            jax.ShapeDtypeStruct(up_weight.shape, BF),
            jax.ShapeDtypeStruct(down_weight.shape, BF),
        ),
        in_specs=[
            pl.BlockSpec(memory_space=vmem),
            pl.BlockSpec(memory_space=vmem),
            pl.BlockSpec(memory_space=anywhere),
            pl.BlockSpec(memory_space=anywhere),
            pl.BlockSpec(memory_space=anywhere),
        ],
        out_specs=(
            pl.BlockSpec(memory_space=vmem),
            pl.BlockSpec(memory_space=vmem),
            pl.BlockSpec(memory_space=anywhere),
            pl.BlockSpec(memory_space=anywhere),
            pl.BlockSpec(memory_space=anywhere),
        ),
        scratch_shapes=[
            vmem((nc, SIDE, 2, ROWS, LANES), BF),
            vmem((SIDE, 3, EXPERTS, 128), F32),
            vmem((2 * nc, 2, slots, LANES), BF),
            vmem((nc, 2, BUNDLE, LANES), BF),
            vmem((128, 128), BF),
            vmem((3, 128, 128), BF),
            vmem((2 * BUNDLE, 128), F32),
            vmem((width, hid), BF),
            vmem((width, hid), BF),
            vmem((2 * nc, hid, LANES), BF),
            vmem((2 * nc, LANES, 768), BF),
            vmem((slots, 768), F32),
            vmem((slots, 384), F32),
            vmem((slots, 768), BF),
            vmem((384, slots), BF),
            vmem((2, slots, LANES), F32),
            vmem((nc, slots, LANES), BF),
            vmem((nc, slots, LANES), BF),
            *chunk_buffers((nc,), LANES),
            vmem((slots, 128), BF),
            vmem((slots, 128), BF),
            *chunk_buffers((), 128),
            dma((2 + 2 * nc,)),
            dma((nc + 1, 3)), dma((nc + 1, 3)),
            dma((nc, 3)), dma((nc, 3)),
            dma((nc, 4)), dma((nc, 4)),
            dma((nc,)), dma((nc,)),
            dma((nc + 1,)), dma((nc + 1,)),
            dma((nc + 1, 2)), dma((nc + 1, 2)),
            dma((nc + 1, 2)), dma((nc + 1, 2)),
            dma((nc + 1, 3)), dma((nc + 1, 3)),
            dma((nc + 1, 3)), dma((nc + 1, 3)),
            dma((2 * nc, 3)),
        ],
        compiler_params=pltpu.CompilerParams(
            collective_id=0, has_side_effects=True, vmem_limit_bytes=63 * 1024 * 1024
        ),
    )(src, info, gate_weight, up_weight, down_weight)
    route_grad = shares[:rows, :TOP] / route_weights
    return token_grad, route_grad, gate_grad, up_grad, down_grad


def solution(mesh):
    return jax.shard_map(
        per_device,
        mesh=mesh,
        in_specs=(
            P("ep", None),
            P("ep", None),
            P("ep", None),
            P("ep", None),
            P("ep", None, "tp"),
            P("ep", None, "tp"),
            P("ep", "tp", None),
        ),
        out_specs=(
            P("ep", "tp"),
            P("ep", None),
            P("ep", None, "tp"),
            P("ep", None, "tp"),
            P("ep", "tp", None),
        ),
        check_vma=False,
    )
```

```python
import functools

import jax
import jax.numpy as jnp
from jax import lax
from jax.experimental import pallas as pl
from jax.experimental.pallas import tpu as pltpu
from jax.sharding import PartitionSpec as P

EXPERTS = 8
TOP = 2
CAP = 12
SIDE = 4
ROWS = 32
BUNDLE = 48
LANES = 256
SIDE_HID = 384
BF = jnp.bfloat16
F32 = jnp.float32
MESH = pl.DeviceIdType.MESH


def dot_nt(a, b):
    return lax.dot_general(a, b, (((1,), (1,)), ((), ())), preferred_element_type=F32)


def dot_tn(a, b):
    return lax.dot_general(a, b, (((0,), (0,)), ((), ())), preferred_element_type=F32)


def dot_nn(a, b):
    return jnp.dot(a, b, preferred_element_type=F32)


def kernel(
    nc, hid,
    src, info, gate, up, down,
    out_tok, out_rg, out_gate, out_up, out_down,
    tz, iz, xc, ob, place, place_t, share,
    wd, wc, pre, hg, gsus, gsus_t, hid_t,
    part, tps, tpr, s_f, xa_f, xb_f, yr_f, zs_f, zr_f,
    part_r, tpr_r, s_r, xa_r, xb_r, yr_r, zs_r, zr_r,
    w_sem, z_send, z_recv, y_send, y_recv, x_send, x_recv, d_send, d_recv,
    e_send, e_recv, a_send, a_recv, b_send, b_recv, v_send, v_recv, q_send, q_recv,
    o_sem,
):
    ep = lax.axis_index("ep")
    core = lax.axis_index("tp")
    z, y, x = ep // 16, (ep // 4) % 4, ep % 4
    pair = y // 2

    def chip(zz, yy, xx):
        return (zz * 16 + yy * 4 + xx, core)

    right = chip(z, y, (x + 1) % 4)
    left = chip(z, y, (x + 3) % 4)
    other_core = (ep, 1 - core)
    partner_y = 2 * pair + (1 - y % 2)
    cross_y = 3 - y
    cross2_y = 2 * (1 - pair) + y % 2
    y_peers = [partner_y, cross_y, cross2_y]
    z_peers = [(z + 1) % 4, (z + 3) % 4, (z + 2) % 4]

    barrier = pltpu.get_barrier_semaphore()
    for zz in z_peers:
        pl.semaphore_signal(barrier, inc=1, device_id=chip(zz, y, x), device_id_type=MESH)
    for yy in y_peers:
        pl.semaphore_signal(barrier, inc=1, device_id=chip(z, yy, x), device_id_type=MESH)
    for dev in (right, left, other_core):
        pl.semaphore_signal(barrier, inc=1, device_id=dev, device_id_type=MESH)

    w_copies = []
    for k in range(2 * nc):
        at = pl.ds(k * LANES, LANES)
        w_copies += [
            pltpu.make_async_copy(gate.at[0, :, at], wc.at[k, pl.ds(0, hid)], w_sem.at[k, 0]),
            pltpu.make_async_copy(up.at[0, :, at], wc.at[k, pl.ds(SIDE_HID, hid)], w_sem.at[k, 1]),
            pltpu.make_async_copy(down.at[0, :, at], wd.at[k], w_sem.at[k, 2]),
        ]
    for cp in w_copies:
        cp.start()

    pl.semaphore_wait(barrier, 9)

    def remote(a, b, ss, rs, dev):
        return pltpu.make_async_remote_copy(
            src_ref=a, dst_ref=b, send_sem=ss, recv_sem=rs, device_id=dev, device_id_type=MESH
        )

    def z_copy(c, i):
        return remote(
            src.at[c], tz.at[c, z], z_send.at[c, i], z_recv.at[c, i], chip(z_peers[i], y, x)
        )

    def zi_copy(i):
        return remote(
            info, iz.at[i + 1], z_send.at[nc, i], z_recv.at[nc, i], chip(z_peers[i], y, x)
        )

    for i in range(3):
        zi_copy(i).start()

    def start_z(c, carry):
        for i in range(3):
            z_copy(c, i).start()
        return carry

    lax.fori_loop(0, nc, start_z, 0)

    iz[0] = info[...]
    pre[...] = jnp.zeros_like(pre)
    hg[...] = jnp.zeros_like(hg)
    for i in range(3):
        zi_copy(i).wait_recv()

    slot_number = lax.broadcasted_iota(jnp.int32, (BUNDLE, 128), 0).astype(F32) + 1.0

    def info_row(kind, expert):
        total = iz[0, kind, pl.ds(expert, 1), :]
        for i in range(1, 4):
            total = total + iz[i, kind, pl.ds(expert, 1), :]
        return total

    spare = jnp.zeros((128 - 2 * BUNDLE, 128), F32)
    first, second = [], []
    for side, expert in ((0, 2 * z + pair), (1, 2 * z + 1 - pair)):
        first.append(jnp.where(slot_number == info_row(0, expert), 1.0, 0.0))
        second.append(jnp.where(slot_number == info_row(1, expert), 1.0, 0.0))
        share[side * BUNDLE:(side + 1) * BUNDLE, :] = jnp.broadcast_to(
            jnp.sum((first[side] + second[side]) * info_row(2, expert), axis=1, keepdims=True),
            (BUNDLE, 128),
        )
    first = jnp.concatenate(first + [spare], axis=0)
    second = jnp.concatenate(second + [spare], axis=0)
    place[...] = (first + second).astype(BF)
    place_t[0] = (first + second).T.astype(BF)
    place_t[1] = first.T.astype(BF)
    place_t[2] = second.T.astype(BF)

    def y_copy(c, i):
        k = core * nc + c
        at = pl.ds(x * 192 + y * BUNDLE, BUNDLE)
        from_ref = xc.at[k, :, at, :] if i == 0 else ob.at[c]
        return remote(
            from_ref, xc.at[k, :, at, :], y_send.at[c, i], y_recv.at[c, i],
            chip(z, y_peers[i], x),
        )

    def y_arrival(c, i):
        k = core * nc + c
        at = pl.ds(x * 192 + y_peers[i] * BUNDLE, BUNDLE)
        return remote(
            ob.at[c], xc.at[k, :, at, :], y_send.at[c, i], y_recv.at[c, i],
            chip(z, y_peers[i], x),
        )

    def x_copy(c, i):
        k = core * nc + c
        if i < 2:
            at = pl.ds(x * 192, 192)
        elif i == 2:
            at = pl.ds(((x + 3) % 4) * 192, 96)
        else:
            at = pl.ds(((x + 1) % 4) * 192 + 96, 96)
        return remote(
            xc.at[k, :, at, :], xc.at[k, :, at, :], x_send.at[c, i], x_recv.at[c, i],
            right if i % 2 == 0 else left,
        )

    def x_arrival(c, i):
        k = core * nc + c
        if i == 0:
            at = pl.ds(((x + 3) % 4) * 192, 192)
        elif i == 1:
            at = pl.ds(((x + 1) % 4) * 192, 192)
        elif i == 2:
            at = pl.ds(((x + 2) % 4) * 192, 96)
        else:
            at = pl.ds(((x + 2) % 4) * 192 + 96, 96)
        return remote(
            xc.at[k, :, at, :], xc.at[k, :, at, :], x_send.at[c, i], x_recv.at[c, i],
            right if i % 2 == 0 else left,
        )

    def d_copy(c, k):
        return remote(xc.at[k], xc.at[k], d_send.at[c], d_recv.at[c], other_core)

    def compact(c):
        for i in range(3):
            z_copy(c, i).wait_recv()
        k = core * nc + c
        at = pl.ds(pl.multiple_of(x * 192 + y * BUNDLE, BUNDLE), BUNDLE)
        for tensor in range(2):
            rows = dot_nn(place[:2 * BUNDLE], tz[c, :, tensor].reshape(SIDE * ROWS, LANES))
            if tensor == 1:
                rows = rows * share[:, 0:1]
            rows = rows.astype(BF)
            xc[k, tensor, at, :] = rows[:BUNDLE]
            ob[c, tensor] = rows[BUNDLE:]
        for i in range(3):
            y_copy(c, i).start()

    def products(k):
        for m in range(3):
            rows = pl.ds(m * 256, 256)
            pre[rows, :] += dot_nt(xc[k, 0, rows, :], wc[k])
            hg[rows, :hid] += dot_nt(xc[k, 1, rows, :], wd[k])

    def blank(k, carry):
        for at in (hid, SIDE_HID + hid):
            wc[k, at:at + SIDE_HID - hid, :] = jnp.zeros((SIDE_HID - hid, LANES), BF)
        return carry

    lax.fori_loop(0, 2 * nc, blank, 0)

    def dispatch(t, carry):
        @pl.when(t < nc)
        def _():
            compact(t)

        @pl.when((t >= 1) & (t < nc + 1))
        def _():
            for i in range(3):
                y_arrival(t - 1, i).wait_recv()
            for i in range(2):
                x_copy(t - 1, i).start()

        @pl.when(t == 1)
        def _():
            for cp in w_copies:
                cp.wait()

        @pl.when((t >= 2) & (t < nc + 2))
        def _():
            for i in range(2):
                x_arrival(t - 2, i).wait_recv()
            for i in range(2, 4):
                x_copy(t - 2, i).start()

        @pl.when((t >= 3) & (t < nc + 3))
        def _():
            for i in range(2, 4):
                x_arrival(t - 3, i).wait_recv()
            d_copy(t - 3, core * nc + t - 3).start()
            products(core * nc + t - 3)

        @pl.when(t >= 4)
        def _():
            d_copy(t - 4, (1 - core) * nc + t - 4).wait_recv()
            products((1 - core) * nc + t - 4)

        return carry

    def own_rows(c, carry):
        tz[c, z] = src[c]
        return carry

    lax.fori_loop(0, nc, own_rows, 0)
    lax.fori_loop(0, nc + 4, dispatch, 0)

    def gates(m, carry):
        rows = pl.ds(pl.multiple_of(m * 128, 128), 128)
        value = jnp.zeros((128, 1), F32)
        for at in range(0, SIDE_HID, 128):
            g = pre[rows, at:at + 128]
            u = pre[rows, SIDE_HID + at:SIDE_HID + at + 128]
            h = hg[rows, at:at + 128]
            s = jax.nn.sigmoid(g)
            active = g * s
            hidden = (active * u).astype(BF).astype(F32)
            g_side = h * u * (s * (1.0 + g * (1.0 - s)))
            u_side = h * active
            value = value + jnp.sum(hidden * h, axis=1, keepdims=True)
            gsus[rows, at:at + 128] = g_side.astype(BF)
            gsus[rows, SIDE_HID + at:SIDE_HID + at + 128] = u_side.astype(BF)
            hid_t[at:at + 128, rows] = hidden.T.astype(BF)
            gsus_t[at:at + 128, rows] = g_side.T.astype(BF)
            gsus_t[SIDE_HID + at:SIDE_HID + at + 128, rows] = u_side.T.astype(BF)
        part_r[rows, :] = jnp.broadcast_to(value, (128, 128)).astype(BF)
        return carry

    lax.fori_loop(0, 6, gates, 0)

    def e_copy(n, feature, c):
        if feature:
            return remote(tps.at[c], tpr.at[c], e_send.at[n], e_recv.at[n], other_core)
        return remote(part_r, tpr_r, e_send.at[n], e_recv.at[n], other_core)

    def pick(feature, c, f_ref, r_ref):
        return f_ref.at[c] if feature else r_ref

    def a_copy(n, feature, c, i):
        s, xa = pick(feature, c, s_f, s_r), pick(feature, c, xa_f, xa_r)
        at = pl.ds(((x + 2) % 4) * 192 + 96 * i, 96)
        return remote(
            s.at[at], xa.at[i], a_send.at[n, i], a_recv.at[n, i], right if i == 0 else left
        )

    def b_copy(n, feature, c, i):
        s, xb = pick(feature, c, s_f, s_r), pick(feature, c, xb_f, xb_r)
        at = pl.ds(((x + 1 + 2 * i) % 4) * 192, 192)
        return remote(
            s.at[at], xb.at[i], b_send.at[n, i], b_recv.at[n, i], right if i == 0 else left
        )

    def v_copy(n, feature, c, i):
        s, yr = pick(feature, c, s_f, s_r), pick(feature, c, yr_f, yr_r)
        at = pl.ds(x * 192 + y_peers[i] * BUNDLE, BUNDLE)
        return remote(
            s.at[at], yr.at[i], v_send.at[n, i], v_recv.at[n, i], chip(z, y_peers[i], x)
        )

    def q_copy(n, feature, c, i):
        zs, zr = pick(feature, c, zs_f, zs_r), pick(feature, c, zr_f, zr_r)
        return remote(
            zs.at[z_peers[i]], zr.at[i], q_send.at[n, i], q_recv.at[n, i], chip(z_peers[i], y, x)
        )

    def stage_core(n, feature, c):
        if not feature:
            e_copy(n, False, c).start()
            return
        k = (1 - core) * nc + c
        for m in range(3):
            rows = pl.ds(m * 256, 256)
            tps[c, rows, :] = dot_nn(gsus[rows, :], wc[k]).astype(BF)
        e_copy(n, True, c).start()
        k = core * nc + c
        for m in range(3):
            rows = pl.ds(m * 256, 256)
            part[c % 2, rows, :] = dot_nn(gsus[rows, :], wc[k])

    def stage_a(n, feature, c):
        e_copy(n, feature, c).wait_recv()
        s = pick(feature, c, s_f, s_r)
        mine = part.at[c % 2] if feature else part_r
        theirs = pick(feature, c, tpr, tpr_r)
        for m in range(3):
            rows = pl.ds(m * 256, 256)
            s[rows, :] = (mine[rows, :].astype(F32) + theirs[rows, :].astype(F32)).astype(BF)
        for i in range(2):
            a_copy(n, feature, c, i).start()

    def stage_b(n, feature, c):
        s, xa = pick(feature, c, s_f, s_r), pick(feature, c, xa_f, xa_r)
        for i in range(2):
            a_copy(n, feature, c, i).wait_recv()
            at = pl.ds(pl.multiple_of(((x + 1 + 2 * i) % 4) * 192 + 96 * i, 96), 96)
            s[at, :] = (s[at, :].astype(F32) + xa[i].astype(F32)).astype(BF)
        for i in range(2):
            b_copy(n, feature, c, i).start()

    def stage_v(n, feature, c):
        s, xb = pick(feature, c, s_f, s_r), pick(feature, c, xb_f, xb_r)
        for i in range(2):
            b_copy(n, feature, c, i).wait_recv()
        at = pl.ds(pl.multiple_of(x * 192, 192), 192)
        s[at, :] = (s[at, :].astype(F32) + xb[0].astype(F32) + xb[1].astype(F32)).astype(BF)
        for i in range(3):
            v_copy(n, feature, c, i).start()

    def stage_q(n, feature, c):
        s, yr = pick(feature, c, s_f, s_r), pick(feature, c, yr_f, yr_r)
        zs = pick(feature, c, zs_f, zs_r)
        for i in range(3):
            v_copy(n, feature, c, i).wait_recv()
        at = pl.ds(pl.multiple_of(x * 192 + y * BUNDLE, BUNDLE), BUNDLE)
        mine = (s[at, :].astype(F32) + yr[0].astype(F32)).astype(BF)
        theirs = (yr[1].astype(F32) + yr[2].astype(F32)).astype(BF)
        slots = jnp.concatenate(
            [mine, theirs, jnp.zeros((128 - 2 * BUNDLE, mine.shape[1]), BF)], axis=0
        )
        if feature:
            rows = dot_nn(place_t[0], slots)
        else:
            lane = lax.broadcasted_iota(jnp.int32, (SIDE * ROWS, 128), 1)
            rows = jnp.where(
                lane == 0,
                dot_nn(place_t[1], slots),
                dot_nn(place_t[2], slots),
            )
        zs[...] = rows.astype(BF).reshape(zs.shape)
        for i in range(3):
            q_copy(n, feature, c, i).start()

    def stage_out(n, feature, c):
        zs, zr = pick(feature, c, zs_f, zs_r), pick(feature, c, zr_f, zr_r)
        for i in range(3):
            q_copy(n, feature, c, i).wait_recv()
        total = zs[z].astype(F32)
        for i in range(3):
            total = total + zr[i].astype(F32)
        if feature:
            out_tok[:, pl.ds(pl.multiple_of(c * LANES, LANES), LANES)] = total[:24].astype(BF)
        else:
            out_rg[...] = total

    def out_copies(k):
        at = pl.ds(pl.multiple_of(k * LANES, LANES), LANES)
        return (
            pltpu.make_async_copy(wc.at[k, pl.ds(0, hid)], out_gate.at[0, :, at], o_sem.at[k, 0]),
            pltpu.make_async_copy(wc.at[k, pl.ds(SIDE_HID, hid)], out_up.at[0, :, at], o_sem.at[k, 1]),
            pltpu.make_async_copy(wd.at[k], out_down.at[0, :, at], o_sem.at[k, 2]),
        )

    def weight_grads(k):
        for m in range(3):
            rows = pl.ds(m * 256, 256)
            wc[k, rows, :] = dot_nn(gsus_t[rows, :], xc[k, 0]).astype(BF)
        wd[k] = dot_nn(hid_t[:hid], xc[k, 1]).astype(BF)
        for cp in out_copies(k):
            cp.start()

    stages = (stage_core, stage_a, stage_b, stage_v, stage_q, stage_out)

    def give_back(t, carry):
        for depth, stage in enumerate(stages):
            n = t - depth

            @pl.when(n == 0)
            def _():
                stage(0, False, 0)

            @pl.when((n >= 1) & (n <= nc))
            def _():
                stage(n, True, n - 1)

        @pl.when((t >= 1) & (t <= nc))
        def _():
            weight_grads(core * nc + t - 1)
            weight_grads((1 - core) * nc + t - 1)

        return carry

    lax.fori_loop(0, nc + 1 + len(stages) - 1, give_back, 0)

    for i in range(3):
        zi_copy(i).wait_send()

    def drain_dispatch(c, carry):
        for i in range(3):
            z_copy(c, i).wait_send()
            y_copy(c, i).wait_send()
        for i in range(4):
            x_copy(c, i).wait_send()
        d_copy(c, core * nc + c).wait_send()
        return carry

    lax.fori_loop(0, nc, drain_dispatch, 0)

    def drain_return(n, feature, c):
        e_copy(n, feature, c).wait_send()
        for i in range(2):
            a_copy(n, feature, c, i).wait_send()
            b_copy(n, feature, c, i).wait_send()
        for i in range(3):
            v_copy(n, feature, c, i).wait_send()
            q_copy(n, feature, c, i).wait_send()

    drain_return(0, False, 0)

    def drain_features(n, carry):
        drain_return(n, True, n - 1)
        return carry

    lax.fori_loop(1, nc + 1, drain_features, 0)

    def drain_outputs(k, carry):
        for cp in out_copies(k):
            cp.wait()
        return carry

    lax.fori_loop(0, 2 * nc, drain_outputs, 0)


def per_device(tokens, cotangent, routes, route_weights, gate_weight, up_weight, down_weight):
    ep = lax.axis_index("ep")
    core = lax.axis_index("tp")
    z = ep // 16
    rows, width = tokens.shape
    half = width // lax.axis_size("tp")
    nc = half // LANES
    hid = gate_weight.shape[2]

    def halves(a):
        piece = lax.dynamic_slice_in_dim(a, core * half, half, 1)
        piece = jnp.pad(piece, ((0, ROWS - rows), (0, 0)))
        return piece.reshape(ROWS, nc, LANES).transpose(1, 0, 2)

    src = jnp.stack([halves(tokens), halves(cotangent)], axis=1)

    hot = routes[:, :, None] == jnp.arange(EXPERTS, dtype=jnp.int32)[None, None, :]
    hit = jnp.any(hot, axis=1)
    earlier = jnp.arange(rows)[:, None] > jnp.arange(rows)[None, :]
    position = jnp.sum((earlier[:, :, None] & hit[None, :, :]).astype(jnp.int32), axis=1)
    code = (position + z * CAP + 1).astype(F32)
    kinds = jnp.stack(
        [
            jnp.where(hot[:, 0], code, 0.0),
            jnp.where(hot[:, 1], code, 0.0),
            jnp.sum(jnp.where(hot, route_weights[:, :, None], 0.0), axis=1),
        ]
    )
    info = jnp.pad(kinds.transpose(0, 2, 1), ((0, 0), (0, 0), (0, ROWS - rows)))
    column = jnp.arange(SIDE, dtype=jnp.int32) == z
    info = jnp.where(column[None, None, :, None], info[:, :, None, :], 0.0)
    info = info.reshape(3, EXPERTS, SIDE * ROWS)

    vmem, anywhere = pltpu.VMEM, pl.ANY
    slots = 16 * BUNDLE

    def chunk_buffers(lead, lanes):
        return [
            vmem((*lead, slots, lanes), BF),
            vmem((*lead, 2, 96, lanes), BF),
            vmem((*lead, 2, 192, lanes), BF),
            vmem((*lead, 3, BUNDLE, lanes), BF),
            vmem((*lead, SIDE, ROWS, lanes), BF),
            vmem((*lead, 3, ROWS, lanes), BF),
        ]

    dma = pltpu.SemaphoreType.DMA
    token_grad, shares, gate_grad, up_grad, down_grad = pl.pallas_call(
        functools.partial(kernel, nc, hid),
        out_shape=(
            jax.ShapeDtypeStruct((rows, half), BF),
            jax.ShapeDtypeStruct((ROWS, 128), F32),
            jax.ShapeDtypeStruct((1, hid, width), BF),
            jax.ShapeDtypeStruct((1, hid, width), BF),
            jax.ShapeDtypeStruct(down_weight.shape, BF),
        ),
        in_specs=[
            pl.BlockSpec(memory_space=vmem),
            pl.BlockSpec(memory_space=vmem),
            pl.BlockSpec(memory_space=anywhere),
            pl.BlockSpec(memory_space=anywhere),
            pl.BlockSpec(memory_space=anywhere),
        ],
        out_specs=(
            pl.BlockSpec(memory_space=vmem),
            pl.BlockSpec(memory_space=vmem),
            pl.BlockSpec(memory_space=anywhere),
            pl.BlockSpec(memory_space=anywhere),
            pl.BlockSpec(memory_space=anywhere),
        ),
        scratch_shapes=[
            vmem((nc, SIDE, 2, ROWS, LANES), BF),
            vmem((SIDE, 3, EXPERTS, 128), F32),
            vmem((2 * nc, 2, slots, LANES), BF),
            vmem((nc, 2, BUNDLE, LANES), BF),
            vmem((128, 128), BF),
            vmem((3, 128, 128), BF),
            vmem((2 * BUNDLE, 128), F32),
            vmem((2 * nc, hid, LANES), BF),
            vmem((2 * nc, 2 * SIDE_HID, LANES), BF),
            vmem((slots, 2 * SIDE_HID), F32),
            vmem((slots, SIDE_HID), F32),
            vmem((slots, 2 * SIDE_HID), BF),
            vmem((2 * SIDE_HID, slots), BF),
            vmem((SIDE_HID, slots), BF),
            vmem((2, slots, LANES), F32),
            vmem((nc, slots, LANES), BF),
            vmem((nc, slots, LANES), BF),
            *chunk_buffers((nc,), LANES),
            vmem((slots, 128), BF),
            vmem((slots, 128), BF),
            *chunk_buffers((), 128),
            dma((2 * nc, 3)),
            dma((nc + 1, 3)), dma((nc + 1, 3)),
            dma((nc, 3)), dma((nc, 3)),
            dma((nc, 4)), dma((nc, 4)),
            dma((nc,)), dma((nc,)),
            dma((nc + 1,)), dma((nc + 1,)),
            dma((nc + 1, 2)), dma((nc + 1, 2)),
            dma((nc + 1, 2)), dma((nc + 1, 2)),
            dma((nc + 1, 3)), dma((nc + 1, 3)),
            dma((nc + 1, 3)), dma((nc + 1, 3)),
            dma((2 * nc, 3)),
        ],
        compiler_params=pltpu.CompilerParams(
            collective_id=0, has_side_effects=True, vmem_limit_bytes=63 * 1024 * 1024
        ),
    )(src, info, gate_weight.transpose(0, 2, 1), up_weight.transpose(0, 2, 1), down_weight)
    route_grad = shares[:rows, :TOP] / route_weights
    return token_grad, route_grad, gate_grad.transpose(0, 2, 1), up_grad.transpose(0, 2, 1), down_grad


def solution(mesh):
    return jax.shard_map(
        per_device,
        mesh=mesh,
        in_specs=(
            P("ep", None),
            P("ep", None),
            P("ep", None),
            P("ep", None),
            P("ep", None, "tp"),
            P("ep", None, "tp"),
            P("ep", "tp", None),
        ),
        out_specs=(
            P("ep", "tp"),
            P("ep", None),
            P("ep", None, "tp"),
            P("ep", None, "tp"),
            P("ep", "tp", None),
        ),
        check_vma=False,
    )
```

```python
import functools

import jax
import jax.numpy as jnp
from jax import lax
from jax.experimental import pallas as pl
from jax.experimental.pallas import tpu as pltpu
from jax.sharding import PartitionSpec as P

EXPERTS = 8
TOP = 2
CAP = 12
SIDE = 4
ROWS = 32
BUNDLE = 48
LANES = 256
AHEAD = 3
SIDE_HID = 384
BF = jnp.bfloat16
F32 = jnp.float32
MESH = pl.DeviceIdType.MESH


def dot_nt(a, b):
    return lax.dot_general(a, b, (((1,), (1,)), ((), ())), preferred_element_type=F32)


def dot_tn(a, b):
    return lax.dot_general(a, b, (((0,), (0,)), ((), ())), preferred_element_type=F32)


def dot_nn(a, b):
    return jnp.dot(a, b, preferred_element_type=F32)


def kernel(
    nc, hid,
    tokens, cotangent, routes, weights, gate, up, down,
    out_tok, out_rg, out_gate, out_up, out_down,
    tz, info, iz, codes, xc, ob, place, place_t, share,
    wd, wc, pre, hg, gsus, gsus_t, hid_t,
    part, tps, tpr, s_f, xa_f, xb_f, yr_f, zs_f, zr_f,
    part_r, tpr_r, s_r, xa_r, xb_r, yr_r, zs_r, zr_r,
    w_sem, own_sem, z_send, z_recv, i_send, i_recv, y_send, y_recv, x_send, x_recv, p_send, p_recv, d_send, d_recv,
    e_send, e_recv, a_send, a_recv, b_send, b_recv, v_send, v_recv, q_send, q_recv,
    o_sem,
):
    ep = lax.axis_index("ep")
    core = lax.axis_index("tp")
    z, y, x = ep // 16, (ep // 4) % 4, ep % 4
    pair = y // 2

    def chip(zz, yy, xx):
        return (zz * 16 + yy * 4 + xx, core)

    right = chip(z, y, (x + 1) % 4)
    left = chip(z, y, (x + 3) % 4)
    other_core = (ep, 1 - core)
    partner_y = 2 * pair + (1 - y % 2)
    cross_y = 3 - y
    cross2_y = 2 * (1 - pair) + y % 2
    y_peers = [partner_y, cross_y, cross2_y]
    z_peers = [(z + 1) % 4, (z + 3) % 4, (z + 2) % 4]

    rows_dev = tokens.shape[0]
    half_of = ((y + 1) // 2) % 2

    def block(xs, ys):
        return xs * 192 + (((ys + 1) // 2) % 2) * 96 + (ys // 2) * BUNDLE

    def pad_rows(c, carry):
        tz[c, :, :, rows_dev:, :] = jnp.zeros((SIDE, 2, ROWS - rows_dev, LANES), BF)
        return carry

    lax.fori_loop(0, nc, pad_rows, 0)

    barrier = pltpu.get_barrier_semaphore()
    for zz in z_peers:
        pl.semaphore_signal(barrier, inc=1, device_id=chip(zz, y, x), device_id_type=MESH)
    for yy in y_peers:
        pl.semaphore_signal(barrier, inc=1, device_id=chip(z, yy, x), device_id_type=MESH)
    for dev in (right, left, other_core):
        pl.semaphore_signal(barrier, inc=1, device_id=dev, device_id_type=MESH)

    w_copies = []
    for k in range(2 * nc):
        at = pl.ds(k * LANES, LANES)
        w_copies += [
            pltpu.make_async_copy(gate.at[0, :, at], wc.at[k, pl.ds(0, hid)], w_sem.at[k, 0]),
            pltpu.make_async_copy(up.at[0, :, at], wc.at[k, pl.ds(SIDE_HID, hid)], w_sem.at[k, 1]),
            pltpu.make_async_copy(down.at[0, :, at], wd.at[k], w_sem.at[k, 2]),
        ]
    for cp in w_copies:
        cp.start()

    pl.semaphore_wait(barrier, 9)

    def remote(a, b, ss, rs, dev):
        return pltpu.make_async_remote_copy(
            src_ref=a, dst_ref=b, send_sem=ss, recv_sem=rs, device_id=dev, device_id_type=MESH
        )

    def piece(ref, c):
        return ref.at[:, pl.ds(pl.multiple_of((core * nc + c) * LANES, LANES), LANES)]

    def landing(c, tensor):
        return tz.at[c, z, tensor, pl.ds(0, rows_dev)]

    def z_copy(c, i, tensor):
        return remote(
            piece(cotangent if tensor else tokens, c), landing(c, tensor),
            z_send.at[c, i, tensor], z_recv.at[c, i, tensor], chip(z_peers[i], y, x),
        )

    def own_copy(c, tensor):
        return pltpu.make_async_copy(
            piece(cotangent if tensor else tokens, c), landing(c, tensor), own_sem.at[c, tensor]
        )

    def zi_copy(i):
        return remote(info, iz.at[z], i_send.at[i], i_recv.at[i], chip(z_peers[i], y, x))

    def start_z(c):
        for tensor in range(2):
            for i in range(3):
                z_copy(c, i, tensor).start()
            own_copy(c, tensor).start()

    start_z(0)

    expert_row = lax.broadcasted_iota(jnp.int32, (EXPERTS, rows_dev), 0)
    hot = [expert_row == routes[k:k + 1, :] for k in range(2)]
    hit = jnp.where(hot[0] | hot[1], 1.0, 0.0).astype(BF)
    before = jnp.where(
        lax.broadcasted_iota(jnp.int32, (rows_dev, rows_dev), 0)
        < lax.broadcasted_iota(jnp.int32, (rows_dev, rows_dev), 1),
        1.0, 0.0,
    ).astype(BF)
    code = dot_nn(hit, before) + (z * CAP + 1).astype(F32)
    info[...] = jnp.zeros_like(info)
    for k in range(2):
        info[k, :, 0:rows_dev] = jnp.where(hot[k], code, 0.0)
    info[2, :, 0:rows_dev] = jnp.where(hot[0], weights[0:1, :], 0.0) + jnp.where(
        hot[1], weights[1:2, :], 0.0
    )
    for i in range(3):
        zi_copy(i).start()
    for c in range(1, AHEAD):
        start_z(c)
    iz[z] = info[...]
    pre[...] = jnp.zeros_like(pre)
    hg[...] = jnp.zeros_like(hg)
    for i in range(3):
        zi_copy(i).wait_recv()
    for kind in range(3):
        total = iz[0, kind]
        for zz in range(1, SIDE):
            total = total + pltpu.roll(iz[zz, kind], zz * ROWS, 1)
        codes[kind] = total

    slot_number = lax.broadcasted_iota(jnp.int32, (BUNDLE, 128), 0).astype(F32) + 1.0

    def info_row(kind, expert):
        return codes[kind, pl.ds(expert, 1), :]

    spare = jnp.zeros((128 - 2 * BUNDLE, 128), F32)
    first, second = [], []
    for side, expert in ((0, 2 * z + pair), (1, 2 * z + 1 - pair)):
        first.append(jnp.where(slot_number == info_row(0, expert), 1.0, 0.0))
        second.append(jnp.where(slot_number == info_row(1, expert), 1.0, 0.0))
        share[side * BUNDLE:(side + 1) * BUNDLE, :] = jnp.broadcast_to(
            jnp.sum((first[side] + second[side]) * info_row(2, expert), axis=1, keepdims=True),
            (BUNDLE, 128),
        )
    first = jnp.concatenate(first + [spare], axis=0)
    second = jnp.concatenate(second + [spare], axis=0)
    place[...] = (first + second).astype(BF)
    place_t[0] = (first + second).T.astype(BF)
    place_t[1] = first.T.astype(BF)
    place_t[2] = second.T.astype(BF)

    def y_copy(c, i):
        k = core * nc + c
        at = pl.ds(block(x, y), BUNDLE)
        tensor = 1 if i == 3 else 0
        peer = cross_y if i == 3 else y_peers[i]
        from_ref = xc.at[k, 0, at, :] if i == 0 else ob.at[c, tensor]
        return remote(
            from_ref, xc.at[k, tensor, at, :], y_send.at[c, i], y_recv.at[c, i], chip(z, peer, x)
        )

    def x_copy(c, i):
        k = core * nc + c
        tensor = i // 4
        step = i % 4
        size, base = (96, half_of * 96) if tensor else (192, 0)
        if step < 2:
            at = pl.ds(x * 192 + base, size)
        elif step == 2:
            at = pl.ds(((x + 3) % 4) * 192 + base, size // 2)
        else:
            at = pl.ds(((x + 1) % 4) * 192 + base + size // 2, size // 2)
        ref = xc.at[k, tensor, at, :]
        return remote(
            ref, ref, x_send.at[c, i], x_recv.at[c, i], right if i % 2 == 0 else left
        )

    def p_copy(c, i):
        at = pl.ds(((x + (0, 3, 1, 2)[i]) % 4) * 192 + half_of * 96, 96)
        ref = xc.at[core * nc + c, 1, at, :]
        return remote(ref, ref, p_send.at[c, i], p_recv.at[c, i], chip(z, partner_y, x))

    def d_copy(c, k, tensor):
        ref = xc.at[k, tensor]
        return remote(ref, ref, d_send.at[c, tensor], d_recv.at[c, tensor], other_core)

    def compact(c):
        for tensor in range(2):
            for i in range(3):
                z_copy(c, i, tensor).wait_recv()
            own_copy(c, tensor).wait()

        @pl.when(c + AHEAD < nc)
        def _():
            start_z(c + AHEAD)

        k = core * nc + c
        at = pl.ds(pl.multiple_of(block(x, y), BUNDLE), BUNDLE)
        for tensor in (1, 0):
            rows = dot_nn(place[:2 * BUNDLE], tz[c, :, tensor].reshape(SIDE * ROWS, LANES))
            if tensor == 1:
                rows = rows * share[:, 0:1]
            rows = rows.astype(BF)
            xc[k, tensor, at, :] = rows[:BUNDLE]
            ob[c, tensor] = rows[BUNDLE:]
            for i in ((3,) if tensor else (0, 1, 2)):
                y_copy(c, i).start()

    def products(k):
        for m in range(3):
            rows = pl.ds(m * 256, 256)
            pre[rows, :] += dot_nt(xc[k, 0, rows, :], wc[k])
            hg[rows, :hid] += dot_nt(xc[k, 1, rows, :], wd[k])

    def blank(k, carry):
        for at in (hid, SIDE_HID + hid):
            wc[k, at:at + SIDE_HID - hid, :] = jnp.zeros((SIDE_HID - hid, LANES), BF)
        return carry

    lax.fori_loop(0, 2 * nc, blank, 0)

    def dispatch(t, carry):
        @pl.when(t < nc)
        def _():
            compact(t)

        @pl.when((t >= 1) & (t < nc + 1))
        def _():
            c = t - 1
            y_copy(c, 3).wait_recv()
            x_copy(c, 4).start()
            x_copy(c, 5).start()
            p_copy(c, 0).start()
            for i in range(3):
                y_copy(c, i).wait_recv()
            x_copy(c, 0).start()
            x_copy(c, 1).start()

        @pl.when(t == 1)
        def _():
            for cp in w_copies:
                cp.wait()

        @pl.when((t >= 2) & (t < nc + 2))
        def _():
            c = t - 2
            for side in range(2):
                x_copy(c, 4 + side).wait_recv()
                x_copy(c, 6 + side).start()
                p_copy(c, 1 + side).start()
            for side in range(2):
                x_copy(c, side).wait_recv()
                x_copy(c, 2 + side).start()

        @pl.when((t >= 3) & (t < nc + 3))
        def _():
            c = t - 3
            for side in range(2):
                x_copy(c, 6 + side).wait_recv()
            p_copy(c, 3).start()
            for side in range(2):
                x_copy(c, 2 + side).wait_recv()
            d_copy(c, core * nc + c, 0).start()

        @pl.when((t >= 4) & (t < nc + 4))
        def _():
            c = t - 4
            for i in range(4):
                p_copy(c, i).wait_recv()
            d_copy(c, core * nc + c, 1).start()
            products(core * nc + c)

        @pl.when(t >= 5)
        def _():
            c = t - 5
            for tensor in range(2):
                d_copy(c, (1 - core) * nc + c, tensor).wait_recv()
            products((1 - core) * nc + c)

        return carry

    lax.fori_loop(0, nc + 5, dispatch, 0)

    def gates(m, carry):
        rows = pl.ds(pl.multiple_of(m * 128, 128), 128)
        value = jnp.zeros((128, 1), F32)
        for at in range(0, SIDE_HID, 128):
            g = pre[rows, at:at + 128]
            u = pre[rows, SIDE_HID + at:SIDE_HID + at + 128]
            h = hg[rows, at:at + 128]
            s = jax.nn.sigmoid(g)
            active = g * s
            hidden = (active * u).astype(BF).astype(F32)
            g_side = h * u * (s * (1.0 + g * (1.0 - s)))
            u_side = h * active
            value = value + jnp.sum(hidden * h, axis=1, keepdims=True)
            gsus[rows, at:at + 128] = g_side.astype(BF)
            gsus[rows, SIDE_HID + at:SIDE_HID + at + 128] = u_side.astype(BF)
            hid_t[at:at + 128, rows] = hidden.T.astype(BF)
            gsus_t[at:at + 128, rows] = g_side.T.astype(BF)
            gsus_t[SIDE_HID + at:SIDE_HID + at + 128, rows] = u_side.T.astype(BF)
        part_r[rows, :] = jnp.broadcast_to(value, (128, 128)).astype(BF)
        return carry

    lax.fori_loop(0, 6, gates, 0)

    def e_copy(n, feature, c):
        if feature:
            return remote(tps.at[c], tpr.at[c], e_send.at[n], e_recv.at[n], other_core)
        return remote(part_r, tpr_r, e_send.at[n], e_recv.at[n], other_core)

    def pick(feature, c, f_ref, r_ref):
        return f_ref.at[c] if feature else r_ref

    def a_copy(n, feature, c, i):
        s, xa = pick(feature, c, s_f, s_r), pick(feature, c, xa_f, xa_r)
        at = pl.ds(((x + 2) % 4) * 192 + 96 * i, 96)
        return remote(
            s.at[at], xa.at[i], a_send.at[n, i], a_recv.at[n, i], right if i == 0 else left
        )

    def b_copy(n, feature, c, i):
        s, xb = pick(feature, c, s_f, s_r), pick(feature, c, xb_f, xb_r)
        at = pl.ds(((x + 1 + 2 * i) % 4) * 192, 192)
        return remote(
            s.at[at], xb.at[i], b_send.at[n, i], b_recv.at[n, i], right if i == 0 else left
        )

    def v_copy(n, feature, c, i):
        s, yr = pick(feature, c, s_f, s_r), pick(feature, c, yr_f, yr_r)
        at = pl.ds(block(x, y_peers[i]), BUNDLE)
        return remote(
            s.at[at], yr.at[i], v_send.at[n, i], v_recv.at[n, i], chip(z, y_peers[i], x)
        )

    def q_copy(n, feature, c, i):
        zs, zr = pick(feature, c, zs_f, zs_r), pick(feature, c, zr_f, zr_r)
        return remote(
            zs.at[z_peers[i]], zr.at[i], q_send.at[n, i], q_recv.at[n, i], chip(z_peers[i], y, x)
        )

    def stage_core(n, feature, c):
        if not feature:
            e_copy(n, False, c).start()
            return
        k = (1 - core) * nc + c
        for m in range(3):
            rows = pl.ds(m * 256, 256)
            tps[c, rows, :] = dot_nn(gsus[rows, :], wc[k]).astype(BF)
        e_copy(n, True, c).start()
        k = core * nc + c
        for m in range(3):
            rows = pl.ds(m * 256, 256)
            part[c % 2, rows, :] = dot_nn(gsus[rows, :], wc[k])

    def stage_a(n, feature, c):
        e_copy(n, feature, c).wait_recv()
        s = pick(feature, c, s_f, s_r)
        mine = part.at[c % 2] if feature else part_r
        theirs = pick(feature, c, tpr, tpr_r)
        for m in range(3):
            rows = pl.ds(m * 256, 256)
            s[rows, :] = (mine[rows, :].astype(F32) + theirs[rows, :].astype(F32)).astype(BF)
        for i in range(2):
            a_copy(n, feature, c, i).start()

    def stage_b(n, feature, c):
        s, xa = pick(feature, c, s_f, s_r), pick(feature, c, xa_f, xa_r)
        for i in range(2):
            a_copy(n, feature, c, i).wait_recv()
            at = pl.ds(pl.multiple_of(((x + 1 + 2 * i) % 4) * 192 + 96 * i, 96), 96)
            s[at, :] = (s[at, :].astype(F32) + xa[i].astype(F32)).astype(BF)
        for i in range(2):
            b_copy(n, feature, c, i).start()

    def stage_v(n, feature, c):
        s, xb = pick(feature, c, s_f, s_r), pick(feature, c, xb_f, xb_r)
        for i in range(2):
            b_copy(n, feature, c, i).wait_recv()
        at = pl.ds(pl.multiple_of(x * 192, 192), 192)
        s[at, :] = (s[at, :].astype(F32) + xb[0].astype(F32) + xb[1].astype(F32)).astype(BF)
        for i in range(3):
            v_copy(n, feature, c, i).start()

    def stage_q(n, feature, c):
        s, yr = pick(feature, c, s_f, s_r), pick(feature, c, yr_f, yr_r)
        zs = pick(feature, c, zs_f, zs_r)
        for i in range(3):
            v_copy(n, feature, c, i).wait_recv()
        at = pl.ds(pl.multiple_of(block(x, y), BUNDLE), BUNDLE)
        mine = (s[at, :].astype(F32) + yr[0].astype(F32)).astype(BF)
        theirs = (yr[1].astype(F32) + yr[2].astype(F32)).astype(BF)
        slots = jnp.concatenate(
            [mine, theirs, jnp.zeros((128 - 2 * BUNDLE, mine.shape[1]), BF)], axis=0
        )
        if feature:
            rows = dot_nn(place_t[0], slots)
        else:
            lane = lax.broadcasted_iota(jnp.int32, (SIDE * ROWS, 128), 1)
            rows = jnp.where(
                lane == 0,
                dot_nn(place_t[1], slots),
                dot_nn(place_t[2], slots),
            )
        zs[...] = rows.astype(BF).reshape(zs.shape)
        for i in range(3):
            q_copy(n, feature, c, i).start()

    def stage_out(n, feature, c):
        zs, zr = pick(feature, c, zs_f, zs_r), pick(feature, c, zr_f, zr_r)
        for i in range(3):
            q_copy(n, feature, c, i).wait_recv()
        total = zs[z].astype(F32)
        for i in range(3):
            total = total + zr[i].astype(F32)
        if feature:
            out_tok[:, pl.ds(pl.multiple_of(c * LANES, LANES), LANES)] = total[:24].astype(BF)
        else:
            turned = jnp.concatenate([total, jnp.zeros((128 - ROWS, 128), F32)], axis=0).T
            out_rg[...] = turned[0:TOP, 0:rows_dev] / weights[...]

    def out_copies(k):
        at = pl.ds(pl.multiple_of(k * LANES, LANES), LANES)
        return (
            pltpu.make_async_copy(wc.at[k, pl.ds(0, hid)], out_gate.at[0, :, at], o_sem.at[k, 0]),
            pltpu.make_async_copy(wc.at[k, pl.ds(SIDE_HID, hid)], out_up.at[0, :, at], o_sem.at[k, 1]),
            pltpu.make_async_copy(wd.at[k], out_down.at[0, :, at], o_sem.at[k, 2]),
        )

    def weight_grads(k):
        for m in range(3):
            rows = pl.ds(m * 256, 256)
            wc[k, rows, :] = dot_nn(gsus_t[rows, :], xc[k, 0]).astype(BF)
        wd[k] = dot_nn(hid_t[:hid], xc[k, 1]).astype(BF)
        for cp in out_copies(k):
            cp.start()

    stages = (stage_core, stage_a, stage_b, stage_v, stage_q, stage_out)

    def give_back(t, carry):
        for depth, stage in enumerate(stages):
            n = t - depth

            @pl.when(n == 0)
            def _():
                stage(0, False, 0)

            @pl.when((n >= 1) & (n <= nc))
            def _():
                stage(n, True, n - 1)

        @pl.when((t >= 1) & (t <= nc))
        def _():
            weight_grads(core * nc + t - 1)
            weight_grads((1 - core) * nc + t - 1)

        return carry

    lax.fori_loop(0, nc + 1 + len(stages) - 1, give_back, 0)

    for i in range(3):
        zi_copy(i).wait_send()

    def drain_dispatch(c, carry):
        for i in range(3):
            for tensor in range(2):
                z_copy(c, i, tensor).wait_send()
        for i in range(4):
            y_copy(c, i).wait_send()
            p_copy(c, i).wait_send()
        for i in range(8):
            x_copy(c, i).wait_send()
        for tensor in range(2):
            d_copy(c, core * nc + c, tensor).wait_send()
        return carry

    lax.fori_loop(0, nc, drain_dispatch, 0)

    def drain_return(n, feature, c):
        e_copy(n, feature, c).wait_send()
        for i in range(2):
            a_copy(n, feature, c, i).wait_send()
            b_copy(n, feature, c, i).wait_send()
        for i in range(3):
            v_copy(n, feature, c, i).wait_send()
            q_copy(n, feature, c, i).wait_send()

    drain_return(0, False, 0)

    def drain_features(n, carry):
        drain_return(n, True, n - 1)
        return carry

    lax.fori_loop(1, nc + 1, drain_features, 0)

    def drain_outputs(k, carry):
        for cp in out_copies(k):
            cp.wait()
        return carry

    lax.fori_loop(0, 2 * nc, drain_outputs, 0)


def per_device(tokens, cotangent, routes, route_weights, gate_weight, up_weight, down_weight):
    rows, width = tokens.shape
    half = width // lax.axis_size("tp")
    nc = half // LANES
    hid = gate_weight.shape[2]
    vmem, anywhere = pltpu.VMEM, pl.ANY
    slots = 16 * BUNDLE

    def chunk_buffers(lead, lanes):
        return [
            vmem((*lead, slots, lanes), BF),
            vmem((*lead, 2, 96, lanes), BF),
            vmem((*lead, 2, 192, lanes), BF),
            vmem((*lead, 3, BUNDLE, lanes), BF),
            vmem((*lead, SIDE, ROWS, lanes), BF),
            vmem((*lead, 3, ROWS, lanes), BF),
        ]

    dma = pltpu.SemaphoreType.DMA
    token_grad, shares, gate_grad, up_grad, down_grad = pl.pallas_call(
        functools.partial(kernel, nc, hid),
        out_shape=(
            jax.ShapeDtypeStruct((rows, half), BF),
            jax.ShapeDtypeStruct((TOP, rows), F32),
            jax.ShapeDtypeStruct((1, hid, width), BF),
            jax.ShapeDtypeStruct((1, hid, width), BF),
            jax.ShapeDtypeStruct(down_weight.shape, BF),
        ),
        in_specs=[
            pl.BlockSpec(memory_space=anywhere),
            pl.BlockSpec(memory_space=anywhere),
            pl.BlockSpec(memory_space=vmem),
            pl.BlockSpec(memory_space=vmem),
            pl.BlockSpec(memory_space=anywhere),
            pl.BlockSpec(memory_space=anywhere),
            pl.BlockSpec(memory_space=anywhere),
        ],
        out_specs=(
            pl.BlockSpec(memory_space=vmem),
            pl.BlockSpec(memory_space=vmem),
            pl.BlockSpec(memory_space=anywhere),
            pl.BlockSpec(memory_space=anywhere),
            pl.BlockSpec(memory_space=anywhere),
        ),
        scratch_shapes=[
            vmem((nc, SIDE, 2, ROWS, LANES), BF),
            vmem((3, EXPERTS, 128), F32),
            vmem((SIDE, 3, EXPERTS, 128), F32),
            vmem((3, EXPERTS, 128), F32),
            vmem((2 * nc, 2, slots, LANES), BF),
            vmem((nc, 2, BUNDLE, LANES), BF),
            vmem((128, 128), BF),
            vmem((3, 128, 128), BF),
            vmem((2 * BUNDLE, 128), F32),
            vmem((2 * nc, hid, LANES), BF),
            vmem((2 * nc, 2 * SIDE_HID, LANES), BF),
            vmem((slots, 2 * SIDE_HID), F32),
            vmem((slots, SIDE_HID), F32),
            vmem((slots, 2 * SIDE_HID), BF),
            vmem((2 * SIDE_HID, slots), BF),
            vmem((SIDE_HID, slots), BF),
            vmem((2, slots, LANES), F32),
            vmem((nc, slots, LANES), BF),
            vmem((nc, slots, LANES), BF),
            *chunk_buffers((nc,), LANES),
            vmem((slots, 128), BF),
            vmem((slots, 128), BF),
            *chunk_buffers((), 128),
            dma((2 * nc, 3)),
            dma((nc, 2)),
            dma((nc, 3, 2)), dma((nc, 3, 2)),
            dma((3,)), dma((3,)),
            dma((nc, 4)), dma((nc, 4)),
            dma((nc, 8)), dma((nc, 8)),
            dma((nc, 4)), dma((nc, 4)),
            dma((nc, 2)), dma((nc, 2)),
            dma((nc + 1,)), dma((nc + 1,)),
            dma((nc + 1, 2)), dma((nc + 1, 2)),
            dma((nc + 1, 2)), dma((nc + 1, 2)),
            dma((nc + 1, 3)), dma((nc + 1, 3)),
            dma((nc + 1, 3)), dma((nc + 1, 3)),
            dma((2 * nc, 3)),
        ],
        compiler_params=pltpu.CompilerParams(
            collective_id=0, has_side_effects=True, vmem_limit_bytes=63 * 1024 * 1024
        ),
    )(
        tokens, cotangent, routes.T, route_weights.T,
        gate_weight.transpose(0, 2, 1), up_weight.transpose(0, 2, 1), down_weight,
    )
    return token_grad, shares.T, gate_grad.transpose(0, 2, 1), up_grad.transpose(0, 2, 1), down_grad


def solution(mesh):
    return jax.shard_map(
        per_device,
        mesh=mesh,
        in_specs=(
            P("ep", None),
            P("ep", None),
            P("ep", None),
            P("ep", None),
            P("ep", None, "tp"),
            P("ep", None, "tp"),
            P("ep", "tp", None),
        ),
        out_specs=(
            P("ep", "tp"),
            P("ep", None),
            P("ep", None, "tp"),
            P("ep", None, "tp"),
            P("ep", "tp", None),
        ),
        check_vma=False,
    )
```

```python
import functools

import jax
import jax.numpy as jnp
from jax import lax
from jax.experimental import pallas as pl
from jax.experimental.pallas import tpu as pltpu
from jax.sharding import PartitionSpec as P

EXPERTS = 8
TOP = 2
CAP = 12
SIDE = 4
ROWS = 32
BUNDLE = 48
LANES = 256
AHEAD = 3
SIDE_HID = 384
BF = jnp.bfloat16
F32 = jnp.float32
MESH = pl.DeviceIdType.MESH


def dot_nt(a, b):
    return lax.dot_general(a, b, (((1,), (1,)), ((), ())), preferred_element_type=F32)


def dot_tn(a, b):
    return lax.dot_general(a, b, (((0,), (0,)), ((), ())), preferred_element_type=F32)


def dot_nn(a, b):
    return jnp.dot(a, b, preferred_element_type=F32)


def kernel(
    nc, hid,
    tokens, cotangent, routes, weights, gate, up, down,
    out_tok, out_rg, out_gate, out_up, out_down,
    tz, info, iz, codes, xc, ob, place, place_t, share,
    wd, wc, pre, hg, gsus, gsus_t, hid_t,
    s_f, tpr, xa_f, xb_f, yr_f, zs_f, zr_f,
    part_r, tpr_r, s_r, xa_r, xb_r, yr_r, zs_r, zr_r,
    w_sem, z_send, z_recv, i_send, i_recv, y_send, y_recv, x_send, x_recv, p_send, p_recv, d_send, d_recv,
    e_send, e_recv, a_send, a_recv, b_send, b_recv, v_send, v_recv, q_send, q_recv,
    o_sem,
):
    ep = lax.axis_index("ep")
    core = lax.axis_index("tp")
    z, y, x = ep // 16, (ep // 4) % 4, ep % 4
    pair = y // 2

    def chip(zz, yy, xx):
        return (zz * 16 + yy * 4 + xx, core)

    right = chip(z, y, (x + 1) % 4)
    left = chip(z, y, (x + 3) % 4)
    other_core = (ep, 1 - core)
    partner_y = 2 * pair + (1 - y % 2)
    cross_y = 3 - y
    cross2_y = 2 * (1 - pair) + y % 2
    y_peers = [partner_y, cross_y, cross2_y]
    z_peers = [(z + 1) % 4, (z + 3) % 4, (z + 2) % 4]

    rows_dev = tokens.shape[0]
    half_of = ((y + 1) // 2) % 2

    def block(xs, ys):
        return xs * 192 + (((ys + 1) // 2) % 2) * 96 + (ys // 2) * BUNDLE

    def pad_rows(c, carry):
        tz[c, :, :, rows_dev:, :] = jnp.zeros((SIDE, 2, ROWS - rows_dev, LANES), BF)
        return carry

    lax.fori_loop(0, nc, pad_rows, 0)

    barrier = pltpu.get_barrier_semaphore()
    for zz in z_peers:
        pl.semaphore_signal(barrier, inc=1, device_id=chip(zz, y, x), device_id_type=MESH)
    for yy in y_peers:
        pl.semaphore_signal(barrier, inc=1, device_id=chip(z, yy, x), device_id_type=MESH)
    for dev in (right, left, other_core):
        pl.semaphore_signal(barrier, inc=1, device_id=dev, device_id_type=MESH)

    w_copies = []
    for k in range(2 * nc):
        at = pl.ds(k * LANES, LANES)
        w_copies += [
            pltpu.make_async_copy(gate.at[0, :, at], wc.at[k, pl.ds(0, hid)], w_sem.at[0]),
            pltpu.make_async_copy(up.at[0, :, at], wc.at[k, pl.ds(SIDE_HID, hid)], w_sem.at[1]),
            pltpu.make_async_copy(down.at[0, :, at], wd.at[k], w_sem.at[2]),
        ]
    for cp in w_copies:
        cp.start()

    pl.semaphore_wait(barrier, 9)

    def remote(a, b, ss, rs, dev):
        return pltpu.make_async_remote_copy(
            src_ref=a, dst_ref=b, send_sem=ss, recv_sem=rs, device_id=dev, device_id_type=MESH
        )

    def settle(ref, sem):
        pltpu.make_async_copy(ref, ref, sem).wait()

    def some(n):
        return xc.at[0, 0, pl.ds(0, n)]

    def piece(ref, c):
        return ref.at[:, pl.ds(pl.multiple_of((core * nc + c) * LANES, LANES), LANES)]

    def landing(c, tensor):
        return tz.at[c, z, tensor, pl.ds(0, rows_dev)]

    def z_copy(c, i, tensor):
        return remote(
            piece(cotangent if tensor else tokens, c), landing(c, tensor),
            z_send.at[0], z_recv.at[c], chip(z_peers[i], y, x),
        )

    def own_copy(c, tensor):
        return pltpu.make_async_copy(
            piece(cotangent if tensor else tokens, c), landing(c, tensor), z_recv.at[c]
        )

    def zi_copy(i):
        return remote(info, iz.at[z], i_send.at[0], i_recv.at[0], chip(z_peers[i], y, x))

    def start_z(c):
        for tensor in range(2):
            for i in range(3):
                z_copy(c, i, tensor).start()
            own_copy(c, tensor).start()

    start_z(0)

    expert_row = lax.broadcasted_iota(jnp.int32, (EXPERTS, rows_dev), 0)
    hot = [expert_row == routes[k:k + 1, :] for k in range(2)]
    hit = jnp.where(hot[0] | hot[1], 1.0, 0.0).astype(BF)
    before = jnp.where(
        lax.broadcasted_iota(jnp.int32, (rows_dev, rows_dev), 0)
        < lax.broadcasted_iota(jnp.int32, (rows_dev, rows_dev), 1),
        1.0, 0.0,
    ).astype(BF)
    code = dot_nn(hit, before) + (z * CAP + 1).astype(F32)
    info[...] = jnp.zeros_like(info)
    for k in range(2):
        info[k, :, 0:rows_dev] = jnp.where(hot[k], code, 0.0)
    info[2, :, 0:rows_dev] = jnp.where(hot[0], weights[0:1, :], 0.0) + jnp.where(
        hot[1], weights[1:2, :], 0.0
    )
    for i in range(3):
        zi_copy(i).start()
    for c in range(1, AHEAD):
        start_z(c)
    iz[z] = info[...]
    pre[...] = jnp.zeros_like(pre)
    hg[...] = jnp.zeros_like(hg)
    settle(iz.at[pl.ds(0, 3)], i_recv.at[0])
    for kind in range(3):
        total = iz[0, kind]
        for zz in range(1, SIDE):
            total = total + pltpu.roll(iz[zz, kind], zz * ROWS, 1)
        codes[kind] = total

    slot_number = lax.broadcasted_iota(jnp.int32, (BUNDLE, 128), 0).astype(F32) + 1.0

    def info_row(kind, expert):
        return codes[kind, pl.ds(expert, 1), :]

    spare = jnp.zeros((128 - 2 * BUNDLE, 128), F32)
    first, second = [], []
    for side, expert in ((0, 2 * z + pair), (1, 2 * z + 1 - pair)):
        first.append(jnp.where(slot_number == info_row(0, expert), 1.0, 0.0))
        second.append(jnp.where(slot_number == info_row(1, expert), 1.0, 0.0))
        share[side * BUNDLE:(side + 1) * BUNDLE, :] = jnp.broadcast_to(
            jnp.sum((first[side] + second[side]) * info_row(2, expert), axis=1, keepdims=True),
            (BUNDLE, 128),
        )
    first = jnp.concatenate(first + [spare], axis=0)
    second = jnp.concatenate(second + [spare], axis=0)
    place[...] = (first + second).astype(BF)
    place_t[0] = (first + second).T.astype(BF)
    place_t[1] = first.T.astype(BF)
    place_t[2] = second.T.astype(BF)

    def y_copy(c, i):
        k = core * nc + c
        at = pl.ds(block(x, y), BUNDLE)
        tensor = 1 if i == 3 else 0
        peer = cross_y if i == 3 else y_peers[i]
        from_ref = xc.at[k, 0, at, :] if i == 0 else ob.at[c, tensor]
        return remote(
            from_ref, xc.at[k, tensor, at, :], y_send.at[0], y_recv.at[c, tensor], chip(z, peer, x)
        )

    def x_copy(c, i):
        k = core * nc + c
        tensor = i // 4
        step = i % 4
        size, base = (96, half_of * 96) if tensor else (192, 0)
        if step < 2:
            at = pl.ds(x * 192 + base, size)
        elif step == 2:
            at = pl.ds(((x + 3) % 4) * 192 + base, size // 2)
        else:
            at = pl.ds(((x + 1) % 4) * 192 + base + size // 2, size // 2)
        ref = xc.at[k, tensor, at, :]
        return remote(
            ref, ref, x_send.at[i // 2], x_recv.at[c, i // 2], right if i % 2 == 0 else left
        )

    def p_copy(c, i):
        at = pl.ds(((x + (0, 3, 1, 2)[i]) % 4) * 192 + half_of * 96, 96)
        ref = xc.at[core * nc + c, 1, at, :]
        return remote(ref, ref, p_send.at[0], p_recv.at[c], chip(z, partner_y, x))

    def d_copy(c, k, tensor):
        ref = xc.at[k, tensor]
        return remote(ref, ref, d_send.at[0], d_recv.at[c], other_core)

    def compact(c):
        settle(some(8 * rows_dev), z_recv.at[c])

        @pl.when(c + AHEAD < nc)
        def _():
            start_z(c + AHEAD)

        k = core * nc + c
        at = pl.ds(pl.multiple_of(block(x, y), BUNDLE), BUNDLE)
        for tensor in (1, 0):
            rows = dot_nn(place[:2 * BUNDLE], tz[c, :, tensor].reshape(SIDE * ROWS, LANES))
            if tensor == 1:
                rows = rows * share[:, 0:1]
            rows = rows.astype(BF)
            xc[k, tensor, at, :] = rows[:BUNDLE]
            ob[c, tensor] = rows[BUNDLE:]
            for i in ((3,) if tensor else (0, 1, 2)):
                y_copy(c, i).start()

    def products(k):
        for m in range(3):
            rows = pl.ds(m * 256, 256)
            pre[rows, :] += dot_nt(xc[k, 0, rows, :], wc[k])
            hg[rows, :hid] += dot_nt(xc[k, 1, rows, :], wd[k])

    def blank(k, carry):
        for at in (hid, SIDE_HID + hid):
            wc[k, at:at + SIDE_HID - hid, :] = jnp.zeros((SIDE_HID - hid, LANES), BF)
        return carry

    lax.fori_loop(0, 2 * nc, blank, 0)

    def dispatch(t, carry):
        @pl.when(t < nc)
        def _():
            compact(t)

        @pl.when((t >= 1) & (t < nc + 1))
        def _():
            c = t - 1
            settle(some(BUNDLE), y_recv.at[c, 1])
            x_copy(c, 4).start()
            x_copy(c, 5).start()
            p_copy(c, 0).start()
            settle(some(3 * BUNDLE), y_recv.at[c, 0])
            x_copy(c, 0).start()
            x_copy(c, 1).start()

        @pl.when(t == 1)
        def _():
            settle(gate.at[0], w_sem.at[0])
            settle(up.at[0], w_sem.at[1])
            settle(down.at[0], w_sem.at[2])

        @pl.when((t >= 2) & (t < nc + 2))
        def _():
            c = t - 2
            settle(some(192), x_recv.at[c, 2])
            for side in range(2):
                x_copy(c, 6 + side).start()
                p_copy(c, 1 + side).start()
            settle(some(384), x_recv.at[c, 0])
            for side in range(2):
                x_copy(c, 2 + side).start()

        @pl.when((t >= 3) & (t < nc + 3))
        def _():
            c = t - 3
            settle(some(96), x_recv.at[c, 3])
            p_copy(c, 3).start()
            settle(some(192), x_recv.at[c, 1])
            d_copy(c, core * nc + c, 0).start()

        @pl.when((t >= 4) & (t < nc + 4))
        def _():
            c = t - 4
            settle(some(384), p_recv.at[c])
            d_copy(c, core * nc + c, 1).start()
            products(core * nc + c)

        @pl.when(t >= 5)
        def _():
            c = t - 5
            settle(xc.at[0], d_recv.at[c])
            products((1 - core) * nc + c)

        return carry

    lax.fori_loop(0, nc + 5, dispatch, 0)

    def gates(m, carry):
        rows = pl.ds(pl.multiple_of(m * 128, 128), 128)
        value = jnp.zeros((128, 1), F32)
        for at in range(0, SIDE_HID, 128):
            g = pre[rows, at:at + 128]
            u = pre[rows, SIDE_HID + at:SIDE_HID + at + 128]
            h = hg[rows, at:at + 128]
            s = jax.nn.sigmoid(g)
            active = g * s
            hidden = (active * u).astype(BF).astype(F32)
            g_side = h * u * (s * (1.0 + g * (1.0 - s)))
            u_side = h * active
            value = value + jnp.sum(hidden * h, axis=1, keepdims=True)
            gsus[rows, at:at + 128] = g_side.astype(BF)
            gsus[rows, SIDE_HID + at:SIDE_HID + at + 128] = u_side.astype(BF)
            hid_t[at:at + 128, rows] = hidden.T.astype(BF)
            gsus_t[at:at + 128, rows] = g_side.T.astype(BF)
            gsus_t[SIDE_HID + at:SIDE_HID + at + 128, rows] = u_side.T.astype(BF)
        part_r[rows, :] = jnp.broadcast_to(value, (128, 128)).astype(BF)
        return carry

    lax.fori_loop(0, 6, gates, 0)

    def e_copy(n, feature, c):
        if feature:
            return remote(s_f.at[c], tpr.at[c], e_send.at[n], e_recv.at[n], other_core)
        return remote(part_r, tpr_r, e_send.at[n], e_recv.at[n], other_core)

    def pick(feature, c, f_ref, r_ref):
        return f_ref.at[c] if feature else r_ref

    def a_copy(n, feature, c, i):
        s, xa = pick(feature, c, s_f, s_r), pick(feature, c, xa_f, xa_r)
        at = pl.ds(((x + 2) % 4) * 192 + 96 * i, 96)
        return remote(
            s.at[at], xa.at[i], a_send.at[int(feature)], a_recv.at[n], right if i == 0 else left
        )

    def b_copy(n, feature, c, i):
        s, xb = pick(feature, c, s_f, s_r), pick(feature, c, xb_f, xb_r)
        at = pl.ds(((x + 1 + 2 * i) % 4) * 192, 192)
        return remote(
            s.at[at], xb.at[i], b_send.at[int(feature)], b_recv.at[n], right if i == 0 else left
        )

    def v_copy(n, feature, c, i):
        s, yr = pick(feature, c, s_f, s_r), pick(feature, c, yr_f, yr_r)
        at = pl.ds(block(x, y_peers[i]), BUNDLE)
        return remote(
            s.at[at], yr.at[i], v_send.at[int(feature)], v_recv.at[n], chip(z, y_peers[i], x)
        )

    def q_copy(n, feature, c, i):
        zs, zr = pick(feature, c, zs_f, zs_r), pick(feature, c, zr_f, zr_r)
        return remote(
            zs.at[z_peers[i]], zr.at[i], q_send.at[int(feature)], q_recv.at[n], chip(z_peers[i], y, x)
        )

    def half_lanes(c):
        return pl.ds(pl.multiple_of((c % 2) * LANES, LANES), LANES)

    def stage_core(n, feature, c):
        if not feature:
            e_copy(n, False, c).start()
            return
        k = (1 - core) * nc + c
        for m in range(3):
            rows = pl.ds(m * 256, 256)
            s_f[c, rows, :] = dot_nn(gsus[rows, :], wc[k]).astype(BF)
        e_copy(n, True, c).start()
        k = core * nc + c
        for m in range(3):
            rows = pl.ds(m * 256, 256)
            pre[rows, half_lanes(c)] = dot_nn(gsus[rows, :], wc[k])

    def stage_a(n, feature, c):
        e_copy(n, feature, c).wait()
        s = pick(feature, c, s_f, s_r)
        theirs = pick(feature, c, tpr, tpr_r)
        for m in range(3):
            rows = pl.ds(m * 256, 256)
            mine = pre[rows, half_lanes(c)] if feature else part_r[rows, :].astype(F32)
            s[rows, :] = (mine + theirs[rows, :].astype(F32)).astype(BF)
        for i in range(2):
            a_copy(n, feature, c, i).start()

    def stage_b(n, feature, c):
        s, xa = pick(feature, c, s_f, s_r), pick(feature, c, xa_f, xa_r)
        settle(xa, a_recv.at[n])
        for i in range(2):
            at = pl.ds(pl.multiple_of(((x + 1 + 2 * i) % 4) * 192 + 96 * i, 96), 96)
            s[at, :] = (s[at, :].astype(F32) + xa[i].astype(F32)).astype(BF)
        for i in range(2):
            b_copy(n, feature, c, i).start()

    def stage_v(n, feature, c):
        s, xb = pick(feature, c, s_f, s_r), pick(feature, c, xb_f, xb_r)
        settle(xb, b_recv.at[n])
        at = pl.ds(pl.multiple_of(x * 192, 192), 192)
        s[at, :] = (s[at, :].astype(F32) + xb[0].astype(F32) + xb[1].astype(F32)).astype(BF)
        for i in range(3):
            v_copy(n, feature, c, i).start()

    def stage_q(n, feature, c):
        s, yr = pick(feature, c, s_f, s_r), pick(feature, c, yr_f, yr_r)
        zs = pick(feature, c, zs_f, zs_r)
        settle(yr, v_recv.at[n])
        at = pl.ds(pl.multiple_of(block(x, y), BUNDLE), BUNDLE)
        mine = (s[at, :].astype(F32) + yr[0].astype(F32)).astype(BF)
        theirs = (yr[1].astype(F32) + yr[2].astype(F32)).astype(BF)
        slots = jnp.concatenate(
            [mine, theirs, jnp.zeros((128 - 2 * BUNDLE, mine.shape[1]), BF)], axis=0
        )
        if feature:
            rows = dot_nn(place_t[0], slots)
        else:
            lane = lax.broadcasted_iota(jnp.int32, (SIDE * ROWS, 128), 1)
            rows = jnp.where(
                lane == 0,
                dot_nn(place_t[1], slots),
                dot_nn(place_t[2], slots),
            )
        zs[...] = rows.astype(BF).reshape(zs.shape)
        for i in range(3):
            q_copy(n, feature, c, i).start()

    def stage_out(n, feature, c):
        zs, zr = pick(feature, c, zs_f, zs_r), pick(feature, c, zr_f, zr_r)
        settle(zr, q_recv.at[n])
        total = zs[z].astype(F32)
        for i in range(3):
            total = total + zr[i].astype(F32)
        if feature:
            out_tok[:, pl.ds(pl.multiple_of(c * LANES, LANES), LANES)] = total[:24].astype(BF)
        else:
            turned = jnp.concatenate([total, jnp.zeros((128 - ROWS, 128), F32)], axis=0).T
            out_rg[...] = turned[0:TOP, 0:rows_dev] / weights[...]

    def out_copies(k):
        at = pl.ds(pl.multiple_of(k * LANES, LANES), LANES)
        return (
            pltpu.make_async_copy(wc.at[k, pl.ds(0, hid)], out_gate.at[0, :, at], o_sem.at[0]),
            pltpu.make_async_copy(wc.at[k, pl.ds(SIDE_HID, hid)], out_up.at[0, :, at], o_sem.at[1]),
            pltpu.make_async_copy(wd.at[k], out_down.at[0, :, at], o_sem.at[2]),
        )

    def weight_grads(k):
        for m in range(3):
            rows = pl.ds(m * 256, 256)
            wc[k, rows, :] = dot_nn(gsus_t[rows, :], xc[k, 0]).astype(BF)
        wd[k] = dot_nn(hid_t[:hid], xc[k, 1]).astype(BF)
        for cp in out_copies(k):
            cp.start()

    stages = (stage_core, stage_a, stage_b, stage_v, stage_q, stage_out)

    def give_back(t, carry):
        for depth, stage in enumerate(stages):
            n = t - depth

            @pl.when(n == 0)
            def _():
                stage(0, False, 0)

            @pl.when((n >= 1) & (n <= nc))
            def _():
                stage(n, True, n - 1)

        @pl.when((t >= 1) & (t <= nc))
        def _():
            weight_grads(core * nc + t - 1)
            weight_grads((1 - core) * nc + t - 1)

        return carry

    lax.fori_loop(0, nc + 1 + len(stages) - 1, give_back, 0)

    settle(iz.at[pl.ds(0, 3)], i_send.at[0])
    settle(xc.at[0, :, pl.ds(0, 3 * rows_dev * nc)], z_send.at[0])
    settle(xc.at[0], y_send.at[0])
    settle(xc.at[pl.ds(0, 2)], x_send.at[0])
    settle(xc.at[0], x_send.at[1])
    settle(xc.at[0], x_send.at[2])
    settle(xc.at[0, 0], x_send.at[3])
    settle(xc.at[pl.ds(0, 2)], p_send.at[0])
    settle(xc.at[pl.ds(0, nc)], d_send.at[0])
    for sem, ref_r, ref_f in (
        (a_send, xa_r, xa_f), (b_send, xb_r, xb_f), (v_send, yr_r, yr_f), (q_send, zr_r, zr_f)
    ):
        settle(ref_r, sem.at[0])
        settle(ref_f, sem.at[1])
    settle(out_gate.at[0], o_sem.at[0])
    settle(out_up.at[0], o_sem.at[1])
    settle(out_down.at[0], o_sem.at[2])


def per_device(tokens, cotangent, routes, route_weights, gate_weight, up_weight, down_weight):
    rows, width = tokens.shape
    half = width // lax.axis_size("tp")
    nc = half // LANES
    hid = gate_weight.shape[2]
    vmem, anywhere = pltpu.VMEM, pl.ANY
    slots = 16 * BUNDLE

    def chunk_buffers(lead, lanes):
        return [
            vmem((*lead, slots, lanes), BF),
            vmem((*lead, 2, 96, lanes), BF),
            vmem((*lead, 2, 192, lanes), BF),
            vmem((*lead, 3, BUNDLE, lanes), BF),
            vmem((*lead, SIDE, ROWS, lanes), BF),
            vmem((*lead, 3, ROWS, lanes), BF),
        ]

    dma = pltpu.SemaphoreType.DMA
    token_grad, shares, gate_grad, up_grad, down_grad = pl.pallas_call(
        functools.partial(kernel, nc, hid),
        out_shape=(
            jax.ShapeDtypeStruct((rows, half), BF),
            jax.ShapeDtypeStruct((TOP, rows), F32),
            jax.ShapeDtypeStruct((1, hid, width), BF),
            jax.ShapeDtypeStruct((1, hid, width), BF),
            jax.ShapeDtypeStruct(down_weight.shape, BF),
        ),
        in_specs=[
            pl.BlockSpec(memory_space=anywhere),
            pl.BlockSpec(memory_space=anywhere),
            pl.BlockSpec(memory_space=vmem),
            pl.BlockSpec(memory_space=vmem),
            pl.BlockSpec(memory_space=anywhere),
            pl.BlockSpec(memory_space=anywhere),
            pl.BlockSpec(memory_space=anywhere),
        ],
        out_specs=(
            pl.BlockSpec(memory_space=vmem),
            pl.BlockSpec(memory_space=vmem),
            pl.BlockSpec(memory_space=anywhere),
            pl.BlockSpec(memory_space=anywhere),
            pl.BlockSpec(memory_space=anywhere),
        ),
        scratch_shapes=[
            vmem((nc, SIDE, 2, ROWS, LANES), BF),
            vmem((3, EXPERTS, 128), F32),
            vmem((SIDE, 3, EXPERTS, 128), F32),
            vmem((3, EXPERTS, 128), F32),
            vmem((2 * nc, 2, slots, LANES), BF),
            vmem((nc, 2, BUNDLE, LANES), BF),
            vmem((128, 128), BF),
            vmem((3, 128, 128), BF),
            vmem((2 * BUNDLE, 128), F32),
            vmem((2 * nc, hid, LANES), BF),
            vmem((2 * nc, 2 * SIDE_HID, LANES), BF),
            vmem((slots, 2 * SIDE_HID), F32),
            vmem((slots, SIDE_HID), F32),
            vmem((slots, 2 * SIDE_HID), BF),
            vmem((2 * SIDE_HID, slots), BF),
            vmem((SIDE_HID, slots), BF),
            vmem((nc, slots, LANES), BF),
            vmem((nc, slots, LANES), BF),
            *chunk_buffers((nc,), LANES)[1:],
            vmem((slots, 128), BF),
            vmem((slots, 128), BF),
            *chunk_buffers((), 128),
            dma((3,)),
            dma((1,)), dma((nc,)),
            dma((1,)), dma((1,)),
            dma((1,)), dma((nc, 2)),
            dma((4,)), dma((nc, 4)),
            dma((1,)), dma((nc,)),
            dma((1,)), dma((nc,)),
            dma((nc + 1,)), dma((nc + 1,)),
            dma((2,)), dma((nc + 1,)),
            dma((2,)), dma((nc + 1,)),
            dma((2,)), dma((nc + 1,)),
            dma((2,)), dma((nc + 1,)),
            dma((3,)),
        ],
        compiler_params=pltpu.CompilerParams(
            collective_id=0, has_side_effects=True, vmem_limit_bytes=43 * 1024 * 1024
        ),
    )(
        tokens, cotangent, routes.T, route_weights.T,
        gate_weight.transpose(0, 2, 1), up_weight.transpose(0, 2, 1), down_weight,
    )
    return token_grad, shares.T, gate_grad.transpose(0, 2, 1), up_grad.transpose(0, 2, 1), down_grad


def solution(mesh):
    return jax.shard_map(
        per_device,
        mesh=mesh,
        in_specs=(
            P("ep", None),
            P("ep", None),
            P("ep", None),
            P("ep", None),
            P("ep", None, "tp"),
            P("ep", None, "tp"),
            P("ep", "tp", None),
        ),
        out_specs=(
            P("ep", "tp"),
            P("ep", None),
            P("ep", None, "tp"),
            P("ep", None, "tp"),
            P("ep", "tp", None),
        ),
        check_vma=False,
    )
```

```python
import functools

import jax
import jax.numpy as jnp
from jax import lax
from jax.experimental import pallas as pl
from jax.experimental.pallas import tpu as pltpu
from jax.sharding import PartitionSpec as P

EXPERTS = 8
TOP = 2
CAP = 12
SIDE = 4
ROWS = 32
BUNDLE = 48
LANES = 256
AHEAD = 3
AT = (1, 2, 3, 4, 5)
BACK_AT = (0, 1, 3, 5, 7, 9)
GRADS_AT = 5
SIDE_HID = 384
BF = jnp.bfloat16
F32 = jnp.float32
MESH = pl.DeviceIdType.MESH


def dot_nt(a, b):
    return lax.dot_general(a, b, (((1,), (1,)), ((), ())), preferred_element_type=F32)


def dot_tn(a, b):
    return lax.dot_general(a, b, (((0,), (0,)), ((), ())), preferred_element_type=F32)


def dot_nn(a, b):
    return jnp.dot(a, b, preferred_element_type=F32)


def kernel(
    nc, hid,
    tokens, cotangent, routes, weights, gate, up, down,
    out_tok, out_rg, out_gate, out_up, out_down,
    tz, info, iz, codes, xc, ob, place, place_t, share,
    wd, wc, pre, hg, gsus, gsus_t, hid_t,
    s_f, tpr, xa_f, xb_f, yr_f, zs_f, zr_f,
    part_r, tpr_r, s_r, xa_r, xb_r, yr_r, zs_r, zr_r,
    w_sem, z_send, z_recv, i_send, i_recv, y_send, y_recv, x_send, x_recv, p_send, p_recv, d_send, d_recv,
    e_send, e_recv, a_send, a_recv, b_send, b_recv, v_send, v_recv, q_send, q_recv,
    o_sem,
):
    ep = lax.axis_index("ep")
    core = lax.axis_index("tp")
    z, y, x = ep // 16, (ep // 4) % 4, ep % 4
    pair = y // 2

    def chip(zz, yy, xx):
        return (zz * 16 + yy * 4 + xx, core)

    right = chip(z, y, (x + 1) % 4)
    left = chip(z, y, (x + 3) % 4)
    other_core = (ep, 1 - core)
    partner_y = 2 * pair + (1 - y % 2)
    cross_y = 3 - y
    cross2_y = 2 * (1 - pair) + y % 2
    y_peers = [partner_y, cross_y, cross2_y]
    z_peers = [(z + 1) % 4, (z + 3) % 4, (z + 2) % 4]

    rows_dev = tokens.shape[0]
    half_of = ((y + 1) // 2) % 2

    def block(xs, ys):
        return xs * 192 + (((ys + 1) // 2) % 2) * 96 + (ys // 2) * BUNDLE

    def pad_rows(c, carry):
        tz[c, :, :, rows_dev:, :] = jnp.zeros((SIDE, 2, ROWS - rows_dev, LANES), BF)
        return carry

    lax.fori_loop(0, nc, pad_rows, 0)

    barrier = pltpu.get_barrier_semaphore()
    for zz in z_peers:
        pl.semaphore_signal(barrier, inc=1, device_id=chip(zz, y, x), device_id_type=MESH)
    for yy in y_peers:
        pl.semaphore_signal(barrier, inc=1, device_id=chip(z, yy, x), device_id_type=MESH)
    for dev in (right, left, other_core):
        pl.semaphore_signal(barrier, inc=1, device_id=dev, device_id_type=MESH)

    w_copies = []
    for k in range(2 * nc):
        at = pl.ds(k * LANES, LANES)
        w_copies += [
            pltpu.make_async_copy(gate.at[0, :, at], wc.at[k, pl.ds(0, hid)], w_sem.at[0]),
            pltpu.make_async_copy(up.at[0, :, at], wc.at[k, pl.ds(SIDE_HID, hid)], w_sem.at[1]),
            pltpu.make_async_copy(down.at[0, :, at], wd.at[k], w_sem.at[2]),
        ]
    for cp in w_copies:
        cp.start()

    pl.semaphore_wait(barrier, 9)

    def remote(a, b, ss, rs, dev):
        return pltpu.make_async_remote_copy(
            src_ref=a, dst_ref=b, send_sem=ss, recv_sem=rs, device_id=dev, device_id_type=MESH
        )

    def settle(ref, sem):
        pltpu.make_async_copy(ref, ref, sem).wait()

    def some(n):
        return xc.at[0, 0, pl.ds(0, n)]

    def piece(ref, c):
        return ref.at[:, pl.ds(pl.multiple_of((core * nc + c) * LANES, LANES), LANES)]

    def landing(c, tensor):
        return tz.at[c, z, tensor, pl.ds(0, rows_dev)]

    def z_copy(c, i, tensor):
        return remote(
            piece(cotangent if tensor else tokens, c), landing(c, tensor),
            z_send.at[0], z_recv.at[c], chip(z_peers[i], y, x),
        )

    def own_copy(c, tensor):
        return pltpu.make_async_copy(
            piece(cotangent if tensor else tokens, c), landing(c, tensor), z_recv.at[c]
        )

    def zi_copy(i):
        return remote(info, iz.at[z], i_send.at[0], i_recv.at[0], chip(z_peers[i], y, x))

    def start_z(c):
        for tensor in range(2):
            for i in range(3):
                z_copy(c, i, tensor).start()
            own_copy(c, tensor).start()

    start_z(0)

    expert_row = lax.broadcasted_iota(jnp.int32, (EXPERTS, rows_dev), 0)
    hot = [expert_row == routes[k:k + 1, :] for k in range(2)]
    hit = jnp.where(hot[0] | hot[1], 1.0, 0.0).astype(BF)
    before = jnp.where(
        lax.broadcasted_iota(jnp.int32, (rows_dev, rows_dev), 0)
        < lax.broadcasted_iota(jnp.int32, (rows_dev, rows_dev), 1),
        1.0, 0.0,
    ).astype(BF)
    code = dot_nn(hit, before) + (z * CAP + 1).astype(F32)
    info[...] = jnp.zeros_like(info)
    for k in range(2):
        info[k, :, 0:rows_dev] = jnp.where(hot[k], code, 0.0)
    info[2, :, 0:rows_dev] = jnp.where(hot[0], weights[0:1, :], 0.0) + jnp.where(
        hot[1], weights[1:2, :], 0.0
    )
    for i in range(3):
        zi_copy(i).start()
    for c in range(1, AHEAD):
        start_z(c)
    iz[z] = info[...]
    pre[...] = jnp.zeros_like(pre)
    hg[...] = jnp.zeros_like(hg)
    settle(iz.at[pl.ds(0, 3)], i_recv.at[0])
    for kind in range(3):
        total = iz[0, kind]
        for zz in range(1, SIDE):
            total = total + pltpu.roll(iz[zz, kind], zz * ROWS, 1)
        codes[kind] = total

    slot_number = lax.broadcasted_iota(jnp.int32, (BUNDLE, 128), 0).astype(F32) + 1.0

    def info_row(kind, expert):
        return codes[kind, pl.ds(expert, 1), :]

    spare = jnp.zeros((128 - 2 * BUNDLE, 128), F32)
    first, second = [], []
    for side, expert in ((0, 2 * z + pair), (1, 2 * z + 1 - pair)):
        first.append(jnp.where(slot_number == info_row(0, expert), 1.0, 0.0))
        second.append(jnp.where(slot_number == info_row(1, expert), 1.0, 0.0))
        share[side * BUNDLE:(side + 1) * BUNDLE, :] = jnp.broadcast_to(
            jnp.sum((first[side] + second[side]) * info_row(2, expert), axis=1, keepdims=True),
            (BUNDLE, 128),
        )
    first = jnp.concatenate(first + [spare], axis=0)
    second = jnp.concatenate(second + [spare], axis=0)
    place[...] = (first + second).astype(BF)
    place_t[0] = (first + second).T.astype(BF)
    place_t[1] = first.T.astype(BF)
    place_t[2] = second.T.astype(BF)

    def y_copy(c, i):
        k = core * nc + c
        at = pl.ds(block(x, y), BUNDLE)
        tensor = 1 if i == 3 else 0
        peer = cross_y if i == 3 else y_peers[i]
        from_ref = xc.at[k, 0, at, :] if i == 0 else ob.at[c, tensor]
        return remote(
            from_ref, xc.at[k, tensor, at, :], y_send.at[0], y_recv.at[c, tensor], chip(z, peer, x)
        )

    def x_copy(c, i):
        k = core * nc + c
        tensor = i // 4
        step = i % 4
        size, base = (96, half_of * 96) if tensor else (192, 0)
        if step < 2:
            at = pl.ds(x * 192 + base, size)
        elif step == 2:
            at = pl.ds(((x + 3) % 4) * 192 + base, size // 2)
        else:
            at = pl.ds(((x + 1) % 4) * 192 + base + size // 2, size // 2)
        ref = xc.at[k, tensor, at, :]
        return remote(
            ref, ref, x_send.at[i // 2], x_recv.at[c, i // 2], right if i % 2 == 0 else left
        )

    def p_copy(c, i):
        at = pl.ds(((x + (0, 3, 1, 2)[i]) % 4) * 192 + half_of * 96, 96)
        ref = xc.at[core * nc + c, 1, at, :]
        return remote(ref, ref, p_send.at[0], p_recv.at[c], chip(z, partner_y, x))

    def d_copy(c, k, tensor):
        ref = xc.at[k, tensor]
        return remote(ref, ref, d_send.at[0], d_recv.at[c], other_core)

    def compact(c):
        settle(some(8 * rows_dev), z_recv.at[c])

        @pl.when(c + AHEAD < nc)
        def _():
            start_z(c + AHEAD)

        k = core * nc + c
        at = pl.ds(pl.multiple_of(block(x, y), BUNDLE), BUNDLE)
        for tensor in (1, 0):
            rows = dot_nn(place[:2 * BUNDLE], tz[c, :, tensor].reshape(SIDE * ROWS, LANES))
            if tensor == 1:
                rows = rows * share[:, 0:1]
            rows = rows.astype(BF)
            xc[k, tensor, at, :] = rows[:BUNDLE]
            ob[c, tensor] = rows[BUNDLE:]
            for i in ((3,) if tensor else (0, 1, 2)):
                y_copy(c, i).start()

    def products(k):
        for m in range(3):
            rows = pl.ds(m * 256, 256)
            pre[rows, :] += dot_nt(xc[k, 0, rows, :], wc[k])
            hg[rows, :hid] += dot_nt(xc[k, 1, rows, :], wd[k])

    def blank(k, carry):
        for at in (hid, SIDE_HID + hid):
            wc[k, at:at + SIDE_HID - hid, :] = jnp.zeros((SIDE_HID - hid, LANES), BF)
        return carry

    lax.fori_loop(0, 2 * nc, blank, 0)

    def dispatch(t, carry):
        @pl.when(t < nc)
        def _():
            compact(t)

        @pl.when((t >= AT[0]) & (t < nc + AT[0]))
        def _():
            c = t - AT[0]
            settle(some(BUNDLE), y_recv.at[c, 1])
            x_copy(c, 4).start()
            x_copy(c, 5).start()
            p_copy(c, 0).start()
            settle(some(3 * BUNDLE), y_recv.at[c, 0])
            x_copy(c, 0).start()
            x_copy(c, 1).start()

        @pl.when(t == 1)
        def _():
            settle(gate.at[0], w_sem.at[0])
            settle(up.at[0], w_sem.at[1])
            settle(down.at[0], w_sem.at[2])

        @pl.when((t >= AT[1]) & (t < nc + AT[1]))
        def _():
            c = t - AT[1]
            settle(some(192), x_recv.at[c, 2])
            for side in range(2):
                x_copy(c, 6 + side).start()
                p_copy(c, 1 + side).start()
            settle(some(384), x_recv.at[c, 0])
            for side in range(2):
                x_copy(c, 2 + side).start()

        @pl.when((t >= AT[2]) & (t < nc + AT[2]))
        def _():
            c = t - AT[2]
            settle(some(96), x_recv.at[c, 3])
            p_copy(c, 3).start()
            settle(some(192), x_recv.at[c, 1])
            d_copy(c, core * nc + c, 0).start()

        @pl.when((t >= AT[3]) & (t < nc + AT[3]))
        def _():
            c = t - AT[3]
            settle(some(384), p_recv.at[c])
            d_copy(c, core * nc + c, 1).start()
            products(core * nc + c)

        @pl.when(t >= AT[4])
        def _():
            c = t - AT[4]
            settle(xc.at[0], d_recv.at[c])
            products((1 - core) * nc + c)

        return carry

    lax.fori_loop(0, nc + AT[4], dispatch, 0)

    def gates(m, carry):
        rows = pl.ds(pl.multiple_of(m * 128, 128), 128)
        value = jnp.zeros((128, 1), F32)
        for at in range(0, SIDE_HID, 128):
            g = pre[rows, at:at + 128]
            u = pre[rows, SIDE_HID + at:SIDE_HID + at + 128]
            h = hg[rows, at:at + 128]
            s = jax.nn.sigmoid(g)
            active = g * s
            hidden = (active * u).astype(BF).astype(F32)
            g_side = h * u * (s * (1.0 + g * (1.0 - s)))
            u_side = h * active
            value = value + jnp.sum(hidden * h, axis=1, keepdims=True)
            gsus[rows, at:at + 128] = g_side.astype(BF)
            gsus[rows, SIDE_HID + at:SIDE_HID + at + 128] = u_side.astype(BF)
            hid_t[at:at + 128, rows] = hidden.T.astype(BF)
            gsus_t[at:at + 128, rows] = g_side.T.astype(BF)
            gsus_t[SIDE_HID + at:SIDE_HID + at + 128, rows] = u_side.T.astype(BF)
        part_r[rows, :] = jnp.broadcast_to(value, (128, 128)).astype(BF)
        return carry

    lax.fori_loop(0, 6, gates, 0)

    def e_copy(n, feature, c):
        if feature:
            return remote(s_f.at[c], tpr.at[c], e_send.at[n], e_recv.at[n], other_core)
        return remote(part_r, tpr_r, e_send.at[n], e_recv.at[n], other_core)

    def pick(feature, c, f_ref, r_ref):
        return f_ref.at[c] if feature else r_ref

    def a_copy(n, feature, c, i):
        s, xa = pick(feature, c, s_f, s_r), pick(feature, c, xa_f, xa_r)
        at = pl.ds(((x + 2) % 4) * 192 + 96 * i, 96)
        return remote(
            s.at[at], xa.at[i], a_send.at[int(feature)], a_recv.at[n], right if i == 0 else left
        )

    def b_copy(n, feature, c, i):
        s, xb = pick(feature, c, s_f, s_r), pick(feature, c, xb_f, xb_r)
        at = pl.ds(((x + 1 + 2 * i) % 4) * 192, 192)
        return remote(
            s.at[at], xb.at[i], b_send.at[int(feature)], b_recv.at[n], right if i == 0 else left
        )

    def v_copy(n, feature, c, i):
        s, yr = pick(feature, c, s_f, s_r), pick(feature, c, yr_f, yr_r)
        at = pl.ds(block(x, y_peers[i]), BUNDLE)
        return remote(
            s.at[at], yr.at[i], v_send.at[int(feature)], v_recv.at[n], chip(z, y_peers[i], x)
        )

    def q_copy(n, feature, c, i):
        zs, zr = pick(feature, c, zs_f, zs_r), pick(feature, c, zr_f, zr_r)
        return remote(
            zs.at[z_peers[i]], zr.at[i], q_send.at[int(feature)], q_recv.at[n], chip(z_peers[i], y, x)
        )

    def half_lanes(c):
        return pl.ds(pl.multiple_of((c % 2) * LANES, LANES), LANES)

    def stage_core(n, feature, c):
        if not feature:
            e_copy(n, False, c).start()
            return
        k = (1 - core) * nc + c
        for m in range(3):
            rows = pl.ds(m * 256, 256)
            s_f[c, rows, :] = dot_nn(gsus[rows, :], wc[k]).astype(BF)
        e_copy(n, True, c).start()
        k = core * nc + c
        for m in range(3):
            rows = pl.ds(m * 256, 256)
            pre[rows, half_lanes(c)] = dot_nn(gsus[rows, :], wc[k])

    def stage_a(n, feature, c):
        e_copy(n, feature, c).wait()
        s = pick(feature, c, s_f, s_r)
        theirs = pick(feature, c, tpr, tpr_r)
        for m in range(3):
            rows = pl.ds(m * 256, 256)
            mine = pre[rows, half_lanes(c)] if feature else part_r[rows, :].astype(F32)
            s[rows, :] = (mine + theirs[rows, :].astype(F32)).astype(BF)
        for i in range(2):
            a_copy(n, feature, c, i).start()

    def stage_b(n, feature, c):
        s, xa = pick(feature, c, s_f, s_r), pick(feature, c, xa_f, xa_r)
        settle(xa, a_recv.at[n])
        for i in range(2):
            at = pl.ds(pl.multiple_of(((x + 1 + 2 * i) % 4) * 192 + 96 * i, 96), 96)
            s[at, :] = (s[at, :].astype(F32) + xa[i].astype(F32)).astype(BF)
        for i in range(2):
            b_copy(n, feature, c, i).start()

    def stage_v(n, feature, c):
        s, xb = pick(feature, c, s_f, s_r), pick(feature, c, xb_f, xb_r)
        settle(xb, b_recv.at[n])
        at = pl.ds(pl.multiple_of(x * 192, 192), 192)
        s[at, :] = (s[at, :].astype(F32) + xb[0].astype(F32) + xb[1].astype(F32)).astype(BF)
        for i in range(3):
            v_copy(n, feature, c, i).start()

    def stage_q(n, feature, c):
        s, yr = pick(feature, c, s_f, s_r), pick(feature, c, yr_f, yr_r)
        zs = pick(feature, c, zs_f, zs_r)
        settle(yr, v_recv.at[n])
        at = pl.ds(pl.multiple_of(block(x, y), BUNDLE), BUNDLE)
        mine = (s[at, :].astype(F32) + yr[0].astype(F32)).astype(BF)
        theirs = (yr[1].astype(F32) + yr[2].astype(F32)).astype(BF)
        slots = jnp.concatenate(
            [mine, theirs, jnp.zeros((128 - 2 * BUNDLE, mine.shape[1]), BF)], axis=0
        )
        if feature:
            rows = dot_nn(place_t[0], slots)
        else:
            lane = lax.broadcasted_iota(jnp.int32, (SIDE * ROWS, 128), 1)
            rows = jnp.where(
                lane == 0,
                dot_nn(place_t[1], slots),
                dot_nn(place_t[2], slots),
            )
        zs[...] = rows.astype(BF).reshape(zs.shape)
        for i in range(3):
            q_copy(n, feature, c, i).start()

    def stage_out(n, feature, c):
        zs, zr = pick(feature, c, zs_f, zs_r), pick(feature, c, zr_f, zr_r)
        settle(zr, q_recv.at[n])
        total = zs[z].astype(F32)
        for i in range(3):
            total = total + zr[i].astype(F32)
        if feature:
            out_tok[:, pl.ds(pl.multiple_of(c * LANES, LANES), LANES)] = total[:24].astype(BF)
        else:
            turned = jnp.concatenate([total, jnp.zeros((128 - ROWS, 128), F32)], axis=0).T
            out_rg[...] = turned[0:TOP, 0:rows_dev] / weights[...]

    def out_copies(k):
        at = pl.ds(pl.multiple_of(k * LANES, LANES), LANES)
        return (
            pltpu.make_async_copy(wc.at[k, pl.ds(0, hid)], out_gate.at[0, :, at], o_sem.at[0]),
            pltpu.make_async_copy(wc.at[k, pl.ds(SIDE_HID, hid)], out_up.at[0, :, at], o_sem.at[1]),
            pltpu.make_async_copy(wd.at[k], out_down.at[0, :, at], o_sem.at[2]),
        )

    def weight_grads(k):
        for m in range(3):
            rows = pl.ds(m * 256, 256)
            wc[k, rows, :] = dot_nn(gsus_t[rows, :], xc[k, 0]).astype(BF)
        wd[k] = dot_nn(hid_t[:hid], xc[k, 1]).astype(BF)
        for cp in out_copies(k):
            cp.start()

    stages = (stage_core, stage_a, stage_b, stage_v, stage_q, stage_out)

    def give_back(t, carry):
        for depth, stage in zip(BACK_AT, stages):
            n = t - depth

            @pl.when(n == 0)
            def _():
                stage(0, False, 0)

            @pl.when((n >= 1) & (n <= nc))
            def _():
                stage(n, True, n - 1)

        @pl.when((t >= GRADS_AT) & (t < nc + GRADS_AT))
        def _():
            weight_grads(core * nc + t - GRADS_AT)
            weight_grads((1 - core) * nc + t - GRADS_AT)

        return carry

    lax.fori_loop(0, nc + 1 + BACK_AT[-1], give_back, 0)

    settle(iz.at[pl.ds(0, 3)], i_send.at[0])
    settle(xc.at[0, :, pl.ds(0, 3 * rows_dev * nc)], z_send.at[0])
    settle(xc.at[0], y_send.at[0])
    settle(xc.at[pl.ds(0, 2)], x_send.at[0])
    settle(xc.at[0], x_send.at[1])
    settle(xc.at[0], x_send.at[2])
    settle(xc.at[0, 0], x_send.at[3])
    settle(xc.at[pl.ds(0, 2)], p_send.at[0])
    settle(xc.at[pl.ds(0, nc)], d_send.at[0])
    for sem, ref_r, ref_f in (
        (a_send, xa_r, xa_f), (b_send, xb_r, xb_f), (v_send, yr_r, yr_f), (q_send, zr_r, zr_f)
    ):
        settle(ref_r, sem.at[0])
        settle(ref_f, sem.at[1])
    settle(out_gate.at[0], o_sem.at[0])
    settle(out_up.at[0], o_sem.at[1])
    settle(out_down.at[0], o_sem.at[2])


def per_device(tokens, cotangent, routes, route_weights, gate_weight, up_weight, down_weight):
    rows, width = tokens.shape
    half = width // lax.axis_size("tp")
    nc = half // LANES
    hid = gate_weight.shape[2]
    vmem, anywhere = pltpu.VMEM, pl.ANY
    slots = 16 * BUNDLE

    def chunk_buffers(lead, lanes):
        return [
            vmem((*lead, slots, lanes), BF),
            vmem((*lead, 2, 96, lanes), BF),
            vmem((*lead, 2, 192, lanes), BF),
            vmem((*lead, 3, BUNDLE, lanes), BF),
            vmem((*lead, SIDE, ROWS, lanes), BF),
            vmem((*lead, 3, ROWS, lanes), BF),
        ]

    dma = pltpu.SemaphoreType.DMA
    token_grad, shares, gate_grad, up_grad, down_grad = pl.pallas_call(
        functools.partial(kernel, nc, hid),
        out_shape=(
            jax.ShapeDtypeStruct((rows, half), BF),
            jax.ShapeDtypeStruct((TOP, rows), F32),
            jax.ShapeDtypeStruct((1, hid, width), BF),
            jax.ShapeDtypeStruct((1, hid, width), BF),
            jax.ShapeDtypeStruct(down_weight.shape, BF),
        ),
        in_specs=[
            pl.BlockSpec(memory_space=anywhere),
            pl.BlockSpec(memory_space=anywhere),
            pl.BlockSpec(memory_space=vmem),
            pl.BlockSpec(memory_space=vmem),
            pl.BlockSpec(memory_space=anywhere),
            pl.BlockSpec(memory_space=anywhere),
            pl.BlockSpec(memory_space=anywhere),
        ],
        out_specs=(
            pl.BlockSpec(memory_space=vmem),
            pl.BlockSpec(memory_space=vmem),
            pl.BlockSpec(memory_space=anywhere),
            pl.BlockSpec(memory_space=anywhere),
            pl.BlockSpec(memory_space=anywhere),
        ),
        scratch_shapes=[
            vmem((nc, SIDE, 2, ROWS, LANES), BF),
            vmem((3, EXPERTS, 128), F32),
            vmem((SIDE, 3, EXPERTS, 128), F32),
            vmem((3, EXPERTS, 128), F32),
            vmem((2 * nc, 2, slots, LANES), BF),
            vmem((nc, 2, BUNDLE, LANES), BF),
            vmem((128, 128), BF),
            vmem((3, 128, 128), BF),
            vmem((2 * BUNDLE, 128), F32),
            vmem((2 * nc, hid, LANES), BF),
            vmem((2 * nc, 2 * SIDE_HID, LANES), BF),
            vmem((slots, 2 * SIDE_HID), F32),
            vmem((slots, SIDE_HID), F32),
            vmem((slots, 2 * SIDE_HID), BF),
            vmem((2 * SIDE_HID, slots), BF),
            vmem((SIDE_HID, slots), BF),
            vmem((nc, slots, LANES), BF),
            vmem((nc, slots, LANES), BF),
            *chunk_buffers((nc,), LANES)[1:],
            vmem((slots, 128), BF),
            vmem((slots, 128), BF),
            *chunk_buffers((), 128),
            dma((3,)),
            dma((1,)), dma((nc,)),
            dma((1,)), dma((1,)),
            dma((1,)), dma((nc, 2)),
            dma((4,)), dma((nc, 4)),
            dma((1,)), dma((nc,)),
            dma((1,)), dma((nc,)),
            dma((nc + 1,)), dma((nc + 1,)),
            dma((2,)), dma((nc + 1,)),
            dma((2,)), dma((nc + 1,)),
            dma((2,)), dma((nc + 1,)),
            dma((2,)), dma((nc + 1,)),
            dma((3,)),
        ],
        compiler_params=pltpu.CompilerParams(
            collective_id=0, has_side_effects=True, vmem_limit_bytes=43 * 1024 * 1024
        ),
    )(
        tokens, cotangent, routes.T, route_weights.T,
        gate_weight.transpose(0, 2, 1), up_weight.transpose(0, 2, 1), down_weight,
    )
    return token_grad, shares.T, gate_grad.transpose(0, 2, 1), up_grad.transpose(0, 2, 1), down_grad


def solution(mesh):
    return jax.shard_map(
        per_device,
        mesh=mesh,
        in_specs=(
            P("ep", None),
            P("ep", None),
            P("ep", None),
            P("ep", None),
            P("ep", None, "tp"),
            P("ep", None, "tp"),
            P("ep", "tp", None),
        ),
        out_specs=(
            P("ep", "tp"),
            P("ep", None),
            P("ep", None, "tp"),
            P("ep", None, "tp"),
            P("ep", "tp", None),
        ),
        check_vma=False,
    )
```

```python
import functools

import jax
import jax.numpy as jnp
from jax import lax
from jax.experimental import pallas as pl
from jax.experimental.pallas import tpu as pltpu
from jax.sharding import PartitionSpec as P

EXPERTS = 8
TOP = 2
CAP = 12
SIDE = 4
ROWS = 32
BUNDLE = 48
LANES = 256
AHEAD = 3
AT = (1, 2, 3, 4, 5)
BACK_AT = (0, 1, 3, 5, 7, 9)
GRADS_AT = 5
SIDE_HID = 384
BF = jnp.bfloat16
F32 = jnp.float32
MESH = pl.DeviceIdType.MESH


def dot_nt(a, b):
    return lax.dot_general(a, b, (((1,), (1,)), ((), ())), preferred_element_type=F32)


def dot_tn(a, b):
    return lax.dot_general(a, b, (((0,), (0,)), ((), ())), preferred_element_type=F32)


def dot_nn(a, b):
    return jnp.dot(a, b, preferred_element_type=F32)


def kernel(
    nc, hid,
    tokens, cotangent, routes_in, weights_in, gate, up, down,
    out_tok, out_rg, out_gate, out_up, out_down,
    routes, weights, tz, info, iz, codes, xc, ob, place, firsts, place_t, share,
    wd, wc, pre, hg, gsus, gsus_t, hid_t,
    s_f, tpr, xa_f, xb_f, yr_f, zs_f, zr_f,
    part_r, tpr_r, s_r, xa_r, xb_r, yr_r, zs_r, zr_r,
    w_sem, z_send, z_recv, i_send, i_recv, y_send, y_recv, x_send, x_recv, p_send, p_recv, d_send, d_recv,
    e_send, e_recv, a_send, a_recv, b_send, b_recv, v_send, v_recv, q_send, q_recv,
    o_sem,
):
    ep = lax.axis_index("ep")
    core = lax.axis_index("tp")
    z, y, x = ep // 16, (ep // 4) % 4, ep % 4
    pair = y // 2

    def chip(zz, yy, xx):
        return (zz * 16 + yy * 4 + xx, core)

    right = chip(z, y, (x + 1) % 4)
    left = chip(z, y, (x + 3) % 4)
    other_core = (ep, 1 - core)
    partner_y = 2 * pair + (1 - y % 2)
    cross_y = 3 - y
    cross2_y = 2 * (1 - pair) + y % 2
    y_peers = [partner_y, cross_y, cross2_y]
    z_peers = [(z + 1) % 4, (z + 3) % 4, (z + 2) % 4]

    rows_dev = tokens.shape[0]
    half_of = ((y + 1) // 2) % 2

    def block(xs, ys):
        return xs * 192 + (((ys + 1) // 2) % 2) * 96 + (ys // 2) * BUNDLE

    small = [
        pltpu.make_async_copy(routes_in, routes, w_sem.at[3]),
        pltpu.make_async_copy(weights_in, weights, w_sem.at[4]),
    ]
    for cp in small:
        cp.start()

    def pad_rows(c, carry):
        tz[c, :, :, rows_dev:, :] = jnp.zeros((SIDE, 2, ROWS - rows_dev, LANES), BF)
        return carry

    lax.fori_loop(0, nc, pad_rows, 0)

    barrier = pltpu.get_barrier_semaphore()
    for zz in z_peers:
        pl.semaphore_signal(barrier, inc=1, device_id=chip(zz, y, x), device_id_type=MESH)
    for yy in y_peers:
        pl.semaphore_signal(barrier, inc=1, device_id=chip(z, yy, x), device_id_type=MESH)
    for dev in (right, left, other_core):
        pl.semaphore_signal(barrier, inc=1, device_id=dev, device_id_type=MESH)

    w_copies = []
    for k in range(2 * nc):
        at = pl.ds(k * LANES, LANES)
        w_copies += [
            pltpu.make_async_copy(gate.at[0, :, at], wc.at[k, pl.ds(0, hid)], w_sem.at[0]),
            pltpu.make_async_copy(up.at[0, :, at], wc.at[k, pl.ds(SIDE_HID, hid)], w_sem.at[1]),
            pltpu.make_async_copy(down.at[0, :, at], wd.at[k], w_sem.at[2]),
        ]
    for cp in w_copies:
        cp.start()

    def remote(a, b, ss, rs, dev):
        return pltpu.make_async_remote_copy(
            src_ref=a, dst_ref=b, send_sem=ss, recv_sem=rs, device_id=dev, device_id_type=MESH
        )

    def settle(ref, sem):
        pltpu.make_async_copy(ref, ref, sem).wait()

    def some(n):
        return xc.at[0, 0, pl.ds(0, n)]

    def piece(ref, c):
        return ref.at[:, pl.ds(pl.multiple_of((core * nc + c) * LANES, LANES), LANES)]

    def landing(c, tensor):
        return tz.at[c, z, tensor, pl.ds(0, rows_dev)]

    def z_copy(c, i, tensor):
        return remote(
            piece(cotangent if tensor else tokens, c), landing(c, tensor),
            z_send.at[0], z_recv.at[c], chip(z_peers[i], y, x),
        )

    def own_copy(c, tensor):
        return pltpu.make_async_copy(
            piece(cotangent if tensor else tokens, c), landing(c, tensor), z_recv.at[c]
        )

    def zi_copy(i):
        return remote(info, iz.at[z], i_send.at[0], i_recv.at[0], chip(z_peers[i], y, x))

    def start_z(c):
        for tensor in range(2):
            for i in range(3):
                z_copy(c, i, tensor).start()
            own_copy(c, tensor).start()

    for cp in small:
        cp.wait()
    expert_row = lax.broadcasted_iota(jnp.int32, (EXPERTS, rows_dev), 0)
    hot = [expert_row == routes[k:k + 1, :] for k in range(2)]
    hit = jnp.where(hot[0] | hot[1], 1.0, 0.0).astype(BF)
    before = jnp.where(
        lax.broadcasted_iota(jnp.int32, (rows_dev, rows_dev), 0)
        < lax.broadcasted_iota(jnp.int32, (rows_dev, rows_dev), 1),
        1.0, 0.0,
    ).astype(BF)
    code = dot_nn(hit, before) + (z * CAP + 1).astype(F32)
    info[...] = jnp.zeros_like(info)
    for k in range(2):
        info[k, :, 0:rows_dev] = jnp.where(hot[k], code, 0.0)
    info[2, :, 0:rows_dev] = jnp.where(hot[0], weights[0:1, :], 0.0) + jnp.where(
        hot[1], weights[1:2, :], 0.0
    )
    iz[z] = info[...]
    pre[...] = jnp.zeros_like(pre)
    hg[...] = jnp.zeros_like(hg)

    def blank(k, carry):
        for at in (hid, SIDE_HID + hid):
            wc[k, at:at + SIDE_HID - hid, :] = jnp.zeros((SIDE_HID - hid, LANES), BF)
        return carry

    lax.fori_loop(0, 2 * nc, blank, 0)

    pl.semaphore_wait(barrier, 9)
    for i in range(3):
        zi_copy(i).start()
    for c in range(AHEAD):
        start_z(c)
    settle(iz.at[pl.ds(0, 3)], i_recv.at[0])
    for kind in range(3):
        total = iz[0, kind]
        for zz in range(1, SIDE):
            total = total + pltpu.roll(iz[zz, kind], zz * ROWS, 1)
        codes[kind] = total

    slot_number = lax.broadcasted_iota(jnp.int32, (BUNDLE, 128), 0).astype(F32) + 1.0

    def info_row(kind, expert):
        return codes[kind, pl.ds(expert, 1), :]

    spare = jnp.zeros((128 - 2 * BUNDLE, 128), F32)
    first, second = [], []
    for side, expert in ((0, 2 * z + pair), (1, 2 * z + 1 - pair)):
        first.append(jnp.where(slot_number == info_row(0, expert), 1.0, 0.0))
        second.append(jnp.where(slot_number == info_row(1, expert), 1.0, 0.0))
        share[side * BUNDLE:(side + 1) * BUNDLE, :] = jnp.broadcast_to(
            jnp.sum((first[side] + second[side]) * info_row(2, expert), axis=1, keepdims=True),
            (BUNDLE, 128),
        )
    first = jnp.concatenate(first + [spare], axis=0)
    second = jnp.concatenate(second + [spare], axis=0)
    place[...] = (first + second).astype(BF)
    firsts[...] = first

    def y_copy(c, i):
        k = core * nc + c
        at = pl.ds(block(x, y), BUNDLE)
        tensor = 1 if i == 3 else 0
        peer = cross_y if i == 3 else y_peers[i]
        from_ref = xc.at[k, 0, at, :] if i == 0 else ob.at[c, tensor]
        return remote(
            from_ref, xc.at[k, tensor, at, :], y_send.at[0], y_recv.at[c, tensor], chip(z, peer, x)
        )

    def x_copy(c, i):
        k = core * nc + c
        tensor = i // 4
        step = i % 4
        size, base = (96, half_of * 96) if tensor else (192, 0)
        if step < 2:
            at = pl.ds(x * 192 + base, size)
        elif step == 2:
            at = pl.ds(((x + 3) % 4) * 192 + base, size // 2)
        else:
            at = pl.ds(((x + 1) % 4) * 192 + base + size // 2, size // 2)
        ref = xc.at[k, tensor, at, :]
        return remote(
            ref, ref, x_send.at[i // 2], x_recv.at[c, i // 2], right if i % 2 == 0 else left
        )

    def p_copy(c, i):
        at = pl.ds(((x + (0, 3, 1, 2)[i]) % 4) * 192 + half_of * 96, 96)
        ref = xc.at[core * nc + c, 1, at, :]
        return remote(ref, ref, p_send.at[0], p_recv.at[c], chip(z, partner_y, x))

    def d_copy(c, k, tensor):
        ref = xc.at[k, tensor]
        return remote(ref, ref, d_send.at[0], d_recv.at[c], other_core)

    def compact(c):
        settle(some(8 * rows_dev), z_recv.at[c])

        @pl.when(c + AHEAD < nc)
        def _():
            start_z(c + AHEAD)

        k = core * nc + c
        at = pl.ds(pl.multiple_of(block(x, y), BUNDLE), BUNDLE)
        for tensor in (1, 0):
            rows = dot_nn(place[:2 * BUNDLE], tz[c, :, tensor].reshape(SIDE * ROWS, LANES))
            if tensor == 1:
                rows = rows * share[:, 0:1]
            rows = rows.astype(BF)
            xc[k, tensor, at, :] = rows[:BUNDLE]
            ob[c, tensor] = rows[BUNDLE:]
            for i in ((3,) if tensor else (0, 1, 2)):
                y_copy(c, i).start()

    def products(k):
        for m in range(3):
            rows = pl.ds(m * 256, 256)
            pre[rows, :] += dot_nt(xc[k, 0, rows, :], wc[k])
            hg[rows, :hid] += dot_nt(xc[k, 1, rows, :], wd[k])

    def dispatch(t, carry):
        @pl.when(t < nc)
        def _():
            compact(t)

        @pl.when((t >= AT[0]) & (t < nc + AT[0]))
        def _():
            c = t - AT[0]
            settle(some(BUNDLE), y_recv.at[c, 1])
            x_copy(c, 4).start()
            x_copy(c, 5).start()
            p_copy(c, 0).start()
            settle(some(3 * BUNDLE), y_recv.at[c, 0])
            x_copy(c, 0).start()
            x_copy(c, 1).start()

        @pl.when(t == 1)
        def _():
            settle(gate.at[0], w_sem.at[0])
            settle(up.at[0], w_sem.at[1])
            settle(down.at[0], w_sem.at[2])

        @pl.when((t >= AT[1]) & (t < nc + AT[1]))
        def _():
            c = t - AT[1]
            settle(some(192), x_recv.at[c, 2])
            for side in range(2):
                x_copy(c, 6 + side).start()
                p_copy(c, 1 + side).start()
            settle(some(384), x_recv.at[c, 0])
            for side in range(2):
                x_copy(c, 2 + side).start()

        @pl.when((t >= AT[2]) & (t < nc + AT[2]))
        def _():
            c = t - AT[2]
            settle(some(96), x_recv.at[c, 3])
            p_copy(c, 3).start()
            settle(some(192), x_recv.at[c, 1])
            d_copy(c, core * nc + c, 0).start()

        @pl.when((t >= AT[3]) & (t < nc + AT[3]))
        def _():
            c = t - AT[3]
            settle(some(384), p_recv.at[c])
            d_copy(c, core * nc + c, 1).start()
            products(core * nc + c)

        @pl.when(t >= AT[4])
        def _():
            c = t - AT[4]
            settle(xc.at[0], d_recv.at[c])
            products((1 - core) * nc + c)

        return carry

    lax.fori_loop(0, nc + AT[4], dispatch, 0)

    first = firsts[...]
    place_t[0] = place[...].astype(F32).T.astype(BF)
    place_t[1] = first.T.astype(BF)
    place_t[2] = (place[...].astype(F32) - first).T.astype(BF)

    def gates(m, carry):
        rows = pl.ds(pl.multiple_of(m * 128, 128), 128)
        value = jnp.zeros((128, 1), F32)
        for at in range(0, SIDE_HID, 128):
            g = pre[rows, at:at + 128]
            u = pre[rows, SIDE_HID + at:SIDE_HID + at + 128]
            h = hg[rows, at:at + 128]
            s = jax.nn.sigmoid(g)
            active = g * s
            hidden = (active * u).astype(BF).astype(F32)
            g_side = h * u * (s * (1.0 + g * (1.0 - s)))
            u_side = h * active
            value = value + jnp.sum(hidden * h, axis=1, keepdims=True)
            gsus[rows, at:at + 128] = g_side.astype(BF)
            gsus[rows, SIDE_HID + at:SIDE_HID + at + 128] = u_side.astype(BF)
            hid_t[at:at + 128, rows] = hidden.T.astype(BF)
            gsus_t[at:at + 128, rows] = g_side.T.astype(BF)
            gsus_t[SIDE_HID + at:SIDE_HID + at + 128, rows] = u_side.T.astype(BF)
        part_r[rows, :] = jnp.broadcast_to(value, (128, 128)).astype(BF)
        return carry

    lax.fori_loop(0, 6, gates, 0)

    def e_copy(n, feature, c):
        if feature:
            return remote(s_f.at[c], tpr.at[c], e_send.at[n], e_recv.at[n], other_core)
        return remote(part_r, tpr_r, e_send.at[n], e_recv.at[n], other_core)

    def pick(feature, c, f_ref, r_ref):
        return f_ref.at[c] if feature else r_ref

    def a_copy(n, feature, c, i):
        s, xa = pick(feature, c, s_f, s_r), pick(feature, c, xa_f, xa_r)
        at = pl.ds(((x + 2) % 4) * 192 + 96 * i, 96)
        return remote(
            s.at[at], xa.at[i], a_send.at[int(feature)], a_recv.at[n], right if i == 0 else left
        )

    def b_copy(n, feature, c, i):
        s, xb = pick(feature, c, s_f, s_r), pick(feature, c, xb_f, xb_r)
        at = pl.ds(((x + 1 + 2 * i) % 4) * 192, 192)
        return remote(
            s.at[at], xb.at[i], b_send.at[int(feature)], b_recv.at[n], right if i == 0 else left
        )

    def v_copy(n, feature, c, i):
        s, yr = pick(feature, c, s_f, s_r), pick(feature, c, yr_f, yr_r)
        at = pl.ds(block(x, y_peers[i]), BUNDLE)
        return remote(
            s.at[at], yr.at[i], v_send.at[int(feature)], v_recv.at[n], chip(z, y_peers[i], x)
        )

    def q_copy(n, feature, c, i):
        zs, zr = pick(feature, c, zs_f, zs_r), pick(feature, c, zr_f, zr_r)
        return remote(
            zs.at[z_peers[i]], zr.at[i], q_send.at[int(feature)], q_recv.at[n], chip(z_peers[i], y, x)
        )

    def half_lanes(c):
        return pl.ds(pl.multiple_of((c % 2) * LANES, LANES), LANES)

    def stage_core(n, feature, c):
        if not feature:
            e_copy(n, False, c).start()
            return
        k = (1 - core) * nc + c
        for m in range(3):
            rows = pl.ds(m * 256, 256)
            s_f[c, rows, :] = dot_nn(gsus[rows, :], wc[k]).astype(BF)
        e_copy(n, True, c).start()
        k = core * nc + c
        for m in range(3):
            rows = pl.ds(m * 256, 256)
            pre[rows, half_lanes(c)] = dot_nn(gsus[rows, :], wc[k])

    def stage_a(n, feature, c):
        e_copy(n, feature, c).wait()
        s = pick(feature, c, s_f, s_r)
        theirs = pick(feature, c, tpr, tpr_r)
        for m in range(3):
            rows = pl.ds(m * 256, 256)
            mine = pre[rows, half_lanes(c)] if feature else part_r[rows, :].astype(F32)
            s[rows, :] = (mine + theirs[rows, :].astype(F32)).astype(BF)
        for i in range(2):
            a_copy(n, feature, c, i).start()

    def stage_b(n, feature, c):
        s, xa = pick(feature, c, s_f, s_r), pick(feature, c, xa_f, xa_r)
        settle(xa, a_recv.at[n])
        for i in range(2):
            at = pl.ds(pl.multiple_of(((x + 1 + 2 * i) % 4) * 192 + 96 * i, 96), 96)
            s[at, :] = (s[at, :].astype(F32) + xa[i].astype(F32)).astype(BF)
        for i in range(2):
            b_copy(n, feature, c, i).start()

    def stage_v(n, feature, c):
        s, xb = pick(feature, c, s_f, s_r), pick(feature, c, xb_f, xb_r)
        settle(xb, b_recv.at[n])
        at = pl.ds(pl.multiple_of(x * 192, 192), 192)
        s[at, :] = (s[at, :].astype(F32) + xb[0].astype(F32) + xb[1].astype(F32)).astype(BF)
        for i in range(3):
            v_copy(n, feature, c, i).start()

    def stage_q(n, feature, c):
        s, yr = pick(feature, c, s_f, s_r), pick(feature, c, yr_f, yr_r)
        zs = pick(feature, c, zs_f, zs_r)
        settle(yr, v_recv.at[n])
        at = pl.ds(pl.multiple_of(block(x, y), BUNDLE), BUNDLE)
        mine = (s[at, :].astype(F32) + yr[0].astype(F32)).astype(BF)
        theirs = (yr[1].astype(F32) + yr[2].astype(F32)).astype(BF)
        slots = jnp.concatenate(
            [mine, theirs, jnp.zeros((128 - 2 * BUNDLE, mine.shape[1]), BF)], axis=0
        )
        if feature:
            rows = dot_nn(place_t[0], slots)
        else:
            lane = lax.broadcasted_iota(jnp.int32, (SIDE * ROWS, 128), 1)
            rows = jnp.where(
                lane == 0,
                dot_nn(place_t[1], slots),
                dot_nn(place_t[2], slots),
            )
        zs[...] = rows.astype(BF).reshape(zs.shape)
        for i in range(3):
            q_copy(n, feature, c, i).start()

    def stage_out(n, feature, c):
        zs, zr = pick(feature, c, zs_f, zs_r), pick(feature, c, zr_f, zr_r)
        settle(zr, q_recv.at[n])
        total = zs[z].astype(F32)
        for i in range(3):
            total = total + zr[i].astype(F32)
        if feature:
            out_tok[:, pl.ds(pl.multiple_of(c * LANES, LANES), LANES)] = total[:24].astype(BF)
        else:
            turned = jnp.concatenate([total, jnp.zeros((128 - ROWS, 128), F32)], axis=0).T
            out_rg[...] = turned[0:TOP, 0:rows_dev] / weights[...]

    def out_copies(k):
        at = pl.ds(pl.multiple_of(k * LANES, LANES), LANES)
        return (
            pltpu.make_async_copy(wc.at[k, pl.ds(0, hid)], out_gate.at[0, :, at], o_sem.at[0]),
            pltpu.make_async_copy(wc.at[k, pl.ds(SIDE_HID, hid)], out_up.at[0, :, at], o_sem.at[1]),
            pltpu.make_async_copy(wd.at[k], out_down.at[0, :, at], o_sem.at[2]),
        )

    def weight_grads(k):
        for m in range(3):
            rows = pl.ds(m * 256, 256)
            wc[k, rows, :] = dot_nn(gsus_t[rows, :], xc[k, 0]).astype(BF)
        wd[k] = dot_nn(hid_t[:hid], xc[k, 1]).astype(BF)
        for cp in out_copies(k):
            cp.start()

    stages = (stage_core, stage_a, stage_b, stage_v, stage_q, stage_out)

    def give_back(t, carry):
        for depth, stage in zip(BACK_AT, stages):
            n = t - depth

            @pl.when(n == 0)
            def _():
                stage(0, False, 0)

            @pl.when((n >= 1) & (n <= nc))
            def _():
                stage(n, True, n - 1)

        @pl.when((t >= GRADS_AT) & (t < nc + GRADS_AT))
        def _():
            weight_grads(core * nc + t - GRADS_AT)
            weight_grads((1 - core) * nc + t - GRADS_AT)

        return carry

    lax.fori_loop(0, nc + 1 + BACK_AT[-1], give_back, 0)

    settle(iz.at[pl.ds(0, 3)], i_send.at[0])
    settle(xc.at[0, :, pl.ds(0, 3 * rows_dev * nc)], z_send.at[0])
    settle(xc.at[0], y_send.at[0])
    settle(xc.at[pl.ds(0, 2)], x_send.at[0])
    settle(xc.at[0], x_send.at[1])
    settle(xc.at[0], x_send.at[2])
    settle(xc.at[0, 0], x_send.at[3])
    settle(xc.at[pl.ds(0, 2)], p_send.at[0])
    settle(xc.at[pl.ds(0, nc)], d_send.at[0])
    for sem, ref_r, ref_f in (
        (a_send, xa_r, xa_f), (b_send, xb_r, xb_f), (v_send, yr_r, yr_f), (q_send, zr_r, zr_f)
    ):
        settle(ref_r, sem.at[0])
        settle(ref_f, sem.at[1])
    settle(out_gate.at[0], o_sem.at[0])
    settle(out_up.at[0], o_sem.at[1])
    settle(out_down.at[0], o_sem.at[2])


def out_kernel(*refs):
    count = (len(refs) - 1) // 2
    sem = refs[-1]
    copies = []
    for i in range(count):
        copies.append(pltpu.make_async_copy(refs[i], refs[count + i], sem.at[i]))
    for cp in copies:
        cp.start()
    for cp in copies:
        cp.wait()


def in_hbm(a):
    return pltpu.with_memory_space_constraint(a, pltpu.HBM)


def put_out(*arrays):
    return pl.pallas_call(
        out_kernel,
        out_shape=tuple(jax.ShapeDtypeStruct(a.shape, a.dtype) for a in arrays),
        in_specs=[pl.BlockSpec(memory_space=pl.ANY)] * len(arrays),
        out_specs=(pl.BlockSpec(memory_space=pl.ANY),) * len(arrays),
        scratch_shapes=[pltpu.SemaphoreType.DMA((len(arrays),))],
        compiler_params=pltpu.CompilerParams(vmem_limit_bytes=43 * 1024 * 1024),
    )(*arrays)


def per_device(tokens, cotangent, routes, route_weights, gate_weight, up_weight, down_weight):
    rows, width = tokens.shape
    half = width // lax.axis_size("tp")
    nc = half // LANES
    hid = gate_weight.shape[2]
    vmem, anywhere = pltpu.VMEM, pl.ANY
    slots = 16 * BUNDLE

    def chunk_buffers(lead, lanes):
        return [
            vmem((*lead, slots, lanes), BF),
            vmem((*lead, 2, 96, lanes), BF),
            vmem((*lead, 2, 192, lanes), BF),
            vmem((*lead, 3, BUNDLE, lanes), BF),
            vmem((*lead, SIDE, ROWS, lanes), BF),
            vmem((*lead, 3, ROWS, lanes), BF),
        ]

    dma = pltpu.SemaphoreType.DMA
    token_grad, shares, gate_grad, up_grad, down_grad = pl.pallas_call(
        functools.partial(kernel, nc, hid),
        out_shape=(
            jax.ShapeDtypeStruct((rows, half), BF),
            jax.ShapeDtypeStruct((TOP, rows), F32),
            jax.ShapeDtypeStruct((1, hid, width), BF),
            jax.ShapeDtypeStruct((1, hid, width), BF),
            jax.ShapeDtypeStruct(down_weight.shape, BF),
        ),
        in_specs=[
            pl.BlockSpec(memory_space=anywhere),
            pl.BlockSpec(memory_space=anywhere),
            pl.BlockSpec(memory_space=anywhere),
            pl.BlockSpec(memory_space=anywhere),
            pl.BlockSpec(memory_space=anywhere),
            pl.BlockSpec(memory_space=anywhere),
            pl.BlockSpec(memory_space=anywhere),
        ],
        out_specs=(
            pl.BlockSpec(memory_space=vmem),
            pl.BlockSpec(memory_space=vmem),
            pl.BlockSpec(memory_space=anywhere),
            pl.BlockSpec(memory_space=anywhere),
            pl.BlockSpec(memory_space=anywhere),
        ),
        scratch_shapes=[
            vmem((TOP, rows), jnp.int32),
            vmem((TOP, rows), F32),
            vmem((nc, SIDE, 2, ROWS, LANES), BF),
            vmem((3, EXPERTS, 128), F32),
            vmem((SIDE, 3, EXPERTS, 128), F32),
            vmem((3, EXPERTS, 128), F32),
            vmem((2 * nc, 2, slots, LANES), BF),
            vmem((nc, 2, BUNDLE, LANES), BF),
            vmem((128, 128), BF),
            vmem((128, 128), F32),
            vmem((3, 128, 128), BF),
            vmem((2 * BUNDLE, 128), F32),
            vmem((2 * nc, hid, LANES), BF),
            vmem((2 * nc, 2 * SIDE_HID, LANES), BF),
            vmem((slots, 2 * SIDE_HID), F32),
            vmem((slots, SIDE_HID), F32),
            vmem((slots, 2 * SIDE_HID), BF),
            vmem((2 * SIDE_HID, slots), BF),
            vmem((SIDE_HID, slots), BF),
            vmem((nc, slots, LANES), BF),
            vmem((nc, slots, LANES), BF),
            *chunk_buffers((nc,), LANES)[1:],
            vmem((slots, 128), BF),
            vmem((slots, 128), BF),
            *chunk_buffers((), 128),
            dma((5,)),
            dma((1,)), dma((nc,)),
            dma((1,)), dma((1,)),
            dma((1,)), dma((nc, 2)),
            dma((4,)), dma((nc, 4)),
            dma((1,)), dma((nc,)),
            dma((1,)), dma((nc,)),
            dma((nc + 1,)), dma((nc + 1,)),
            dma((2,)), dma((nc + 1,)),
            dma((2,)), dma((nc + 1,)),
            dma((2,)), dma((nc + 1,)),
            dma((2,)), dma((nc + 1,)),
            dma((3,)),
        ],
        compiler_params=pltpu.CompilerParams(
            collective_id=0, has_side_effects=True, vmem_limit_bytes=43 * 1024 * 1024
        ),
    )(
        in_hbm(tokens), in_hbm(cotangent), in_hbm(routes.T), in_hbm(route_weights.T),
        in_hbm(gate_weight.transpose(0, 2, 1)), in_hbm(up_weight.transpose(0, 2, 1)),
        in_hbm(down_weight),
    )
    token_grad, shares, gate_grad, up_grad, down_grad = put_out(
        token_grad, shares, gate_grad, up_grad, down_grad
    )
    return token_grad, shares.T, gate_grad.transpose(0, 2, 1), up_grad.transpose(0, 2, 1), down_grad


def solution(mesh):
    return jax.shard_map(
        per_device,
        mesh=mesh,
        in_specs=(
            P("ep", None),
            P("ep", None),
            P("ep", None),
            P("ep", None),
            P("ep", None, "tp"),
            P("ep", None, "tp"),
            P("ep", "tp", None),
        ),
        out_specs=(
            P("ep", "tp"),
            P("ep", None),
            P("ep", None, "tp"),
            P("ep", None, "tp"),
            P("ep", "tp", None),
        ),
        check_vma=False,
    )
```

```python
import functools

import jax
import jax.numpy as jnp
from jax import lax
from jax.experimental import pallas as pl
from jax.experimental.pallas import tpu as pltpu
from jax.sharding import PartitionSpec as P

EXPERTS = 8
TOP = 2
CAP = 12
SIDE = 4
ROWS = 32
BUNDLE = 48
LANES = 256
AHEAD = 4
AT = (2, 3, 4, 5, 6)
BACK_AT = (0, 1, 3, 5, 7, 9)
GRADS_AT = 5
SIDE_HID = 384
BF = jnp.bfloat16
F32 = jnp.float32
MESH = pl.DeviceIdType.MESH


def dot_nt(a, b):
    return lax.dot_general(a, b, (((1,), (1,)), ((), ())), preferred_element_type=F32)


def dot_tn(a, b):
    return lax.dot_general(a, b, (((0,), (0,)), ((), ())), preferred_element_type=F32)


def dot_nn(a, b):
    return jnp.dot(a, b, preferred_element_type=F32)


def kernel(
    nc, hid,
    tokens, cotangent, routes_in, weights_in, gate, up, down,
    out_tok, out_rg, out_gate, out_up, out_down,
    routes, weights, tz, info, iz, codes, xc, ob, place, firsts, place_t, share,
    wd, wc, pre, hg, gsus, gsus_t, hid_t,
    s_f, tpr, xa_f, xb_f, yr_f, zs_f, zr_f,
    part_r, tpr_r, s_r, xa_r, xb_r, yr_r, zs_r, zr_r,
    w_sem, z_send, z_recv, i_send, i_recv, y_send, y_recv, x_send, x_recv, p_send, p_recv, d_send, d_recv,
    e_send, e_recv, a_send, a_recv, b_send, b_recv, v_send, v_recv, q_send, q_recv,
    o_sem,
):
    ep = lax.axis_index("ep")
    core = lax.axis_index("tp")
    z, y, x = ep // 16, (ep // 4) % 4, ep % 4
    pair = y // 2

    def chip(zz, yy, xx):
        return (zz * 16 + yy * 4 + xx, core)

    right = chip(z, y, (x + 1) % 4)
    left = chip(z, y, (x + 3) % 4)
    other_core = (ep, 1 - core)
    partner_y = 2 * pair + (1 - y % 2)
    cross_y = 3 - y
    cross2_y = 2 * (1 - pair) + y % 2
    y_peers = [partner_y, cross_y, cross2_y]
    z_peers = [(z + 1) % 4, (z + 3) % 4, (z + 2) % 4]

    rows_dev = tokens.shape[0]
    half_of = ((y + 1) // 2) % 2

    def block(xs, ys):
        return xs * 192 + (((ys + 1) // 2) % 2) * 96 + (ys // 2) * BUNDLE

    small = [
        pltpu.make_async_copy(routes_in, routes, w_sem.at[3]),
        pltpu.make_async_copy(weights_in, weights, w_sem.at[4]),
    ]
    for cp in small:
        cp.start()

    def pad_rows(c, carry):
        tz[c, :, :, rows_dev:, :] = jnp.zeros((SIDE, 2, ROWS - rows_dev, LANES), BF)
        return carry

    lax.fori_loop(0, nc, pad_rows, 0)

    barrier = pltpu.get_barrier_semaphore()
    for zz in z_peers:
        pl.semaphore_signal(barrier, inc=1, device_id=chip(zz, y, x), device_id_type=MESH)
    for yy in y_peers:
        pl.semaphore_signal(barrier, inc=1, device_id=chip(z, yy, x), device_id_type=MESH)
    for dev in (right, left, other_core):
        pl.semaphore_signal(barrier, inc=1, device_id=dev, device_id_type=MESH)

    w_copies = []
    for k in range(2 * nc):
        at = pl.ds(k * LANES, LANES)
        w_copies += [
            pltpu.make_async_copy(gate.at[0, :, at], wc.at[k, pl.ds(0, hid)], w_sem.at[0]),
            pltpu.make_async_copy(up.at[0, :, at], wc.at[k, pl.ds(SIDE_HID, hid)], w_sem.at[1]),
            pltpu.make_async_copy(down.at[0, :, at], wd.at[k], w_sem.at[2]),
        ]
    for cp in w_copies:
        cp.start()

    def remote(a, b, ss, rs, dev):
        return pltpu.make_async_remote_copy(
            src_ref=a, dst_ref=b, send_sem=ss, recv_sem=rs, device_id=dev, device_id_type=MESH
        )

    def settle(ref, sem):
        pltpu.make_async_copy(ref, ref, sem).wait()

    def some(n):
        return xc.at[0, 0, pl.ds(0, n)]

    def piece(ref, c):
        return ref.at[:, pl.ds(pl.multiple_of((core * nc + c) * LANES, LANES), LANES)]

    def landing(c, tensor):
        return tz.at[c, z, tensor, pl.ds(0, rows_dev)]

    def z_copy(c, i, tensor):
        return remote(
            piece(cotangent if tensor else tokens, c), landing(c, tensor),
            z_send.at[0], z_recv.at[c], chip(z_peers[i], y, x),
        )

    def own_copy(c, tensor):
        return pltpu.make_async_copy(
            piece(cotangent if tensor else tokens, c), landing(c, tensor), z_recv.at[c]
        )

    def zi_copy(i):
        return remote(info, iz.at[z], i_send.at[0], i_recv.at[0], chip(z_peers[i], y, x))

    def start_z(c):
        for tensor in range(2):
            for i in range(3):
                z_copy(c, i, tensor).start()
            own_copy(c, tensor).start()

    for cp in small:
        cp.wait()
    expert_row = lax.broadcasted_iota(jnp.int32, (EXPERTS, rows_dev), 0)
    hot = [expert_row == routes[k:k + 1, :] for k in range(2)]
    hit = jnp.where(hot[0] | hot[1], 1.0, 0.0).astype(BF)
    before = jnp.where(
        lax.broadcasted_iota(jnp.int32, (rows_dev, rows_dev), 0)
        < lax.broadcasted_iota(jnp.int32, (rows_dev, rows_dev), 1),
        1.0, 0.0,
    ).astype(BF)
    code = dot_nn(hit, before) + (z * CAP + 1).astype(F32)
    info[...] = jnp.zeros_like(info)
    for k in range(2):
        info[k, :, 0:rows_dev] = jnp.where(hot[k], code, 0.0)
    info[2, :, 0:rows_dev] = jnp.where(hot[0], weights[0:1, :], 0.0) + jnp.where(
        hot[1], weights[1:2, :], 0.0
    )
    iz[z] = info[...]
    pre[...] = jnp.zeros_like(pre)
    hg[...] = jnp.zeros_like(hg)

    def blank(k, carry):
        for at in (hid, SIDE_HID + hid):
            wc[k, at:at + SIDE_HID - hid, :] = jnp.zeros((SIDE_HID - hid, LANES), BF)
        return carry

    lax.fori_loop(0, 2 * nc, blank, 0)

    pl.semaphore_wait(barrier, 9)
    for i in range(3):
        zi_copy(i).start()
    for c in range(AHEAD):
        start_z(c)
    settle(iz.at[pl.ds(0, 3)], i_recv.at[0])
    for kind in range(3):
        total = iz[0, kind]
        for zz in range(1, SIDE):
            total = total + pltpu.roll(iz[zz, kind], zz * ROWS, 1)
        codes[kind] = total

    slot_number = lax.broadcasted_iota(jnp.int32, (BUNDLE, 128), 0).astype(F32) + 1.0

    def info_row(kind, expert):
        return codes[kind, pl.ds(expert, 1), :]

    spare = jnp.zeros((128 - 2 * BUNDLE, 128), F32)
    first, second = [], []
    for side, expert in ((0, 2 * z + pair), (1, 2 * z + 1 - pair)):
        first.append(jnp.where(slot_number == info_row(0, expert), 1.0, 0.0))
        second.append(jnp.where(slot_number == info_row(1, expert), 1.0, 0.0))
        share[side * BUNDLE:(side + 1) * BUNDLE, :] = jnp.broadcast_to(
            jnp.sum((first[side] + second[side]) * info_row(2, expert), axis=1, keepdims=True),
            (BUNDLE, 128),
        )
    first = jnp.concatenate(first + [spare], axis=0)
    second = jnp.concatenate(second + [spare], axis=0)
    place[...] = (first + second).astype(BF)
    firsts[...] = first

    def y_copy(c, i):
        k = core * nc + c
        at = pl.ds(block(x, y), BUNDLE)
        tensor = 1 if i == 3 else 0
        peer = cross_y if i == 3 else y_peers[i]
        from_ref = xc.at[k, 0, at, :] if i == 0 else ob.at[c, tensor]
        return remote(
            from_ref, xc.at[k, tensor, at, :], y_send.at[0], y_recv.at[c, tensor], chip(z, peer, x)
        )

    def x_copy(c, i):
        k = core * nc + c
        tensor = i // 4
        step = i % 4
        size, base = (96, half_of * 96) if tensor else (192, 0)
        if step < 2:
            at = pl.ds(x * 192 + base, size)
        elif step == 2:
            at = pl.ds(((x + 3) % 4) * 192 + base, size // 2)
        else:
            at = pl.ds(((x + 1) % 4) * 192 + base + size // 2, size // 2)
        ref = xc.at[k, tensor, at, :]
        return remote(
            ref, ref, x_send.at[i // 2], x_recv.at[c, i // 2], right if i % 2 == 0 else left
        )

    def p_copy(c, i):
        at = pl.ds(((x + (0, 3, 1, 2)[i]) % 4) * 192 + half_of * 96, 96)
        ref = xc.at[core * nc + c, 1, at, :]
        return remote(ref, ref, p_send.at[0], p_recv.at[c], chip(z, partner_y, x))

    def d_copy(c, k, tensor):
        ref = xc.at[k, tensor]
        return remote(ref, ref, d_send.at[0], d_recv.at[c], other_core)

    def compact(c):
        settle(some(8 * rows_dev), z_recv.at[c])

        @pl.when(c + AHEAD < nc)
        def _():
            start_z(c + AHEAD)

        k = core * nc + c
        at = pl.ds(pl.multiple_of(block(x, y), BUNDLE), BUNDLE)
        for tensor in (1, 0):
            rows = dot_nn(place[:2 * BUNDLE], tz[c, :, tensor].reshape(SIDE * ROWS, LANES))
            if tensor == 1:
                rows = rows * share[:, 0:1]
            rows = rows.astype(BF)
            xc[k, tensor, at, :] = rows[:BUNDLE]
            ob[c, tensor] = rows[BUNDLE:]
            for i in ((3,) if tensor else (0, 1, 2)):
                y_copy(c, i).start()

    def products(k):
        for m in range(3):
            rows = pl.ds(m * 256, 256)
            pre[rows, :] += dot_nt(xc[k, 0, rows, :], wc[k])
            hg[rows, :hid] += dot_nt(xc[k, 1, rows, :], wd[k])

    def dispatch(t, carry):
        @pl.when(t < nc)
        def _():
            compact(t)

        @pl.when((t >= AT[0]) & (t < nc + AT[0]))
        def _():
            c = t - AT[0]
            settle(some(BUNDLE), y_recv.at[c, 1])
            x_copy(c, 4).start()
            x_copy(c, 5).start()
            p_copy(c, 0).start()
            settle(some(3 * BUNDLE), y_recv.at[c, 0])
            x_copy(c, 0).start()
            x_copy(c, 1).start()

        @pl.when(t == 1)
        def _():
            settle(gate.at[0], w_sem.at[0])
            settle(up.at[0], w_sem.at[1])
            settle(down.at[0], w_sem.at[2])

        @pl.when((t >= AT[1]) & (t < nc + AT[1]))
        def _():
            c = t - AT[1]
            settle(some(192), x_recv.at[c, 2])
            for side in range(2):
                x_copy(c, 6 + side).start()
                p_copy(c, 1 + side).start()
            settle(some(384), x_recv.at[c, 0])
            for side in range(2):
                x_copy(c, 2 + side).start()

        @pl.when((t >= AT[2]) & (t < nc + AT[2]))
        def _():
            c = t - AT[2]
            settle(some(96), x_recv.at[c, 3])
            p_copy(c, 3).start()
            settle(some(192), x_recv.at[c, 1])
            d_copy(c, core * nc + c, 0).start()

        @pl.when((t >= AT[3]) & (t < nc + AT[3]))
        def _():
            c = t - AT[3]
            settle(some(384), p_recv.at[c])
            d_copy(c, core * nc + c, 1).start()
            products(core * nc + c)

        @pl.when(t >= AT[4])
        def _():
            c = t - AT[4]
            settle(xc.at[0], d_recv.at[c])
            products((1 - core) * nc + c)

        return carry

    lax.fori_loop(0, nc + AT[4], dispatch, 0)

    first = firsts[...]
    place_t[0] = place[...].astype(F32).T.astype(BF)
    place_t[1] = first.T.astype(BF)
    place_t[2] = (place[...].astype(F32) - first).T.astype(BF)

    def gates(m, carry):
        rows = pl.ds(pl.multiple_of(m * 128, 128), 128)
        value = jnp.zeros((128, 1), F32)
        for at in range(0, SIDE_HID, 128):
            g = pre[rows, at:at + 128]
            u = pre[rows, SIDE_HID + at:SIDE_HID + at + 128]
            h = hg[rows, at:at + 128]
            s = jax.nn.sigmoid(g)
            active = g * s
            hidden = (active * u).astype(BF).astype(F32)
            g_side = h * u * (s * (1.0 + g * (1.0 - s)))
            u_side = h * active
            value = value + jnp.sum(hidden * h, axis=1, keepdims=True)
            gsus[rows, at:at + 128] = g_side.astype(BF)
            gsus[rows, SIDE_HID + at:SIDE_HID + at + 128] = u_side.astype(BF)
            hid_t[at:at + 128, rows] = hidden.T.astype(BF)
            gsus_t[at:at + 128, rows] = g_side.T.astype(BF)
            gsus_t[SIDE_HID + at:SIDE_HID + at + 128, rows] = u_side.T.astype(BF)
        part_r[rows, :] = jnp.broadcast_to(value, (128, 128)).astype(BF)
        return carry

    lax.fori_loop(0, 6, gates, 0)

    def e_copy(n, feature, c):
        if feature:
            return remote(s_f.at[c], tpr.at[c], e_send.at[n], e_recv.at[n], other_core)
        return remote(part_r, tpr_r, e_send.at[n], e_recv.at[n], other_core)

    def pick(feature, c, f_ref, r_ref):
        return f_ref.at[c] if feature else r_ref

    def a_copy(n, feature, c, i):
        s, xa = pick(feature, c, s_f, s_r), pick(feature, c, xa_f, xa_r)
        at = pl.ds(((x + 2) % 4) * 192 + 96 * i, 96)
        return remote(
            s.at[at], xa.at[i], a_send.at[int(feature)], a_recv.at[n], right if i == 0 else left
        )

    def b_copy(n, feature, c, i):
        s, xb = pick(feature, c, s_f, s_r), pick(feature, c, xb_f, xb_r)
        at = pl.ds(((x + 1 + 2 * i) % 4) * 192, 192)
        return remote(
            s.at[at], xb.at[i], b_send.at[int(feature)], b_recv.at[n], right if i == 0 else left
        )

    def v_copy(n, feature, c, i):
        s, yr = pick(feature, c, s_f, s_r), pick(feature, c, yr_f, yr_r)
        at = pl.ds(block(x, y_peers[i]), BUNDLE)
        return remote(
            s.at[at], yr.at[i], v_send.at[int(feature)], v_recv.at[n], chip(z, y_peers[i], x)
        )

    def q_copy(n, feature, c, i):
        zs, zr = pick(feature, c, zs_f, zs_r), pick(feature, c, zr_f, zr_r)
        return remote(
            zs.at[z_peers[i]], zr.at[i], q_send.at[int(feature)], q_recv.at[n], chip(z_peers[i], y, x)
        )

    def half_lanes(c):
        return pl.ds(pl.multiple_of((c % 2) * LANES, LANES), LANES)

    def stage_core(n, feature, c):
        if not feature:
            e_copy(n, False, c).start()
            return
        k = (1 - core) * nc + c
        for m in range(3):
            rows = pl.ds(m * 256, 256)
            s_f[c, rows, :] = dot_nn(gsus[rows, :], wc[k]).astype(BF)
        e_copy(n, True, c).start()
        k = core * nc + c
        for m in range(3):
            rows = pl.ds(m * 256, 256)
            pre[rows, half_lanes(c)] = dot_nn(gsus[rows, :], wc[k])

    def stage_a(n, feature, c):
        e_copy(n, feature, c).wait()
        s = pick(feature, c, s_f, s_r)
        theirs = pick(feature, c, tpr, tpr_r)
        for m in range(3):
            rows = pl.ds(m * 256, 256)
            mine = pre[rows, half_lanes(c)] if feature else part_r[rows, :].astype(F32)
            s[rows, :] = (mine + theirs[rows, :].astype(F32)).astype(BF)
        for i in range(2):
            a_copy(n, feature, c, i).start()

    def stage_b(n, feature, c):
        s, xa = pick(feature, c, s_f, s_r), pick(feature, c, xa_f, xa_r)
        settle(xa, a_recv.at[n])
        for i in range(2):
            at = pl.ds(pl.multiple_of(((x + 1 + 2 * i) % 4) * 192 + 96 * i, 96), 96)
            s[at, :] = (s[at, :].astype(F32) + xa[i].astype(F32)).astype(BF)
        for i in range(2):
            b_copy(n, feature, c, i).start()

    def stage_v(n, feature, c):
        s, xb = pick(feature, c, s_f, s_r), pick(feature, c, xb_f, xb_r)
        settle(xb, b_recv.at[n])
        at = pl.ds(pl.multiple_of(x * 192, 192), 192)
        s[at, :] = (s[at, :].astype(F32) + xb[0].astype(F32) + xb[1].astype(F32)).astype(BF)
        for i in range(3):
            v_copy(n, feature, c, i).start()

    def stage_q(n, feature, c):
        s, yr = pick(feature, c, s_f, s_r), pick(feature, c, yr_f, yr_r)
        zs = pick(feature, c, zs_f, zs_r)
        settle(yr, v_recv.at[n])
        at = pl.ds(pl.multiple_of(block(x, y), BUNDLE), BUNDLE)
        mine = (s[at, :].astype(F32) + yr[0].astype(F32)).astype(BF)
        theirs = (yr[1].astype(F32) + yr[2].astype(F32)).astype(BF)
        slots = jnp.concatenate(
            [mine, theirs, jnp.zeros((128 - 2 * BUNDLE, mine.shape[1]), BF)], axis=0
        )
        if feature:
            rows = dot_nn(place_t[0], slots)
        else:
            lane = lax.broadcasted_iota(jnp.int32, (SIDE * ROWS, 128), 1)
            rows = jnp.where(
                lane == 0,
                dot_nn(place_t[1], slots),
                dot_nn(place_t[2], slots),
            )
        zs[...] = rows.astype(BF).reshape(zs.shape)
        for i in range(3):
            q_copy(n, feature, c, i).start()

    def stage_out(n, feature, c):
        zs, zr = pick(feature, c, zs_f, zs_r), pick(feature, c, zr_f, zr_r)
        settle(zr, q_recv.at[n])
        total = zs[z].astype(F32)
        for i in range(3):
            total = total + zr[i].astype(F32)
        if feature:
            out_tok[:, pl.ds(pl.multiple_of(c * LANES, LANES), LANES)] = total[:24].astype(BF)
        else:
            turned = jnp.concatenate([total, jnp.zeros((128 - ROWS, 128), F32)], axis=0).T
            out_rg[...] = turned[0:TOP, 0:rows_dev] / weights[...]

    def out_copies(k):
        at = pl.ds(pl.multiple_of(k * LANES, LANES), LANES)
        return (
            pltpu.make_async_copy(wc.at[k, pl.ds(0, hid)], out_gate.at[0, :, at], o_sem.at[0]),
            pltpu.make_async_copy(wc.at[k, pl.ds(SIDE_HID, hid)], out_up.at[0, :, at], o_sem.at[1]),
            pltpu.make_async_copy(wd.at[k], out_down.at[0, :, at], o_sem.at[2]),
        )

    def weight_grads(k):
        for m in range(3):
            rows = pl.ds(m * 256, 256)
            wc[k, rows, :] = dot_nn(gsus_t[rows, :], xc[k, 0]).astype(BF)
        wd[k] = dot_nn(hid_t[:hid], xc[k, 1]).astype(BF)
        for cp in out_copies(k):
            cp.start()

    stages = (stage_core, stage_a, stage_b, stage_v, stage_q, stage_out)

    def give_back(t, carry):
        for depth, stage in zip(BACK_AT, stages):
            n = t - depth

            @pl.when(n == 0)
            def _():
                stage(0, False, 0)

            @pl.when((n >= 1) & (n <= nc))
            def _():
                stage(n, True, n - 1)

        @pl.when((t >= GRADS_AT) & (t < nc + GRADS_AT))
        def _():
            weight_grads(core * nc + t - GRADS_AT)
            weight_grads((1 - core) * nc + t - GRADS_AT)

        return carry

    lax.fori_loop(0, nc + 1 + BACK_AT[-1], give_back, 0)

    settle(iz.at[pl.ds(0, 3)], i_send.at[0])
    settle(xc.at[0, :, pl.ds(0, 3 * rows_dev * nc)], z_send.at[0])
    settle(xc.at[0], y_send.at[0])
    settle(xc.at[pl.ds(0, 2)], x_send.at[0])
    settle(xc.at[0], x_send.at[1])
    settle(xc.at[0], x_send.at[2])
    settle(xc.at[0, 0], x_send.at[3])
    settle(xc.at[pl.ds(0, 2)], p_send.at[0])
    settle(xc.at[pl.ds(0, nc)], d_send.at[0])
    for sem, ref_r, ref_f in (
        (a_send, xa_r, xa_f), (b_send, xb_r, xb_f), (v_send, yr_r, yr_f), (q_send, zr_r, zr_f)
    ):
        settle(ref_r, sem.at[0])
        settle(ref_f, sem.at[1])
    settle(out_gate.at[0], o_sem.at[0])
    settle(out_up.at[0], o_sem.at[1])
    settle(out_down.at[0], o_sem.at[2])


def out_kernel(*refs):
    count = (len(refs) - 1) // 2
    sem = refs[-1]
    copies = []
    for i in range(count):
        copies.append(pltpu.make_async_copy(refs[i], refs[count + i], sem.at[i]))
    for cp in copies:
        cp.start()
    for cp in copies:
        cp.wait()


def in_hbm(a):
    return pltpu.with_memory_space_constraint(a, pltpu.HBM)


def put_out(*arrays):
    return pl.pallas_call(
        out_kernel,
        out_shape=tuple(jax.ShapeDtypeStruct(a.shape, a.dtype) for a in arrays),
        in_specs=[pl.BlockSpec(memory_space=pl.ANY)] * len(arrays),
        out_specs=(pl.BlockSpec(memory_space=pl.ANY),) * len(arrays),
        scratch_shapes=[pltpu.SemaphoreType.DMA((len(arrays),))],
        compiler_params=pltpu.CompilerParams(vmem_limit_bytes=43 * 1024 * 1024),
    )(*arrays)


def per_device(tokens, cotangent, routes, route_weights, gate_weight, up_weight, down_weight):
    rows, width = tokens.shape
    half = width // lax.axis_size("tp")
    nc = half // LANES
    hid = gate_weight.shape[2]
    vmem, anywhere = pltpu.VMEM, pl.ANY
    slots = 16 * BUNDLE

    def chunk_buffers(lead, lanes):
        return [
            vmem((*lead, slots, lanes), BF),
            vmem((*lead, 2, 96, lanes), BF),
            vmem((*lead, 2, 192, lanes), BF),
            vmem((*lead, 3, BUNDLE, lanes), BF),
            vmem((*lead, SIDE, ROWS, lanes), BF),
            vmem((*lead, 3, ROWS, lanes), BF),
        ]

    dma = pltpu.SemaphoreType.DMA
    token_grad, shares, gate_grad, up_grad, down_grad = pl.pallas_call(
        functools.partial(kernel, nc, hid),
        out_shape=(
            jax.ShapeDtypeStruct((rows, half), BF),
            jax.ShapeDtypeStruct((TOP, rows), F32),
            jax.ShapeDtypeStruct((1, hid, width), BF),
            jax.ShapeDtypeStruct((1, hid, width), BF),
            jax.ShapeDtypeStruct(down_weight.shape, BF),
        ),
        in_specs=[
            pl.BlockSpec(memory_space=anywhere),
            pl.BlockSpec(memory_space=anywhere),
            pl.BlockSpec(memory_space=anywhere),
            pl.BlockSpec(memory_space=anywhere),
            pl.BlockSpec(memory_space=anywhere),
            pl.BlockSpec(memory_space=anywhere),
            pl.BlockSpec(memory_space=anywhere),
        ],
        out_specs=(
            pl.BlockSpec(memory_space=vmem),
            pl.BlockSpec(memory_space=vmem),
            pl.BlockSpec(memory_space=anywhere),
            pl.BlockSpec(memory_space=anywhere),
            pl.BlockSpec(memory_space=anywhere),
        ),
        scratch_shapes=[
            vmem((TOP, rows), jnp.int32),
            vmem((TOP, rows), F32),
            vmem((nc, SIDE, 2, ROWS, LANES), BF),
            vmem((3, EXPERTS, 128), F32),
            vmem((SIDE, 3, EXPERTS, 128), F32),
            vmem((3, EXPERTS, 128), F32),
            vmem((2 * nc, 2, slots, LANES), BF),
            vmem((nc, 2, BUNDLE, LANES), BF),
            vmem((128, 128), BF),
            vmem((128, 128), F32),
            vmem((3, 128, 128), BF),
            vmem((2 * BUNDLE, 128), F32),
            vmem((2 * nc, hid, LANES), BF),
            vmem((2 * nc, 2 * SIDE_HID, LANES), BF),
            vmem((slots, 2 * SIDE_HID), F32),
            vmem((slots, SIDE_HID), F32),
            vmem((slots, 2 * SIDE_HID), BF),
            vmem((2 * SIDE_HID, slots), BF),
            vmem((SIDE_HID, slots), BF),
            vmem((nc, slots, LANES), BF),
            vmem((nc, slots, LANES), BF),
            *chunk_buffers((nc,), LANES)[1:],
            vmem((slots, 128), BF),
            vmem((slots, 128), BF),
            *chunk_buffers((), 128),
            dma((5,)),
            dma((1,)), dma((nc,)),
            dma((1,)), dma((1,)),
            dma((1,)), dma((nc, 2)),
            dma((4,)), dma((nc, 4)),
            dma((1,)), dma((nc,)),
            dma((1,)), dma((nc,)),
            dma((nc + 1,)), dma((nc + 1,)),
            dma((2,)), dma((nc + 1,)),
            dma((2,)), dma((nc + 1,)),
            dma((2,)), dma((nc + 1,)),
            dma((2,)), dma((nc + 1,)),
            dma((3,)),
        ],
        compiler_params=pltpu.CompilerParams(
            collective_id=0, has_side_effects=True, vmem_limit_bytes=43 * 1024 * 1024
        ),
    )(
        in_hbm(tokens), in_hbm(cotangent), in_hbm(routes.T), in_hbm(route_weights.T),
        in_hbm(gate_weight.transpose(0, 2, 1)), in_hbm(up_weight.transpose(0, 2, 1)),
        in_hbm(down_weight),
    )
    token_grad, shares, gate_grad, up_grad, down_grad = put_out(
        token_grad, shares, gate_grad, up_grad, down_grad
    )
    return token_grad, shares.T, gate_grad.transpose(0, 2, 1), up_grad.transpose(0, 2, 1), down_grad


def solution(mesh):
    return jax.shard_map(
        per_device,
        mesh=mesh,
        in_specs=(
            P("ep", None),
            P("ep", None),
            P("ep", None),
            P("ep", None),
            P("ep", None, "tp"),
            P("ep", None, "tp"),
            P("ep", "tp", None),
        ),
        out_specs=(
            P("ep", "tp"),
            P("ep", None),
            P("ep", None, "tp"),
            P("ep", None, "tp"),
            P("ep", "tp", None),
        ),
        check_vma=False,
    )
```

```python
import functools

import jax
import jax.numpy as jnp
from jax import lax
from jax.experimental import pallas as pl
from jax.experimental.pallas import tpu as pltpu
from jax.sharding import PartitionSpec as P

EXPERTS = 8
TOP = 2
CAP = 12
SIDE = 4
ROWS = 32
BUNDLE = 48
LANES = 256
AHEAD = 4
AT = (2, 3, 4, 5, 6)
BACK_AT = (0, 1, 3, 5, 7, 9)
GRADS_AT = 5
SIDE_HID = 384
BF = jnp.bfloat16
F32 = jnp.float32
MESH = pl.DeviceIdType.MESH


def dot_nt(a, b):
    return lax.dot_general(a, b, (((1,), (1,)), ((), ())), preferred_element_type=F32)


def dot_tn(a, b):
    return lax.dot_general(a, b, (((0,), (0,)), ((), ())), preferred_element_type=F32)


def dot_nn(a, b):
    return jnp.dot(a, b, preferred_element_type=F32)


def kernel(
    nc, hid,
    tokens, cotangent, routes_in, weights_in, gate, up, down,
    out_tok, out_rg, out_gate, out_up, out_down,
    routes, weights, tz, info, iz, codes, xc, ob, place, firsts, place_t, share,
    wd, wc, pre, hg, gsus, gsus_t, hid_t,
    s_f, tpr, xa_f, xb_f, yr_f, zs_f, zr_f,
    part_r, tpr_r, s_r, xa_r, xb_r, yr_r, zs_r, zr_r,
    w_sem, z_send, z_recv, i_send, i_recv, y_send, y_recv, x_send, x_recv, p_send, p_recv, d_send, d_recv,
    e_send, e_recv, a_send, a_recv, b_send, b_recv, v_send, v_recv, q_send, q_recv,
    o_sem,
):
    ep = lax.axis_index("ep")
    core = lax.axis_index("tp")
    z, y, x = ep // 16, (ep // 4) % 4, ep % 4
    pair = y // 2

    def chip(zz, yy, xx):
        return (zz * 16 + yy * 4 + xx, core)

    right = chip(z, y, (x + 1) % 4)
    left = chip(z, y, (x + 3) % 4)
    other_core = (ep, 1 - core)
    partner_y = 2 * pair + (1 - y % 2)
    cross_y = 3 - y
    cross2_y = 2 * (1 - pair) + y % 2
    y_peers = [partner_y, cross_y, cross2_y]
    z_peers = [(z + 1) % 4, (z + 3) % 4, (z + 2) % 4]

    rows_dev = tokens.shape[0]
    half_of = ((y + 1) // 2) % 2

    def block(xs, ys):
        return xs * 192 + (((ys + 1) // 2) % 2) * 96 + (ys // 2) * BUNDLE

    small = [
        pltpu.make_async_copy(routes_in, routes, w_sem.at[3]),
        pltpu.make_async_copy(weights_in, weights, w_sem.at[4]),
    ]
    for cp in small:
        cp.start()

    def pad_rows(c, carry):
        tz[c, :, :, rows_dev:, :] = jnp.zeros((SIDE, 2, ROWS - rows_dev, LANES), BF)
        return carry

    lax.fori_loop(0, nc, pad_rows, 0)

    barrier = pltpu.get_barrier_semaphore()
    for zz in z_peers:
        pl.semaphore_signal(barrier, inc=1, device_id=chip(zz, y, x), device_id_type=MESH)
    for yy in y_peers:
        pl.semaphore_signal(barrier, inc=1, device_id=chip(z, yy, x), device_id_type=MESH)
    for dev in (right, left, other_core):
        pl.semaphore_signal(barrier, inc=1, device_id=dev, device_id_type=MESH)

    w_copies = []
    for k in range(2 * nc):
        at = pl.ds(k * LANES, LANES)
        w_copies += [
            pltpu.make_async_copy(gate.at[0, :, at], wc.at[k, pl.ds(0, hid)], w_sem.at[0]),
            pltpu.make_async_copy(up.at[0, :, at], wc.at[k, pl.ds(SIDE_HID, hid)], w_sem.at[1]),
            pltpu.make_async_copy(down.at[0, :, at], wd.at[k], w_sem.at[2]),
        ]
    for cp in w_copies:
        cp.start()

    def remote(a, b, ss, rs, dev):
        return pltpu.make_async_remote_copy(
            src_ref=a, dst_ref=b, send_sem=ss, recv_sem=rs, device_id=dev, device_id_type=MESH
        )

    def settle(ref, sem):
        pltpu.make_async_copy(ref, ref, sem).wait()

    def some(n):
        return xc.at[0, 0, pl.ds(0, n)]

    def piece(ref, c):
        return ref.at[:, pl.ds(pl.multiple_of((core * nc + c) * LANES, LANES), LANES)]

    def landing(c, tensor):
        return tz.at[c, z, tensor, pl.ds(0, rows_dev)]

    def z_copy(c, i, tensor):
        return remote(
            piece(cotangent if tensor else tokens, c), landing(c, tensor),
            z_send.at[0], z_recv.at[c], chip(z_peers[i], y, x),
        )

    def own_copy(c, tensor):
        return pltpu.make_async_copy(
            piece(cotangent if tensor else tokens, c), landing(c, tensor), z_recv.at[c]
        )

    def zi_copy(i):
        return remote(info, iz.at[z], i_send.at[0], i_recv.at[0], chip(z_peers[i], y, x))

    def start_z(c):
        for tensor in range(2):
            for i in range(3):
                z_copy(c, i, tensor).start()
            own_copy(c, tensor).start()

    for cp in small:
        cp.wait()
    expert_row = lax.broadcasted_iota(jnp.int32, (EXPERTS, rows_dev), 0)
    hot = [expert_row == routes[k:k + 1, :] for k in range(2)]
    hit = jnp.where(hot[0] | hot[1], 1.0, 0.0).astype(BF)
    before = jnp.where(
        lax.broadcasted_iota(jnp.int32, (rows_dev, rows_dev), 0)
        < lax.broadcasted_iota(jnp.int32, (rows_dev, rows_dev), 1),
        1.0, 0.0,
    ).astype(BF)
    code = dot_nn(hit, before) + (z * CAP + 1).astype(F32)
    info[...] = jnp.zeros_like(info)
    for k in range(2):
        info[k, :, 0:rows_dev] = jnp.where(hot[k], code, 0.0)
    info[2, :, 0:rows_dev] = jnp.where(hot[0], weights[0:1, :], 0.0) + jnp.where(
        hot[1], weights[1:2, :], 0.0
    )
    iz[z] = info[...]
    pre[...] = jnp.zeros_like(pre)
    hg[...] = jnp.zeros_like(hg)

    def blank(k, carry):
        for at in (hid, SIDE_HID + hid):
            wc[k, at:at + SIDE_HID - hid, :] = jnp.zeros((SIDE_HID - hid, LANES), BF)
        return carry

    lax.fori_loop(0, 2 * nc, blank, 0)

    pl.semaphore_wait(barrier, 9)
    for i in range(3):
        zi_copy(i).start()
    for c in range(AHEAD):
        start_z(c)
    settle(iz.at[pl.ds(0, 3)], i_recv.at[0])
    for kind in range(3):
        total = iz[0, kind]
        for zz in range(1, SIDE):
            total = total + pltpu.roll(iz[zz, kind], zz * ROWS, 1)
        codes[kind] = total

    slot_number = lax.broadcasted_iota(jnp.int32, (BUNDLE, 128), 0).astype(F32) + 1.0

    def info_row(kind, expert):
        return codes[kind, pl.ds(expert, 1), :]

    spare = jnp.zeros((128 - 2 * BUNDLE, 128), F32)
    first, second = [], []
    for side, expert in ((0, 2 * z + pair), (1, 2 * z + 1 - pair)):
        first.append(jnp.where(slot_number == info_row(0, expert), 1.0, 0.0))
        second.append(jnp.where(slot_number == info_row(1, expert), 1.0, 0.0))
        share[side * BUNDLE:(side + 1) * BUNDLE, :] = jnp.broadcast_to(
            jnp.sum((first[side] + second[side]) * info_row(2, expert), axis=1, keepdims=True),
            (BUNDLE, 128),
        )
    first = jnp.concatenate(first + [spare], axis=0)
    second = jnp.concatenate(second + [spare], axis=0)
    place[...] = (first + second).astype(BF)
    firsts[...] = first

    def y_copy(c, i):
        k = core * nc + c
        at = pl.ds(block(x, y), BUNDLE)
        tensor = 1 if i == 3 else 0
        peer = cross_y if i == 3 else y_peers[i]
        from_ref = xc.at[k, 0, at, :] if i == 0 else ob.at[c, tensor]
        return remote(
            from_ref, xc.at[k, tensor, at, :], y_send.at[0], y_recv.at[c, tensor], chip(z, peer, x)
        )

    def x_copy(c, i):
        k = core * nc + c
        tensor = i // 4
        step = i % 4
        size, base = (96, half_of * 96) if tensor else (192, 0)
        if step < 2:
            at = pl.ds(x * 192 + base, size)
        elif step == 2:
            at = pl.ds(((x + 3) % 4) * 192 + base, size // 2)
        else:
            at = pl.ds(((x + 1) % 4) * 192 + base + size // 2, size // 2)
        ref = xc.at[k, tensor, at, :]
        return remote(
            ref, ref, x_send.at[i // 2], x_recv.at[c, i // 2], right if i % 2 == 0 else left
        )

    def p_copy(c, i):
        at = pl.ds(((x + (0, 3, 1, 2)[i]) % 4) * 192 + half_of * 96, 96)
        ref = xc.at[core * nc + c, 1, at, :]
        return remote(ref, ref, p_send.at[0], p_recv.at[c], chip(z, partner_y, x))

    def d_copy(c, k, tensor):
        ref = xc.at[k, tensor]
        return remote(ref, ref, d_send.at[0], d_recv.at[c], other_core)

    def compact(c):
        settle(some(8 * rows_dev), z_recv.at[c])

        @pl.when(c + AHEAD < nc)
        def _():
            start_z(c + AHEAD)

        k = core * nc + c
        at = pl.ds(pl.multiple_of(block(x, y), BUNDLE), BUNDLE)
        for tensor in (1, 0):
            rows = dot_nn(place[:2 * BUNDLE], tz[c, :, tensor].reshape(SIDE * ROWS, LANES))
            if tensor == 1:
                rows = rows * share[:, 0:1]
            rows = rows.astype(BF)
            xc[k, tensor, at, :] = rows[:BUNDLE]
            ob[c, tensor] = rows[BUNDLE:]
            for i in ((3,) if tensor else (0, 1, 2)):
                y_copy(c, i).start()

    def products(k):
        for m in range(3):
            rows = pl.ds(m * 256, 256)
            pre[rows, :] += dot_nt(xc[k, 0, rows, :], wc[k])
            hg[rows, :hid] += dot_nt(xc[k, 1, rows, :], wd[k])

    def dispatch(t, carry):
        @pl.when(t < nc)
        def _():
            compact(t)

        @pl.when((t >= AT[0]) & (t < nc + AT[0]))
        def _():
            c = t - AT[0]
            settle(some(BUNDLE), y_recv.at[c, 1])
            x_copy(c, 4).start()
            x_copy(c, 5).start()
            p_copy(c, 0).start()
            settle(some(3 * BUNDLE), y_recv.at[c, 0])
            x_copy(c, 0).start()
            x_copy(c, 1).start()

        @pl.when(t == 1)
        def _():
            settle(gate.at[0], w_sem.at[0])
            settle(up.at[0], w_sem.at[1])
            settle(down.at[0], w_sem.at[2])

        @pl.when((t >= AT[1]) & (t < nc + AT[1]))
        def _():
            c = t - AT[1]
            settle(some(192), x_recv.at[c, 2])
            for side in range(2):
                x_copy(c, 6 + side).start()
                p_copy(c, 1 + side).start()
            settle(some(384), x_recv.at[c, 0])
            for side in range(2):
                x_copy(c, 2 + side).start()

        @pl.when((t >= AT[2]) & (t < nc + AT[2]))
        def _():
            c = t - AT[2]
            settle(some(96), x_recv.at[c, 3])
            p_copy(c, 3).start()
            settle(some(192), x_recv.at[c, 1])
            d_copy(c, core * nc + c, 0).start()

        @pl.when((t >= AT[3]) & (t < nc + AT[3]))
        def _():
            c = t - AT[3]
            settle(some(384), p_recv.at[c])
            d_copy(c, core * nc + c, 1).start()
            products(core * nc + c)

        @pl.when(t >= AT[4])
        def _():
            c = t - AT[4]
            settle(xc.at[0], d_recv.at[c])
            products((1 - core) * nc + c)

        return carry

    lax.fori_loop(0, nc + AT[4], dispatch, 0)

    def gates(m, carry):
        rows = pl.ds(pl.multiple_of(m * 128, 128), 128)
        value = jnp.zeros((128, 1), F32)
        for at in range(0, SIDE_HID, 128):
            g = pre[rows, at:at + 128]
            u = pre[rows, SIDE_HID + at:SIDE_HID + at + 128]
            h = hg[rows, at:at + 128]
            s = jax.nn.sigmoid(g)
            active = g * s
            hidden = (active * u).astype(BF).astype(F32)
            g_side = h * u * (s * (1.0 + g * (1.0 - s)))
            u_side = h * active
            value = value + jnp.sum(hidden * h, axis=1, keepdims=True)
            gsus[rows, at:at + 128] = g_side.astype(BF)
            gsus[rows, SIDE_HID + at:SIDE_HID + at + 128] = u_side.astype(BF)
            hid_t[at:at + 128, rows] = hidden.T.astype(BF)
            gsus_t[at:at + 128, rows] = g_side.T.astype(BF)
            gsus_t[SIDE_HID + at:SIDE_HID + at + 128, rows] = u_side.T.astype(BF)
        part_r[rows, :] = jnp.broadcast_to(value, (128, 128)).astype(BF)
        return carry

    lax.fori_loop(0, 6, gates, 0)

    def e_copy(n, feature, c):
        if feature:
            return remote(s_f.at[c], tpr.at[c], e_send.at[n], e_recv.at[n], other_core)
        return remote(part_r, tpr_r, e_send.at[n], e_recv.at[n], other_core)

    def pick(feature, c, f_ref, r_ref):
        return f_ref.at[c] if feature else r_ref

    def a_copy(n, feature, c, i):
        s, xa = pick(feature, c, s_f, s_r), pick(feature, c, xa_f, xa_r)
        at = pl.ds(((x + 2) % 4) * 192 + 96 * i, 96)
        return remote(
            s.at[at], xa.at[i], a_send.at[int(feature)], a_recv.at[n], right if i == 0 else left
        )

    def b_copy(n, feature, c, i):
        s, xb = pick(feature, c, s_f, s_r), pick(feature, c, xb_f, xb_r)
        at = pl.ds(((x + 1 + 2 * i) % 4) * 192, 192)
        return remote(
            s.at[at], xb.at[i], b_send.at[int(feature)], b_recv.at[n], right if i == 0 else left
        )

    def v_copy(n, feature, c, i):
        s, yr = pick(feature, c, s_f, s_r), pick(feature, c, yr_f, yr_r)
        at = pl.ds(block(x, y_peers[i]), BUNDLE)
        return remote(
            s.at[at], yr.at[i], v_send.at[int(feature)], v_recv.at[n], chip(z, y_peers[i], x)
        )

    def q_copy(n, feature, c, i):
        zs, zr = pick(feature, c, zs_f, zs_r), pick(feature, c, zr_f, zr_r)
        return remote(
            zs.at[z_peers[i]], zr.at[i], q_send.at[int(feature)], q_recv.at[n], chip(z_peers[i], y, x)
        )

    def half_lanes(c):
        return pl.ds(pl.multiple_of((c % 2) * LANES, LANES), LANES)

    def stage_core(n, feature, c):
        if not feature:
            e_copy(n, False, c).start()
            return
        k = (1 - core) * nc + c
        for m in range(3):
            rows = pl.ds(m * 256, 256)
            s_f[c, rows, :] = dot_nn(gsus[rows, :], wc[k]).astype(BF)
        e_copy(n, True, c).start()
        k = core * nc + c
        for m in range(3):
            rows = pl.ds(m * 256, 256)
            pre[rows, half_lanes(c)] = dot_nn(gsus[rows, :], wc[k])

    def stage_a(n, feature, c):
        e_copy(n, feature, c).wait()
        s = pick(feature, c, s_f, s_r)
        theirs = pick(feature, c, tpr, tpr_r)
        for m in range(3):
            rows = pl.ds(m * 256, 256)
            mine = pre[rows, half_lanes(c)] if feature else part_r[rows, :].astype(F32)
            s[rows, :] = (mine + theirs[rows, :].astype(F32)).astype(BF)
        for i in range(2):
            a_copy(n, feature, c, i).start()

    def stage_b(n, feature, c):
        s, xa = pick(feature, c, s_f, s_r), pick(feature, c, xa_f, xa_r)
        settle(xa, a_recv.at[n])
        for i in range(2):
            at = pl.ds(pl.multiple_of(((x + 1 + 2 * i) % 4) * 192 + 96 * i, 96), 96)
            s[at, :] = (s[at, :].astype(F32) + xa[i].astype(F32)).astype(BF)
        for i in range(2):
            b_copy(n, feature, c, i).start()

    def stage_v(n, feature, c):
        s, xb = pick(feature, c, s_f, s_r), pick(feature, c, xb_f, xb_r)
        settle(xb, b_recv.at[n])
        at = pl.ds(pl.multiple_of(x * 192, 192), 192)
        s[at, :] = (s[at, :].astype(F32) + xb[0].astype(F32) + xb[1].astype(F32)).astype(BF)
        for i in range(3):
            v_copy(n, feature, c, i).start()

    def stage_q(n, feature, c):
        s, yr = pick(feature, c, s_f, s_r), pick(feature, c, yr_f, yr_r)
        zs = pick(feature, c, zs_f, zs_r)
        settle(yr, v_recv.at[n])
        at = pl.ds(pl.multiple_of(block(x, y), BUNDLE), BUNDLE)
        mine = (s[at, :].astype(F32) + yr[0].astype(F32)).astype(BF)
        theirs = (yr[1].astype(F32) + yr[2].astype(F32)).astype(BF)
        slots = jnp.concatenate(
            [mine, theirs, jnp.zeros((128 - 2 * BUNDLE, mine.shape[1]), BF)], axis=0
        )
        if feature:
            rows = dot_nn(place_t[0], slots)
        else:
            lane = lax.broadcasted_iota(jnp.int32, (SIDE * ROWS, 128), 1)
            rows = jnp.where(
                lane == 0,
                dot_nn(place_t[1], slots),
                dot_nn(place_t[2], slots),
            )
        zs[...] = rows.astype(BF).reshape(zs.shape)
        for i in range(3):
            q_copy(n, feature, c, i).start()

    def stage_out(n, feature, c):
        zs, zr = pick(feature, c, zs_f, zs_r), pick(feature, c, zr_f, zr_r)
        settle(zr, q_recv.at[n])
        total = zs[z].astype(F32)
        for i in range(3):
            total = total + zr[i].astype(F32)
        if feature:
            out_tok[:, pl.ds(pl.multiple_of(c * LANES, LANES), LANES)] = total[:24].astype(BF)
        else:
            turned = jnp.concatenate([total, jnp.zeros((128 - ROWS, 128), F32)], axis=0).T
            out_rg[...] = turned[0:TOP, 0:rows_dev] / weights[...]

    def out_copies(k):
        at = pl.ds(pl.multiple_of(k * LANES, LANES), LANES)
        return (
            pltpu.make_async_copy(wc.at[k, pl.ds(0, hid)], out_gate.at[0, :, at], o_sem.at[0]),
            pltpu.make_async_copy(wc.at[k, pl.ds(SIDE_HID, hid)], out_up.at[0, :, at], o_sem.at[1]),
            pltpu.make_async_copy(wd.at[k], out_down.at[0, :, at], o_sem.at[2]),
        )

    def weight_grads(k):
        for m in range(3):
            rows = pl.ds(m * 256, 256)
            wc[k, rows, :] = dot_nn(gsus_t[rows, :], xc[k, 0]).astype(BF)
        wd[k] = dot_nn(hid_t[:hid], xc[k, 1]).astype(BF)
        for cp in out_copies(k):
            cp.start()

    stages = (stage_core, stage_a, stage_b, stage_v, stage_q, stage_out)

    def give_back(t, carry):
        for depth, stage in zip(BACK_AT, stages):
            n = t - depth

            @pl.when(n == 0)
            def _():
                stage(0, False, 0)

            @pl.when((n >= 1) & (n <= nc))
            def _():
                stage(n, True, n - 1)

        @pl.when(t == 2)
        def _():
            first = firsts[...]
            place_t[0] = place[...].astype(F32).T.astype(BF)
            place_t[1] = first.T.astype(BF)
            place_t[2] = (place[...].astype(F32) - first).T.astype(BF)

        @pl.when((t >= GRADS_AT) & (t < nc + GRADS_AT))
        def _():
            weight_grads(core * nc + t - GRADS_AT)
            weight_grads((1 - core) * nc + t - GRADS_AT)

        return carry

    lax.fori_loop(0, nc + 1 + BACK_AT[-1], give_back, 0)

    settle(iz.at[pl.ds(0, 3)], i_send.at[0])
    settle(xc.at[0, :, pl.ds(0, 3 * rows_dev * nc)], z_send.at[0])
    settle(xc.at[0], y_send.at[0])
    settle(xc.at[pl.ds(0, 2)], x_send.at[0])
    settle(xc.at[0], x_send.at[1])
    settle(xc.at[0], x_send.at[2])
    settle(xc.at[0, 0], x_send.at[3])
    settle(xc.at[pl.ds(0, 2)], p_send.at[0])
    settle(xc.at[pl.ds(0, nc)], d_send.at[0])
    for sem, ref_r, ref_f in (
        (a_send, xa_r, xa_f), (b_send, xb_r, xb_f), (v_send, yr_r, yr_f), (q_send, zr_r, zr_f)
    ):
        settle(ref_r, sem.at[0])
        settle(ref_f, sem.at[1])
    settle(out_gate.at[0], o_sem.at[0])
    settle(out_up.at[0], o_sem.at[1])
    settle(out_down.at[0], o_sem.at[2])


def out_kernel(*refs):
    count = (len(refs) - 1) // 2
    sem = refs[-1]
    copies = []
    for i in range(count):
        copies.append(pltpu.make_async_copy(refs[i], refs[count + i], sem.at[i]))
    for cp in copies:
        cp.start()
    for cp in copies:
        cp.wait()


def in_hbm(a):
    return pltpu.with_memory_space_constraint(a, pltpu.HBM)


def put_out(*arrays):
    return pl.pallas_call(
        out_kernel,
        out_shape=tuple(jax.ShapeDtypeStruct(a.shape, a.dtype) for a in arrays),
        in_specs=[pl.BlockSpec(memory_space=pl.ANY)] * len(arrays),
        out_specs=(pl.BlockSpec(memory_space=pl.ANY),) * len(arrays),
        scratch_shapes=[pltpu.SemaphoreType.DMA((len(arrays),))],
        compiler_params=pltpu.CompilerParams(vmem_limit_bytes=43 * 1024 * 1024),
    )(*arrays)


def per_device(tokens, cotangent, routes, route_weights, gate_weight, up_weight, down_weight):
    rows, width = tokens.shape
    half = width // lax.axis_size("tp")
    nc = half // LANES
    hid = gate_weight.shape[2]
    vmem, anywhere = pltpu.VMEM, pl.ANY
    slots = 16 * BUNDLE

    def chunk_buffers(lead, lanes):
        return [
            vmem((*lead, slots, lanes), BF),
            vmem((*lead, 2, 96, lanes), BF),
            vmem((*lead, 2, 192, lanes), BF),
            vmem((*lead, 3, BUNDLE, lanes), BF),
            vmem((*lead, SIDE, ROWS, lanes), BF),
            vmem((*lead, 3, ROWS, lanes), BF),
        ]

    dma = pltpu.SemaphoreType.DMA
    token_grad, shares, gate_grad, up_grad, down_grad = pl.pallas_call(
        functools.partial(kernel, nc, hid),
        out_shape=(
            jax.ShapeDtypeStruct((rows, half), BF),
            jax.ShapeDtypeStruct((TOP, rows), F32),
            jax.ShapeDtypeStruct((1, hid, width), BF),
            jax.ShapeDtypeStruct((1, hid, width), BF),
            jax.ShapeDtypeStruct(down_weight.shape, BF),
        ),
        in_specs=[
            pl.BlockSpec(memory_space=anywhere),
            pl.BlockSpec(memory_space=anywhere),
            pl.BlockSpec(memory_space=anywhere),
            pl.BlockSpec(memory_space=anywhere),
            pl.BlockSpec(memory_space=anywhere),
            pl.BlockSpec(memory_space=anywhere),
            pl.BlockSpec(memory_space=anywhere),
        ],
        out_specs=(
            pl.BlockSpec(memory_space=vmem),
            pl.BlockSpec(memory_space=vmem),
            pl.BlockSpec(memory_space=anywhere),
            pl.BlockSpec(memory_space=anywhere),
            pl.BlockSpec(memory_space=anywhere),
        ),
        scratch_shapes=[
            vmem((TOP, rows), jnp.int32),
            vmem((TOP, rows), F32),
            vmem((nc, SIDE, 2, ROWS, LANES), BF),
            vmem((3, EXPERTS, 128), F32),
            vmem((SIDE, 3, EXPERTS, 128), F32),
            vmem((3, EXPERTS, 128), F32),
            vmem((2 * nc, 2, slots, LANES), BF),
            vmem((nc, 2, BUNDLE, LANES), BF),
            vmem((128, 128), BF),
            vmem((128, 128), F32),
            vmem((3, 128, 128), BF),
            vmem((2 * BUNDLE, 128), F32),
            vmem((2 * nc, hid, LANES), BF),
            vmem((2 * nc, 2 * SIDE_HID, LANES), BF),
            vmem((slots, 2 * SIDE_HID), F32),
            vmem((slots, SIDE_HID), F32),
            vmem((slots, 2 * SIDE_HID), BF),
            vmem((2 * SIDE_HID, slots), BF),
            vmem((SIDE_HID, slots), BF),
            vmem((nc, slots, LANES), BF),
            vmem((nc, slots, LANES), BF),
            *chunk_buffers((nc,), LANES)[1:],
            vmem((slots, 128), BF),
            vmem((slots, 128), BF),
            *chunk_buffers((), 128),
            dma((5,)),
            dma((1,)), dma((nc,)),
            dma((1,)), dma((1,)),
            dma((1,)), dma((nc, 2)),
            dma((4,)), dma((nc, 4)),
            dma((1,)), dma((nc,)),
            dma((1,)), dma((nc,)),
            dma((nc + 1,)), dma((nc + 1,)),
            dma((2,)), dma((nc + 1,)),
            dma((2,)), dma((nc + 1,)),
            dma((2,)), dma((nc + 1,)),
            dma((2,)), dma((nc + 1,)),
            dma((3,)),
        ],
        compiler_params=pltpu.CompilerParams(
            collective_id=0, has_side_effects=True, vmem_limit_bytes=43 * 1024 * 1024
        ),
    )(
        in_hbm(tokens), in_hbm(cotangent), in_hbm(routes.T), in_hbm(route_weights.T),
        in_hbm(gate_weight.transpose(0, 2, 1)), in_hbm(up_weight.transpose(0, 2, 1)),
        in_hbm(down_weight),
    )
    token_grad, shares, gate_grad, up_grad, down_grad = put_out(
        token_grad, shares, gate_grad, up_grad, down_grad
    )
    return token_grad, shares.T, gate_grad.transpose(0, 2, 1), up_grad.transpose(0, 2, 1), down_grad


def solution(mesh):
    return jax.shard_map(
        per_device,
        mesh=mesh,
        in_specs=(
            P("ep", None),
            P("ep", None),
            P("ep", None),
            P("ep", None),
            P("ep", None, "tp"),
            P("ep", None, "tp"),
            P("ep", "tp", None),
        ),
        out_specs=(
            P("ep", "tp"),
            P("ep", None),
            P("ep", None, "tp"),
            P("ep", None, "tp"),
            P("ep", "tp", None),
        ),
        check_vma=False,
    )
```
